512 devices in a mesh: grp: 2 (over y), sp: 16 (over z), tp: 16 (over x, core).
Axes of the slice: x: 8, y: 2, z: 16, core: 2. Of those that a mesh axis runs over, the one named last changes fastest.
The devices are a block of a 8x16x16 slice.
Arguments:
- hidden_in: bfloat16 [8192, 2048], P(('grp', 'sp'), 'tp'), parts along dimension 0, may hold values from -40 to 40
- norm_gain: float32 [3, 2048], replicated, may hold values from 0.1 to 1.9
- query_weight: bfloat16 [3, 1024, 2048], P(None, 'tp'), may hold values from -6 to 6
- key_weight: bfloat16 [3, 1024, 2048], P(None, 'tp'), may hold values from -6 to 6
- value_weight: bfloat16 [3, 1024, 2048], P(None, 'tp'), may hold values from -0.125 to 0.125
- output_weight: bfloat16 [3, 1024, 2048], P(None, None, 'tp'), may hold values from -0.75 to 0.75
- offset_bias: float32 [3, 16, 15, 31], P(None, 'tp'), may hold values from -4 to 4
Outputs:
- hidden_out: bfloat16 [8192, 2048], P(('grp', 'sp'), 'tp'), parts along dimension 0
The draws below stay inside these ranges and needn't reach their ends.
There are 2 independent parts, one for each index of `grp`. The reference program is written for one: setup_inputs(seed, part) draws one part's arguments, and reference() takes and returns one part's arrays. A program takes and returns all parts, laid end to end along the dimension named above; an argument that names none is the same for every part. Nothing has to cross between parts.
All inputs are finite; a program needn't handle non-finite values.
Results may differ from the reference program's by a relative error of at most 0.028.
Values may be sent and summed in bfloat16 or wider, within the bound.
A program may use at most 64 MiB of HBM per device.

```python
import jax
import jax.numpy as jnp
import numpy as np
from jax import lax

D = 2048
HEADS = 16
HEAD_DIM = 64
GRID_W = 64
ROW_SPAN = 8
COL_SPAN = 16
LAYERS = 3
TOKENS = 4096


def query_draw(key):
    drawn = jax.random.normal(jax.random.fold_in(key, 101), (LAYERS, HEADS * HEAD_DIM, D), jnp.float32)
    return drawn * D ** (-0.5)


def draw_hidden_in(key, part):
    subkeys = jax.random.split(jax.random.fold_in(key, 505), 3)
    normal_part = jax.random.normal(subkeys[0], (TOKENS, D), jnp.float32)
    col_pos = jnp.arange(D, dtype=jnp.float32) / D
    col_scale = jnp.exp(jnp.log(4.0) * col_pos + jax.random.uniform(subkeys[1], (D,), jnp.float32, -0.6, 0.6))
    row_scale = jnp.exp(jax.random.uniform(subkeys[2], (TOKENS, 1), jnp.float32, -1.0, 1.0))
    values = normal_part * col_scale[None, :] * row_scale * 0.6
    return jnp.clip(values, -40.0, 40.0).astype(jnp.bfloat16)


def draw_query_weight(key, part):
    return jnp.clip(query_draw(key), -6.0, 6.0).astype(jnp.bfloat16)


def draw_key_weight(key, part):
    values = jax.random.normal(jax.random.fold_in(key, 202), (LAYERS, HEADS * HEAD_DIM, D), jnp.float32) * D ** (-0.5)
    return jnp.clip(values, -6.0, 6.0).astype(jnp.bfloat16)


def block_levels(rng, shape, shards, low, top_value):
    level = 1.0
    for axis_at, parts in shards:
        heights = jax.random.uniform(jax.random.fold_in(jax.random.fold_in(rng, 6), axis_at), (parts,), jnp.float32, low / len(shards), top_value / len(shards))
        level = level * jnp.repeat(jnp.exp(heights), shape[axis_at] // parts).reshape((-1,) + (1,) * (len(shape) - 1 - axis_at))
    return level


def scatter_about(key, dims, scale, most, cuts=(), held_as=jnp.bfloat16):
    gain = block_levels(key, dims, cuts, -0.22, 0.18) if cuts else 1.0
    values = jax.random.normal(key, dims, jnp.float32) * scale * gain
    return jnp.minimum(jnp.maximum(values, -most), most).astype(held_as)


def setup_inputs(seed: int = 0, part: int = 0) -> dict:
    key_of = jax.random.split(jax.random.key(seed), 8)
    part_keys = jax.random.split(jax.random.fold_in(key_of[7], part), 8)
    return {
        "hidden_in": draw_hidden_in(jax.random.fold_in(jax.random.fold_in(key_of[7], part), 71), part),
        "norm_gain": jnp.clip(1.0 + 0.18 * jax.random.normal(key_of[1], (LAYERS, D), jnp.float32), 0.1, 1.9),
        "query_weight": draw_query_weight(jax.random.fold_in(key_of[7], 71), part),
        "key_weight": draw_key_weight(jax.random.fold_in(key_of[7], 71), part),
        "value_weight": scatter_about(key_of[4], (LAYERS, HEADS * HEAD_DIM, D), D ** -0.5, 0.125, ((1, 16),)),
        "output_weight": scatter_about(key_of[5], (LAYERS, HEADS * HEAD_DIM, D), (HEADS * HEAD_DIM // 16) ** -0.5, 0.75, ((2, 16),)),
        "offset_bias": scatter_about(key_of[6], (LAYERS, HEADS, 2 * ROW_SPAN - 1, 2 * COL_SPAN - 1), 1.0, 4.0, ((1, 16),), jnp.float32),
    }


EPS = 1e-06
NEG = -1e+30
QBLOCK = 16

def column_tables():
    nblocks = GRID_W // QBLOCK
    key_span = QBLOCK + COL_SPAN
    block_start = np.clip(np.arange(nblocks) * QBLOCK - COL_SPAN // 2, 0, GRID_W - key_span)
    key_cols = block_start[:, None] + np.arange(key_span)[None, :]
    query_cols = np.arange(nblocks)[:, None] * QBLOCK + np.arange(QBLOCK)[None, :]
    window_cols = np.clip(query_cols - COL_SPAN // 2, 0, GRID_W - COL_SPAN)
    inside = (key_cols[:, None, :] >= window_cols[:, :, None]) & (key_cols[:, None, :] < window_cols[:, :, None] + COL_SPAN)
    col_offset = np.clip(key_cols[:, None, :] - query_cols[:, :, None], 1 - COL_SPAN, COL_SPAN - 1) + COL_SPAN - 1
    return (block_start, inside, col_offset)

def block_firsts():
    nblocks = GRID_W // QBLOCK
    key_span = QBLOCK + COL_SPAN
    return [min(max(block * QBLOCK - COL_SPAN // 2, 0), GRID_W - key_span) for block in range(nblocks)]

def bias_rows(bias_table, row_offset):
    block_start, inside, col_offset = column_tables()
    nblocks = block_start.shape[0]
    key_span = QBLOCK + COL_SPAN
    rows_n = row_offset.shape[0]
    heads_n = bias_table.shape[0]
    by_row = bias_table[:, row_offset]
    chosen = by_row[:, :, :, jnp.asarray(col_offset, dtype=jnp.int32)]
    chosen = chosen.transpose(1, 0, 3, 4, 2, 5)
    return chosen.reshape(rows_n, heads_n, nblocks, QBLOCK, ROW_SPAN * key_span)

def attend_rows(queries, key_rows, value_rows, bias):
    block_start, inside, col_offset = column_tables()
    nblocks = block_start.shape[0]
    key_span = QBLOCK + COL_SPAN
    rows_n, heads_n, head_size = (queries.shape[0], queries.shape[2], queries.shape[3])

    def pick_blocks(tensor):
        pieces = [tensor[:, :, first_col:first_col + key_span] for first_col in block_firsts()]
        return jnp.stack(pieces, axis=1).reshape(rows_n, nblocks, ROW_SPAN * key_span, heads_n, head_size)
    key_blocks = pick_blocks(key_rows).astype(jnp.float32)
    value_blocks = pick_blocks(value_rows).astype(jnp.float32)
    query_blocks = queries.reshape(rows_n, nblocks, QBLOCK, heads_n, head_size).astype(jnp.float32)
    scores = jnp.einsum('rcqhd,rckhd->rhcqk', query_blocks, key_blocks) * head_size ** (-0.5) + bias
    allowed = np.broadcast_to(inside[:, :, None, :], (nblocks, QBLOCK, ROW_SPAN, key_span))
    allowed = allowed.reshape(nblocks, QBLOCK, ROW_SPAN * key_span)
    scores = jnp.where(jnp.asarray(allowed)[None, None], scores, NEG)
    row_peak = lax.optimization_barrier(jnp.max(scores, axis=-1, keepdims=True))
    lifted = jnp.exp(scores - row_peak)
    weights = (lifted / lax.optimization_barrier(jnp.sum(lifted, axis=-1, keepdims=True))).astype(jnp.bfloat16)
    attended = jnp.einsum('rhcqk,rckhd->rcqhd', weights.astype(jnp.float32), value_blocks)
    return attended.astype(jnp.bfloat16).reshape(rows_n, GRID_W, heads_n, head_size)

def reference(hidden_in, norm_gain, query_weight, key_weight, value_weight, output_weight, offset_bias):
    all_rows = hidden_in.shape[0] // GRID_W
    span_half = ROW_SPAN // 2
    channels = HEADS * HEAD_DIM
    stream = hidden_in
    for layer_idx in range(LAYERS):
        stream_wide = stream.astype(jnp.float32)
        row_scale = lax.rsqrt(lax.optimization_barrier(jnp.mean(stream_wide * stream_wide, axis=1, keepdims=True)) + EPS)
        normed = (stream_wide * row_scale * norm_gain[layer_idx][None, :]).astype(jnp.bfloat16)
        query_grid = jnp.dot(normed, query_weight[layer_idx].T, preferred_element_type=jnp.float32).astype(jnp.bfloat16)
        key_grid = jnp.dot(normed, key_weight[layer_idx].T, preferred_element_type=jnp.float32).astype(jnp.bfloat16)
        value_grid = jnp.dot(normed, value_weight[layer_idx].T, preferred_element_type=jnp.float32).astype(jnp.bfloat16)
        query_grid = query_grid.reshape(all_rows, GRID_W, HEADS, HEAD_DIM)
        key_grid = key_grid.reshape(all_rows, GRID_W, HEADS, HEAD_DIM)
        value_grid = value_grid.reshape(all_rows, GRID_W, HEADS, HEAD_DIM)
        bias_table = offset_bias[layer_idx]

        def one_row(row_idx):
            first_row = jnp.clip(row_idx - span_half, 0, all_rows - ROW_SPAN).astype(jnp.int32)
            key_rows = lax.dynamic_slice_in_dim(key_grid, first_row, ROW_SPAN, 0)[None]
            value_rows = lax.dynamic_slice_in_dim(value_grid, first_row, ROW_SPAN, 0)[None]
            query_row = lax.dynamic_slice_in_dim(query_grid, row_idx, 1, 0)
            row_offset = (first_row + jnp.arange(ROW_SPAN, dtype=jnp.int32) - row_idx + ROW_SPAN - 1).astype(jnp.int32)[None]
            bias = bias_rows(bias_table, row_offset)
            return attend_rows(query_row, key_rows, value_rows, bias)[0]
        attended = lax.map(one_row, jnp.arange(all_rows, dtype=jnp.int32)).reshape(all_rows * GRID_W, channels)
        projected = jnp.dot(attended, output_weight[layer_idx], preferred_element_type=jnp.float32)
        stream = (stream.astype(jnp.float32) + projected).astype(jnp.bfloat16)
    return stream
```

```python
import functools

import jax
import jax.numpy as jnp
from jax import lax
from jax.experimental import pallas as pl
from jax.experimental.pallas import tpu as pltpu
from jax.sharding import PartitionSpec as P

HEAD_DIM = 64
GRID_W = 64
ROW_SPAN = 8
COL_SPAN = 16
EPS = 1e-06
NEG = -1e30
MESH = pl.DeviceIdType.MESH
ORDER = (4, 3, 5, 2, 6, 1, 7)
ARRIVE = (1, 7, 2, 6, 3, 5, 4)


def kernel(
    n_sp,
    n_tp,
    layers,
    hid_ref,
    gain_ref,
    wq_ref,
    wk_ref,
    wv_ref,
    wo_ref,
    ob_ref,
    out_ref,
    xst,
    last_half,
    xs,
    atts,
    kv,
    wraw,
    wg,
    wout,
    tab,
    bias,
    own_w_sem,
    own_o_sem,
    own_x_sem,
    d2d_s,
    d2d_r,
    x_s,
    x_r,
    a_s,
    a_r,
    h_s,
    h_r,
):
    chips = n_tp // 2
    tok = xs.shape[2]
    feat = xs.shape[3]
    half = feat // 2
    tp = lax.axis_index("tp")
    sp = lax.axis_index("sp")
    core = lax.rem(tp, 2)
    chip = lax.div(tp, 2)
    mate = tp + 1 - 2 * core
    up = lax.rem(sp + 1, n_sp)
    down = lax.rem(sp + n_sp - 1, n_sp)

    def peer(j):
        return {"tp": lax.rem(tp + 2 * j, n_tp)}

    def rows_at(start, size, align):
        return pl.ds(pl.multiple_of(start, align), size)

    greet = [peer(j) for j in range(1, chips)]
    greet += [{"tp": mate}]
    greet += [{"sp": z, "tp": t} for z in (up, down) for t in (tp, mate)]
    barrier = pltpu.get_barrier_semaphore()
    for device in greet:
        pl.semaphore_signal(barrier, inc=1, device_id=device, device_id_type=MESH)

    my_lanes = rows_at(core * half, half, half)
    own_x = [
        pltpu.make_async_copy(
            hid_ref.at[rows_at((1 - core) * tok, tok, tok), :], xst, own_x_sem.at[0]
        ),
        pltpu.make_async_copy(
            hid_ref.at[rows_at(core * tok, tok, tok), :], xs.at[0, 0, :, my_lanes], own_x_sem.at[1]
        ),
    ]
    for copy in own_x:
        copy.start()
    w_rows = (
        rows_at(HEAD_DIM * (1 - core), HEAD_DIM, HEAD_DIM),
        rows_at(192 + 64 * core, HEAD_DIM, HEAD_DIM),
        rows_at(128 + 192 * core, HEAD_DIM, HEAD_DIM),
    )
    own_w = []
    own_o = []
    for layer in range(layers):
        for i, w_ref in enumerate((wq_ref, wk_ref, wv_ref)):
            copy = pltpu.make_async_copy(
                w_ref.at[layer], wraw.at[layer, w_rows[i], :], own_w_sem.at[layer, i]
            )
            copy.start()
            own_w.append(copy)
    for layer in range(layers):
        copy = pltpu.make_async_copy(
            wo_ref.at[layer], wout.at[layer, :, my_lanes], own_o_sem.at[layer]
        )
        copy.start()
        own_o.append(copy)

    tab[1] = jnp.zeros(tab.shape[1:], jnp.float32)
    for layer in range(layers):
        tab[1, layer, 0:15, 0:31] = ob_ref[layer]
    for layer in range(layers):
        raw = tab[1, layer]
        low = pltpu.roll(raw, 128 - 15, 1)
        high = pltpu.roll(pltpu.roll(raw, 64 - 15, 1), 15, 0)
        tab[0, layer] = low + high

    pl.semaphore_wait(barrier, len(greet))

    sends = []

    def send(src, dst, s_sem, r_sem, device):
        copy = pltpu.make_async_remote_copy(
            src_ref=src,
            dst_ref=dst,
            send_sem=s_sem,
            recv_sem=r_sem,
            device_id=device,
            device_id_type=MESH,
        )
        copy.start()
        sends.append(copy)
        return copy

    own_x[0].wait()
    x_mate = send(xst, xs.at[0, 0, :, my_lanes], d2d_s.at[0], d2d_r.at[0], {"tp": mate})
    w_mate = []
    sem = 2
    for layer in range(layers):
        for i, w_ref in enumerate((wq_ref, wk_ref, wv_ref)):
            w_mate.append(
                send(
                    w_ref.at[layer],
                    wraw.at[layer, w_rows[i], :],
                    d2d_s.at[sem],
                    d2d_r.at[sem],
                    {"tp": mate},
                )
            )
            sem += 1
        if layer == 0:
            own_x[1].wait()
            x_mate.wait_recv()
            x_gather = [None] * chips
            for j in ORDER:
                x_gather[j] = send(xs.at[0, 0], xs.at[0, j], x_s.at[0, j], x_r.at[0, j], peer(j))
            t_mate = send(tab.at[0], tab.at[2], d2d_s.at[1], d2d_r.at[1], {"tp": mate})
    o_mate = []
    for layer in range(layers):
        o_mate.append(
            send(
                wo_ref.at[layer],
                wout.at[layer, :, my_lanes],
                d2d_s.at[sem],
                d2d_r.at[sem],
                {"tp": mate},
            )
        )
        sem += 1

    def scale_layer(layer):
        for copy in own_w[3 * layer : 3 * layer + 3]:
            copy.wait()
        for copy in w_mate[3 * layer : 3 * layer + 3]:
            copy.wait_recv()

        def one(j, carry):
            source = lax.rem(chip - j + chips, chips)
            lanes = rows_at(source * feat, feat, feat)
            gain = gain_ref[pl.ds(layer, 1), lanes]
            scale = HEAD_DIM ** (-0.5)
            wg[layer, j, 0:128, :] = (
                wraw[layer, 0:128, lanes].astype(jnp.float32) * (gain * scale)
            ).astype(jnp.bfloat16)
            wg[layer, j, 128:384, :] = (
                wraw[layer, 128:384, lanes].astype(jnp.float32) * gain
            ).astype(jnp.bfloat16)
            return carry

        lax.fori_loop(0, chips, one, 0)

    all_rows = n_sp * 4
    starts = []
    offsets = []
    for i in range(2):
        row = sp * 4 + core * 2 + i
        first = jnp.clip(row - ROW_SPAN // 2, 0, all_rows - ROW_SPAN)
        starts.append(first - sp * 4 + 4)
        offsets.append(first - row + ROW_SPAN - 1)

    def make_bias():
        t_mate.wait_recv()
        lane = lax.broadcasted_iota(jnp.int32, (GRID_W, 128), 1)
        key_col = jnp.where(lane < GRID_W, lane, lane - GRID_W)
        query_col = lax.broadcasted_iota(jnp.int32, (GRID_W, 128), 0)
        window = jnp.clip(query_col - COL_SPAN // 2, 0, GRID_W - COL_SPAN)
        inside = (key_col >= window) & (key_col < window + COL_SPAN)

        def one(layer, carry):
            for head in range(2):
                which = jnp.where(core == head, 0, 2)
                for i in range(2):
                    for pair in range(4):
                        line = tab[which, layer, pl.ds(offsets[i] + 2 * pair, 1), :]
                        wide = jnp.broadcast_to(line, (GRID_W, 128))
                        rolled = pltpu.roll(wide, 0, 1, stride=1, stride_axis=0)
                        bias[layer, head, i, :, 128 * pair : 128 * pair + 128] = jnp.where(
                            inside, rolled, NEG
                        )
            return carry

        lax.fori_loop(0, layers, one, 0)

    scale_layer(0)
    make_bias()

    my_rows = rows_at(256 + core * tok, tok, tok)
    lane_low = lax.broadcasted_iota(jnp.int32, (GRID_W, 128), 1) < HEAD_DIM

    for layer in range(layers):
        made = None
        squares = None
        for j in (0,) + ARRIVE:
            if j:
                x_gather[j].wait_recv()
            block = xs[layer, j]
            wide = block.astype(jnp.float32)
            square = wide * wide
            part = lax.dot_general(
                block, wg[layer, j], (((1,), (1,)), ((), ())), preferred_element_type=jnp.float32
            )
            made = part if made is None else made + part
            squares = square if squares is None else squares + square
        mean = jnp.sum(squares, axis=1, keepdims=True) * (1.0 / (feat * chips))
        normed = made * lax.rsqrt(mean + EPS)
        queries = normed[:, 0:128].astype(jnp.bfloat16)
        kv[layer, my_rows, :] = normed[:, 128:384].astype(jnp.bfloat16)
        mine = kv.at[layer, my_rows, :]
        halo = [send(mine, mine, h_s.at[layer, 0], h_r.at[layer, 0], {"tp": mate})]
        above = kv.at[layer, rows_at(core * tok, tok, tok), :]
        below = kv.at[layer, rows_at(512 + core * tok, tok, tok), :]
        spots = ((above, up, tp), (below, down, tp), (above, up, mate), (below, down, mate))
        for i, (spot, z, t) in enumerate(spots):
            halo.append(
                send(mine, spot, h_s.at[layer, i + 1], h_r.at[layer, i + 1], {"sp": z, "tp": t})
            )
        if layer == 0:
            for other in range(1, layers):
                scale_layer(other)
        for copy in halo:
            copy.wait_recv()

        for i in range(2):
            outs = []
            for head in range(2):
                pick = lane_low if head == 1 else jnp.logical_not(lane_low)
                query = jnp.where(pick, queries[GRID_W * i : GRID_W * (i + 1)], 0)
                pairs = kv[
                    layer,
                    rows_at(starts[i] * GRID_W, ROW_SPAN * GRID_W, GRID_W),
                    128 * head : 128 * head + 128,
                ]
                scores = lax.dot_general(
                    query, pairs, (((1,), (1,)), ((), ())), preferred_element_type=jnp.float32
                )
                scores = scores + bias[layer, head, i]
                peak = jnp.max(scores, axis=1, keepdims=True)
                lifted = jnp.exp(scores - peak)
                total = jnp.sum(lifted, axis=1, keepdims=True)
                mixed = jnp.dot(
                    lifted.astype(jnp.bfloat16), pairs, preferred_element_type=jnp.float32
                )
                outs.append(mixed / total)
            both = jnp.where(lane_low, outs[0], outs[1])
            atts[layer, 0, GRID_W * i : GRID_W * (i + 1), :] = both.astype(jnp.bfloat16)

        gather = [None] * chips
        for j in ORDER:
            gather[j] = send(
                atts.at[layer, 0], atts.at[layer, j], a_s.at[layer, j], a_r.at[layer, j], peer(j)
            )
        own_o[layer].wait()
        o_mate[layer].wait_recv()
        stream = xs[layer, 0].astype(jnp.float32)
        for j in (0,) + ARRIVE:
            if j:
                gather[j].wait_recv()
            source = lax.rem(chip - j + chips, chips)
            stream = stream + jnp.dot(
                atts[layer, j],
                wout[layer, rows_at(source * 128, 128, 128), :],
                preferred_element_type=jnp.float32,
            )
        if layer + 1 < layers:
            xs[layer + 1, 0] = stream.astype(jnp.bfloat16)
            for j in ORDER:
                x_gather[j] = send(
                    xs.at[layer + 1, 0],
                    xs.at[layer + 1, j],
                    x_s.at[layer + 1, j],
                    x_r.at[layer + 1, j],
                    peer(j),
                )
        else:
            final = stream.astype(jnp.bfloat16)
            swap = core == 0
            keep = jnp.where(swap, final[:, 0:half], final[:, half:feat])
            last_half[...] = jnp.where(swap, final[:, half:feat], final[:, 0:half])
            place = rows_at(core * tok, tok, tok)
            last = send(last_half, out_ref.at[place, :], d2d_s.at[sem], d2d_r.at[sem], {"tp": mate})
            out_ref[place, :] = keep
            last.wait_recv()
    for copy in sends:
        copy.wait_send()


def body(hidden_in, norm_gain, query_weight, key_weight, value_weight, output_weight, offset_bias):
    n_sp = lax.axis_size("sp")
    n_tp = lax.axis_size("tp")
    chips = n_tp // 2
    layers = norm_gain.shape[0]
    width = norm_gain.shape[1]
    tokens, _ = hidden_in.shape
    tok = tokens // 2
    feat = width // chips
    any_space = pl.BlockSpec(memory_space=pl.ANY)
    vmem = pl.BlockSpec(memory_space=pltpu.VMEM)
    dma = pltpu.SemaphoreType.DMA
    bf16 = jnp.bfloat16
    table = offset_bias.reshape(layers, 2 * ROW_SPAN - 1, 2 * COL_SPAN - 1)
    return pl.pallas_call(
        functools.partial(kernel, n_sp, n_tp, layers),
        out_shape=jax.ShapeDtypeStruct(hidden_in.shape, bf16),
        in_specs=[any_space, vmem, any_space, any_space, any_space, any_space, vmem],
        out_specs=vmem,
        scratch_shapes=[
            pltpu.VMEM((tok, feat // 2), bf16),
            pltpu.VMEM((tok, feat // 2), bf16),
            pltpu.VMEM((layers, chips, tok, feat), bf16),
            pltpu.VMEM((layers, chips, tok, 128), bf16),
            pltpu.VMEM((layers, 768, 256), bf16),
            pltpu.VMEM((layers, 384, width), bf16),
            pltpu.VMEM((layers, chips, 384, feat), bf16),
            pltpu.VMEM((layers, 1024, feat), bf16),
            pltpu.VMEM((3, layers, 16, 128), jnp.float32),
            pltpu.VMEM((layers, 2, 2, GRID_W, ROW_SPAN * GRID_W), jnp.float32),
            dma((layers, 3)),
            dma((layers,)),
            dma((2,)),
            dma((3 + 4 * layers,)),
            dma((3 + 4 * layers,)),
            dma((layers, chips)),
            dma((layers, chips)),
            dma((layers, chips)),
            dma((layers, chips)),
            dma((layers, 5)),
            dma((layers, 5)),
        ],
        compiler_params=pltpu.CompilerParams(
            collective_id=0, has_side_effects=True, vmem_limit_bytes=48 * 1024 * 1024
        ),
        name="layers",
    )(hidden_in, norm_gain, query_weight, key_weight, value_weight, output_weight, table)


def solution(mesh):
    return jax.shard_map(
        body,
        mesh=mesh,
        in_specs=(
            P(("grp", "sp"), "tp"),
            P(),
            P(None, "tp", None),
            P(None, "tp", None),
            P(None, "tp", None),
            P(None, None, "tp"),
            P(None, "tp", None, None),
        ),
        out_specs=P(("grp", "sp"), "tp"),
        check_vma=False,
    )
```

```python
import functools

import jax
import jax.numpy as jnp
from jax import lax
from jax.experimental import pallas as pl
from jax.experimental.pallas import tpu as pltpu
from jax.sharding import PartitionSpec as P

HEAD_DIM = 64
GRID_W = 64
ROW_SPAN = 8
COL_SPAN = 16
EPS = 1e-06
NEG = -1e30
MESH = pl.DeviceIdType.MESH
ORDER = (4, 3, 5, 2, 6, 1, 7)
ARRIVE = (1, 7, 2, 6, 3, 5, 4)


def kernel(
    n_sp,
    n_tp,
    layers,
    hid_ref,
    gain_hbm,
    wq_ref,
    wk_ref,
    wv_ref,
    wo_ref,
    ob_hbm,
    out_ref,
    gain_ref,
    ob_ref,
    xst,
    last_half,
    xs,
    atts,
    kv,
    wraw,
    wg,
    wout,
    tab,
    bias,
    own_w_sem,
    own_o_sem,
    own_x_sem,
    d2d_s,
    d2d_r,
    x_s,
    x_r,
    a_s,
    a_r,
    h_s,
    h_r,
):
    chips = n_tp // 2
    tok = xs.shape[2]
    feat = xs.shape[3]
    half = feat // 2
    tp = lax.axis_index("tp")
    sp = lax.axis_index("sp")
    core = lax.rem(tp, 2)
    chip = lax.div(tp, 2)
    mate = tp + 1 - 2 * core
    up = lax.rem(sp + 1, n_sp)
    down = lax.rem(sp + n_sp - 1, n_sp)

    def peer(j):
        return {"tp": lax.rem(tp + 2 * j, n_tp)}

    def rows_at(start, size, align):
        return pl.ds(pl.multiple_of(start, align), size)

    greet = [peer(j) for j in range(1, chips)]
    greet += [{"tp": mate}]
    greet += [{"sp": z, "tp": t} for z in (up, down) for t in (tp, mate)]
    barrier = pltpu.get_barrier_semaphore()
    for device in greet:
        pl.semaphore_signal(barrier, inc=1, device_id=device, device_id_type=MESH)

    my_lanes = rows_at(core * half, half, half)
    own_x = [
        pltpu.make_async_copy(
            hid_ref.at[rows_at((1 - core) * tok, tok, tok), :], xst, own_x_sem.at[0]
        ),
        pltpu.make_async_copy(
            hid_ref.at[rows_at(core * tok, tok, tok), :], xs.at[0, 0, :, my_lanes], own_x_sem.at[1]
        ),
    ]
    own_g = pltpu.make_async_copy(gain_hbm, gain_ref, own_x_sem.at[2])
    own_b = pltpu.make_async_copy(ob_hbm, ob_ref, own_x_sem.at[3])
    for copy in own_x + [own_b, own_g]:
        copy.start()
    w_rows = (
        rows_at(HEAD_DIM * (1 - core), HEAD_DIM, HEAD_DIM),
        rows_at(192 + 64 * core, HEAD_DIM, HEAD_DIM),
        rows_at(128 + 192 * core, HEAD_DIM, HEAD_DIM),
    )
    own_w = []
    own_o = []
    for layer in range(layers):
        for i, w_ref in enumerate((wq_ref, wk_ref, wv_ref)):
            copy = pltpu.make_async_copy(
                w_ref.at[layer], wraw.at[layer, w_rows[i], :], own_w_sem.at[layer, i]
            )
            copy.start()
            own_w.append(copy)
    for layer in range(layers):
        copy = pltpu.make_async_copy(
            wo_ref.at[layer], wout.at[layer, :, my_lanes], own_o_sem.at[layer]
        )
        copy.start()
        own_o.append(copy)

    tab[1] = jnp.zeros(tab.shape[1:], jnp.float32)
    own_b.wait()
    for layer in range(layers):
        for line in range(2 * ROW_SPAN - 1):
            tab[1, layer, line : line + 1, 0:31] = ob_ref[layer, line]
    for layer in range(layers):
        raw = tab[1, layer]
        low = pltpu.roll(raw, 128 - 15, 1)
        high = pltpu.roll(pltpu.roll(raw, 64 - 15, 1), 15, 0)
        tab[0, layer] = low + high

    pl.semaphore_wait(barrier, len(greet))

    sends = []

    def send(src, dst, s_sem, r_sem, device):
        copy = pltpu.make_async_remote_copy(
            src_ref=src,
            dst_ref=dst,
            send_sem=s_sem,
            recv_sem=r_sem,
            device_id=device,
            device_id_type=MESH,
        )
        copy.start()
        sends.append(copy)
        return copy

    own_x[0].wait()
    x_mate = send(xst, xs.at[0, 0, :, my_lanes], d2d_s.at[0], d2d_r.at[0], {"tp": mate})
    w_mate = []
    sem = 2
    for layer in range(layers):
        for i, w_ref in enumerate((wq_ref, wk_ref, wv_ref)):
            w_mate.append(
                send(
                    w_ref.at[layer],
                    wraw.at[layer, w_rows[i], :],
                    d2d_s.at[sem],
                    d2d_r.at[sem],
                    {"tp": mate},
                )
            )
            sem += 1
        if layer == 0:
            own_x[1].wait()
            x_mate.wait_recv()
            x_gather = [None] * chips
            for j in ORDER:
                x_gather[j] = send(xs.at[0, 0], xs.at[0, j], x_s.at[0, j], x_r.at[0, j], peer(j))
            t_mate = send(tab.at[0], tab.at[2], d2d_s.at[1], d2d_r.at[1], {"tp": mate})
    o_mate = []
    for layer in range(layers):
        o_mate.append(
            send(
                wo_ref.at[layer],
                wout.at[layer, :, my_lanes],
                d2d_s.at[sem],
                d2d_r.at[sem],
                {"tp": mate},
            )
        )
        sem += 1

    def scale_layer(layer):
        for copy in own_w[3 * layer : 3 * layer + 3]:
            copy.wait()
        for copy in w_mate[3 * layer : 3 * layer + 3]:
            copy.wait_recv()

        def one(j, carry):
            source = lax.rem(chip - j + chips, chips)
            lanes = rows_at(source * feat, feat, feat)
            gain = gain_ref[pl.ds(layer, 1), lanes]
            scale = HEAD_DIM ** (-0.5)
            wg[layer, j, 0:128, :] = (
                wraw[layer, 0:128, lanes].astype(jnp.float32) * (gain * scale)
            ).astype(jnp.bfloat16)
            wg[layer, j, 128:384, :] = (
                wraw[layer, 128:384, lanes].astype(jnp.float32) * gain
            ).astype(jnp.bfloat16)
            return carry

        lax.fori_loop(0, chips, one, 0)

    all_rows = n_sp * 4
    starts = []
    offsets = []
    for i in range(2):
        row = sp * 4 + core * 2 + i
        first = jnp.clip(row - ROW_SPAN // 2, 0, all_rows - ROW_SPAN)
        starts.append(first - sp * 4 + 4)
        offsets.append(first - row + ROW_SPAN - 1)

    def make_bias():
        t_mate.wait_recv()
        lane = lax.broadcasted_iota(jnp.int32, (GRID_W, 128), 1)
        key_col = jnp.where(lane < GRID_W, lane, lane - GRID_W)
        query_col = lax.broadcasted_iota(jnp.int32, (GRID_W, 128), 0)
        window = jnp.clip(query_col - COL_SPAN // 2, 0, GRID_W - COL_SPAN)
        inside = (key_col >= window) & (key_col < window + COL_SPAN)

        def one(layer, carry):
            for head in range(2):
                which = jnp.where(core == head, 0, 2)
                for i in range(2):
                    for pair in range(4):
                        line = tab[which, layer, pl.ds(offsets[i] + 2 * pair, 1), :]
                        wide = jnp.broadcast_to(line, (GRID_W, 128))
                        rolled = pltpu.roll(wide, 0, 1, stride=1, stride_axis=0)
                        bias[layer, head, i, :, 128 * pair : 128 * pair + 128] = jnp.where(
                            inside, rolled, NEG
                        )
            return carry

        lax.fori_loop(0, layers, one, 0)

    own_g.wait()
    scale_layer(0)
    make_bias()
    scale_layer(1)

    my_rows = rows_at(256 + core * tok, tok, tok)
    lane_low = lax.broadcasted_iota(jnp.int32, (GRID_W, 128), 1) < HEAD_DIM

    for layer in range(layers):
        made = None
        squares = None
        for j in (0,) + ARRIVE:
            if j:
                x_gather[j].wait_recv()
            block = xs[layer, j]
            wide = block.astype(jnp.float32)
            square = wide * wide
            part = lax.dot_general(
                block, wg[layer, j], (((1,), (1,)), ((), ())), preferred_element_type=jnp.float32
            )
            made = part if made is None else made + part
            squares = square if squares is None else squares + square
        mean = jnp.sum(squares, axis=1, keepdims=True) * (1.0 / (feat * chips))
        normed = made * lax.rsqrt(mean + EPS)
        queries = normed[:, 0:128].astype(jnp.bfloat16)
        kv[layer, my_rows, :] = normed[:, 128:384].astype(jnp.bfloat16)
        mine = kv.at[layer, my_rows, :]
        halo = [send(mine, mine, h_s.at[layer, 0], h_r.at[layer, 0], {"tp": mate})]
        above = kv.at[layer, rows_at(core * tok, tok, tok), :]
        below = kv.at[layer, rows_at(512 + core * tok, tok, tok), :]
        spots = ((above, up, tp), (below, down, tp), (above, up, mate), (below, down, mate))
        for i, (spot, z, t) in enumerate(spots):
            halo.append(
                send(mine, spot, h_s.at[layer, i + 1], h_r.at[layer, i + 1], {"sp": z, "tp": t})
            )
        if layer == 0:
            for other in range(2, layers):
                scale_layer(other)
        for copy in halo:
            copy.wait_recv()

        for i in range(2):
            outs = []
            for head in range(2):
                pick = lane_low if head == 1 else jnp.logical_not(lane_low)
                query = jnp.where(pick, queries[GRID_W * i : GRID_W * (i + 1)], 0)
                pairs = kv[
                    layer,
                    rows_at(starts[i] * GRID_W, ROW_SPAN * GRID_W, GRID_W),
                    128 * head : 128 * head + 128,
                ]
                scores = lax.dot_general(
                    query, pairs, (((1,), (1,)), ((), ())), preferred_element_type=jnp.float32
                )
                scores = scores + bias[layer, head, i]
                peak = jnp.max(scores, axis=1, keepdims=True)
                lifted = jnp.exp(scores - peak)
                total = jnp.sum(lifted, axis=1, keepdims=True)
                mixed = jnp.dot(
                    lifted.astype(jnp.bfloat16), pairs, preferred_element_type=jnp.float32
                )
                outs.append(mixed / total)
            both = jnp.where(lane_low, outs[0], outs[1])
            atts[layer, 0, GRID_W * i : GRID_W * (i + 1), :] = both.astype(jnp.bfloat16)

        gather = [None] * chips
        for j in ORDER:
            gather[j] = send(
                atts.at[layer, 0], atts.at[layer, j], a_s.at[layer, j], a_r.at[layer, j], peer(j)
            )
        own_o[layer].wait()
        o_mate[layer].wait_recv()
        stream = xs[layer, 0].astype(jnp.float32)
        for j in (0,) + ARRIVE:
            if j:
                gather[j].wait_recv()
            source = lax.rem(chip - j + chips, chips)
            stream = stream + jnp.dot(
                atts[layer, j],
                wout[layer, rows_at(source * 128, 128, 128), :],
                preferred_element_type=jnp.float32,
            )
        if layer + 1 < layers:
            xs[layer + 1, 0] = stream.astype(jnp.bfloat16)
            for j in ORDER:
                x_gather[j] = send(
                    xs.at[layer + 1, 0],
                    xs.at[layer + 1, j],
                    x_s.at[layer + 1, j],
                    x_r.at[layer + 1, j],
                    peer(j),
                )
        else:
            final = stream.astype(jnp.bfloat16)
            swap = core == 0
            keep = jnp.where(swap, final[:, 0:half], final[:, half:feat])
            last_half[...] = jnp.where(swap, final[:, half:feat], final[:, 0:half])
            place = rows_at(core * tok, tok, tok)
            last = send(last_half, out_ref.at[place, :], d2d_s.at[sem], d2d_r.at[sem], {"tp": mate})
            out_ref[place, :] = keep
            last.wait_recv()
    for copy in sends:
        copy.wait_send()


def body(hidden_in, norm_gain, query_weight, key_weight, value_weight, output_weight, offset_bias):
    n_sp = lax.axis_size("sp")
    n_tp = lax.axis_size("tp")
    chips = n_tp // 2
    layers = norm_gain.shape[0]
    width = norm_gain.shape[1]
    tokens, _ = hidden_in.shape
    tok = tokens // 2
    feat = width // chips
    any_space = pl.BlockSpec(memory_space=pltpu.HBM)
    vmem = pl.BlockSpec(memory_space=pltpu.VMEM)
    dma = pltpu.SemaphoreType.DMA
    bf16 = jnp.bfloat16
    table = offset_bias.transpose(0, 2, 1, 3)
    return pl.pallas_call(
        functools.partial(kernel, n_sp, n_tp, layers),
        out_shape=jax.ShapeDtypeStruct(hidden_in.shape, bf16),
        in_specs=[any_space] * 7,
        out_specs=vmem,
        scratch_shapes=[
            pltpu.VMEM(norm_gain.shape, jnp.float32),
            pltpu.VMEM(table.shape, jnp.float32),
            pltpu.VMEM((tok, feat // 2), bf16),
            pltpu.VMEM((tok, feat // 2), bf16),
            pltpu.VMEM((layers, chips, tok, feat), bf16),
            pltpu.VMEM((layers, chips, tok, 128), bf16),
            pltpu.VMEM((layers, 768, 256), bf16),
            pltpu.VMEM((layers, 384, width), bf16),
            pltpu.VMEM((layers, chips, 384, feat), bf16),
            pltpu.VMEM((layers, 1024, feat), bf16),
            pltpu.VMEM((3, layers, 16, 128), jnp.float32),
            pltpu.VMEM((layers, 2, 2, GRID_W, ROW_SPAN * GRID_W), jnp.float32),
            dma((layers, 3)),
            dma((layers,)),
            dma((4,)),
            dma((3 + 4 * layers,)),
            dma((3 + 4 * layers,)),
            dma((layers, chips)),
            dma((layers, chips)),
            dma((layers, chips)),
            dma((layers, chips)),
            dma((layers, 5)),
            dma((layers, 5)),
        ],
        compiler_params=pltpu.CompilerParams(
            collective_id=0, has_side_effects=True, vmem_limit_bytes=67043328
        ),
        name="layers",
    )(hidden_in, norm_gain, query_weight, key_weight, value_weight, output_weight, table)


def solution(mesh):
    return jax.shard_map(
        body,
        mesh=mesh,
        in_specs=(
            P(("grp", "sp"), "tp"),
            P(),
            P(None, "tp", None),
            P(None, "tp", None),
            P(None, "tp", None),
            P(None, None, "tp"),
            P(None, "tp", None, None),
        ),
        out_specs=P(("grp", "sp"), "tp"),
        check_vma=False,
    )
```

```python
import functools

import jax
import jax.numpy as jnp
from jax import lax
from jax.experimental import pallas as pl
from jax.experimental.pallas import tpu as pltpu
from jax.sharding import PartitionSpec as P

HEAD_DIM = 64
GRID_W = 64
ROW_SPAN = 8
COL_SPAN = 16
EPS = 1e-06
NEG = -1e30
MESH = pl.DeviceIdType.MESH
ORDER = (4, 3, 5, 2, 6, 1, 7)
ARRIVE = (1, 7, 2, 6, 3, 5, 4)


def kernel(
    n_sp,
    n_tp,
    layers,
    hid_ref,
    gain_hbm,
    wq_ref,
    wk_ref,
    wv_ref,
    wo_ref,
    ob_hbm,
    out_ref,
    gain_ref,
    ob_ref,
    xst,
    last_half,
    xs,
    atts,
    kv,
    wraw,
    wg,
    wout,
    tab,
    bias,
    own_w_sem,
    own_o_sem,
    own_x_sem,
    d2d_s,
    d2d_r,
    f_s,
    f_r,
    x_s,
    x_r,
    a_s,
    a_r,
    h_s,
    h_r,
):
    chips = n_tp // 2
    tok = xs.shape[2]
    feat = xs.shape[3]
    half = feat // 2
    tp = lax.axis_index("tp")
    sp = lax.axis_index("sp")
    core = lax.rem(tp, 2)
    chip = lax.div(tp, 2)
    mate = tp + 1 - 2 * core
    up = lax.rem(sp + 1, n_sp)
    down = lax.rem(sp + n_sp - 1, n_sp)

    def peer(j):
        return {"tp": lax.rem(tp + 2 * j, n_tp)}

    def rows_at(start, size, align):
        return pl.ds(pl.multiple_of(start, align), size)

    greet = [{"tp": lax.rem(tp + j, n_tp)} for j in range(1, n_tp)]
    greet += [{"sp": z, "tp": t} for z in (up, down) for t in (tp, mate)]
    barrier = pltpu.get_barrier_semaphore()
    for device in greet:
        pl.semaphore_signal(barrier, inc=1, device_id=device, device_id_type=MESH)

    my_lanes = rows_at(core * half, half, half)
    own_x = [
        pltpu.make_async_copy(hid_ref, xst, own_x_sem.at[0]),
        pltpu.make_async_copy(
            hid_ref.at[rows_at(core * tok, tok, tok), :], xs.at[0, 0, :, my_lanes], own_x_sem.at[1]
        ),
    ]
    own_g = pltpu.make_async_copy(gain_hbm, gain_ref, own_x_sem.at[2])
    own_b = pltpu.make_async_copy(ob_hbm, ob_ref, own_x_sem.at[3])
    for copy in own_x + [own_b, own_g]:
        copy.start()
    w_rows = (
        rows_at(HEAD_DIM * (1 - core), HEAD_DIM, HEAD_DIM),
        rows_at(192 + 64 * core, HEAD_DIM, HEAD_DIM),
        rows_at(128 + 192 * core, HEAD_DIM, HEAD_DIM),
    )
    own_w = []
    own_o = []
    for layer in range(layers):
        for i, w_ref in enumerate((wq_ref, wk_ref, wv_ref)):
            copy = pltpu.make_async_copy(
                w_ref.at[layer], wraw.at[layer, w_rows[i], :], own_w_sem.at[layer, i]
            )
            copy.start()
            own_w.append(copy)
    for layer in range(layers):
        copy = pltpu.make_async_copy(
            wo_ref.at[layer], wout.at[layer, :, my_lanes], own_o_sem.at[layer]
        )
        copy.start()
        own_o.append(copy)

    tab[1] = jnp.zeros(tab.shape[1:], jnp.float32)
    own_b.wait()
    for layer in range(layers):
        for line in range(2 * ROW_SPAN - 1):
            tab[1, layer, line : line + 1, 0:31] = ob_ref[layer, line]
    for layer in range(layers):
        raw = tab[1, layer]
        low = pltpu.roll(raw, 128 - 15, 1)
        high = pltpu.roll(pltpu.roll(raw, 64 - 15, 1), 15, 0)
        tab[0, layer] = low + high

    pl.semaphore_wait(barrier, len(greet))

    sends = []

    def send(src, dst, s_sem, r_sem, device):
        copy = pltpu.make_async_remote_copy(
            src_ref=src,
            dst_ref=dst,
            send_sem=s_sem,
            recv_sem=r_sem,
            device_id=device,
            device_id_type=MESH,
        )
        copy.start()
        sends.append(copy)
        return copy

    own_x[0].wait()
    first_gather = [{}, {}]
    for i in range(2):
        spot = pl.ds(GRID_W * i, GRID_W)
        given = xst.at[rows_at((1 - core) * tok + GRID_W * i, GRID_W, GRID_W), :]
        kept = xst.at[rows_at(core * tok + GRID_W * i, GRID_W, GRID_W), :]
        for j in ORDER + (0,):
            far = (2 * j + 1 - 2 * core + n_tp) if j else (1 - 2 * core + n_tp)
            there = xs.at[0, j, spot, my_lanes]
            pair = []
            if j:
                pair.append(send(kept, there, f_s.at[i, 0, j], f_r.at[i, 0, j], peer(j)))
            device = {"tp": lax.rem(tp + far, n_tp)}
            pair.append(send(given, there, f_s.at[i, 1, j], f_r.at[i, 1, j], device))
            first_gather[i][j] = pair
    t_mate = send(tab.at[0], tab.at[2], d2d_s.at[1], d2d_r.at[1], {"tp": mate})
    w_mate = []
    sem = 2
    for layer in range(layers):
        for i, w_ref in enumerate((wq_ref, wk_ref, wv_ref)):
            w_mate.append(
                send(
                    w_ref.at[layer],
                    wraw.at[layer, w_rows[i], :],
                    d2d_s.at[sem],
                    d2d_r.at[sem],
                    {"tp": mate},
                )
            )
            sem += 1
    o_mate = []
    for layer in range(layers):
        o_mate.append(
            send(
                wo_ref.at[layer],
                wout.at[layer, :, my_lanes],
                d2d_s.at[sem],
                d2d_r.at[sem],
                {"tp": mate},
            )
        )
        sem += 1

    def scale_layer(layer):
        for copy in own_w[3 * layer : 3 * layer + 3]:
            copy.wait()
        for copy in w_mate[3 * layer : 3 * layer + 3]:
            copy.wait_recv()

        def one(j, carry):
            source = lax.rem(chip - j + chips, chips)
            lanes = rows_at(source * feat, feat, feat)
            gain = gain_ref[pl.ds(layer, 1), lanes]
            scale = HEAD_DIM ** (-0.5)
            wg[layer, j, 0:128, :] = (
                wraw[layer, 0:128, lanes].astype(jnp.float32) * (gain * scale)
            ).astype(jnp.bfloat16)
            wg[layer, j, 128:384, :] = (
                wraw[layer, 128:384, lanes].astype(jnp.float32) * gain
            ).astype(jnp.bfloat16)
            return carry

        lax.fori_loop(0, chips, one, 0)

    all_rows = n_sp * 4
    starts = []
    offsets = []
    for i in range(2):
        row = sp * 4 + core * 2 + i
        first = jnp.clip(row - ROW_SPAN // 2, 0, all_rows - ROW_SPAN)
        starts.append(first - sp * 4 + 4)
        offsets.append(first - row + ROW_SPAN - 1)

    def make_bias():
        t_mate.wait_recv()
        lane = lax.broadcasted_iota(jnp.int32, (GRID_W, 128), 1)
        key_col = jnp.where(lane < GRID_W, lane, lane - GRID_W)
        query_col = lax.broadcasted_iota(jnp.int32, (GRID_W, 128), 0)
        window = jnp.clip(query_col - COL_SPAN // 2, 0, GRID_W - COL_SPAN)
        inside = (key_col >= window) & (key_col < window + COL_SPAN)

        def one(layer, carry):
            for head in range(2):
                which = jnp.where(core == head, 0, 2)
                for i in range(2):
                    for pair in range(4):
                        line = tab[which, layer, pl.ds(offsets[i] + 2 * pair, 1), :]
                        wide = jnp.broadcast_to(line, (GRID_W, 128))
                        rolled = pltpu.roll(wide, 0, 1, stride=1, stride_axis=0)
                        bias[layer, head, i, :, 128 * pair : 128 * pair + 128] = jnp.where(
                            inside, rolled, NEG
                        )
            return carry

        lax.fori_loop(0, layers, one, 0)

    own_g.wait()
    scale_layer(0)
    make_bias()
    scale_layer(1)

    lane_low = lax.broadcasted_iota(jnp.int32, (GRID_W, 128), 1) < HEAD_DIM
    not_last = sp < n_sp - 1
    not_first = sp > 0
    places = [rows_at(256 + core * tok + GRID_W * i, GRID_W, GRID_W) for i in range(2)]

    def halo_copies(layer, i):
        mine = kv.at[layer, places[i], :]
        above = kv.at[layer, rows_at(core * tok + GRID_W * i, GRID_W, GRID_W), :]
        below = kv.at[layer, rows_at(512 + core * tok + GRID_W * i, GRID_W, GRID_W), :]
        to_first = sp == 1
        to_last = sp == n_sp - 2
        at_first = sp == 0
        at_last = sp == n_sp - 1
        low = core == 0
        high = core == 1
        if i == 0:
            down_same, down_same_got = not_first, not_last
        else:
            down_same, down_same_got = to_first, at_first
        plan = (
            (above, up, tp, not_last, not_first),
            (below, down, tp, down_same, down_same_got),
            (
                above,
                up,
                mate,
                not_last & (high | to_last),
                not_first & (low | at_last),
            ),
            (
                below,
                down,
                mate,
                not_first & (low | to_first),
                not_last & (high | at_first),
            ),
        )
        copies = []
        for n, (spot, z, t, sent, got) in enumerate(plan):
            copy = pltpu.make_async_remote_copy(
                src_ref=mine,
                dst_ref=spot,
                send_sem=h_s.at[layer, i, n + 1],
                recv_sem=h_r.at[layer, i, n + 1],
                device_id={"sp": z, "tp": t},
                device_id_type=MESH,
            )
            copies.append((copy, sent, got))
        return mine, copies

    conditional = []
    x_gather = [[None] * chips for _ in range(2)]
    for layer in range(layers):
        queries = []
        mates = []
        halos = []
        for i in range(2):
            spot = slice(GRID_W * i, GRID_W * (i + 1))
            if layer == 0:
                order = [(j, first_gather[i][j]) for j in (0,) + ARRIVE]
            else:
                order = [(0, ())] + [(j, (x_gather[i][j],)) for j in ARRIVE]
            made = None
            squares = None
            for j, copies in order:
                if layer == 0 and i == 0 and j == 0:
                    own_x[1].wait()
                for copy in copies:
                    copy.wait_recv()
                block = xs[layer, j, spot]
                wide = block.astype(jnp.float32)
                square = wide * wide
                part = lax.dot_general(
                    block,
                    wg[layer, j],
                    (((1,), (1,)), ((), ())),
                    preferred_element_type=jnp.float32,
                )
                made = part if made is None else made + part
                squares = square if squares is None else squares + square
            mean = jnp.sum(squares, axis=1, keepdims=True) * (1.0 / (feat * chips))
            normed = made * lax.rsqrt(mean + EPS)
            queries.append(normed[:, 0:128].astype(jnp.bfloat16))
            kv[layer, places[i], :] = normed[:, 128:384].astype(jnp.bfloat16)
            mine, copies = halo_copies(layer, i)
            mates.append(send(mine, mine, h_s.at[layer, i, 0], h_r.at[layer, i, 0], {"tp": mate}))
            for copy, sent, _ in copies:

                @pl.when(sent)
                def _(copy=copy):
                    copy.start()

            halos += copies
            conditional += copies
        if layer == 0:
            for other in range(2, layers):
                scale_layer(other)
        for copy in mates:
            copy.wait_recv()
        for copy, _, got in halos:

            @pl.when(got)
            def _(copy=copy):
                copy.wait_recv()

        gather = [[None] * chips for _ in range(2)]
        for i in range(2):
            spot = pl.ds(GRID_W * i, GRID_W)
            outs = []
            for head in range(2):
                pick = lane_low if head == 1 else jnp.logical_not(lane_low)
                query = jnp.where(pick, queries[i], 0)
                pairs = kv[
                    layer,
                    rows_at(starts[i] * GRID_W, ROW_SPAN * GRID_W, GRID_W),
                    128 * head : 128 * head + 128,
                ]
                scores = lax.dot_general(
                    query, pairs, (((1,), (1,)), ((), ())), preferred_element_type=jnp.float32
                )
                scores = scores + bias[layer, head, i]
                peak = jnp.max(scores, axis=1, keepdims=True)
                lifted = jnp.exp(scores - peak)
                total = jnp.sum(lifted, axis=1, keepdims=True)
                mixed = jnp.dot(
                    lifted.astype(jnp.bfloat16), pairs, preferred_element_type=jnp.float32
                )
                outs.append(mixed / total)
            both = jnp.where(lane_low, outs[0], outs[1])
            atts[layer, 0, spot, :] = both.astype(jnp.bfloat16)
            for j in ORDER:
                gather[i][j] = send(
                    atts.at[layer, 0, spot, :],
                    atts.at[layer, j, spot, :],
                    a_s.at[layer, i, j],
                    a_r.at[layer, i, j],
                    peer(j),
                )

        own_o[layer].wait()
        o_mate[layer].wait_recv()
        last = []
        for i in range(2):
            spot = pl.ds(GRID_W * i, GRID_W)
            stream = xs[layer, 0, spot].astype(jnp.float32)
            for j in (0,) + ARRIVE:
                if j:
                    gather[i][j].wait_recv()
                source = lax.rem(chip - j + chips, chips)
                stream = stream + jnp.dot(
                    atts[layer, j, spot],
                    wout[layer, rows_at(source * 128, 128, 128), :],
                    preferred_element_type=jnp.float32,
                )
            final = stream.astype(jnp.bfloat16)
            if layer + 1 < layers:
                xs[layer + 1, 0, spot, :] = final
                for j in ORDER:
                    x_gather[i][j] = send(
                        xs.at[layer + 1, 0, spot, :],
                        xs.at[layer + 1, j, spot, :],
                        x_s.at[layer, i, j],
                        x_r.at[layer, i, j],
                        peer(j),
                    )
            else:
                swap = core == 0
                last_half[spot, :] = jnp.where(swap, final[:, half:feat], final[:, 0:half])
                place = rows_at(core * tok + GRID_W * i, GRID_W, GRID_W)
                last.append(
                    send(
                        last_half.at[spot, :],
                        out_ref.at[place, :],
                        d2d_s.at[sem],
                        d2d_r.at[sem],
                        {"tp": mate},
                    )
                )
                sem += 1
                out_ref[place, :] = jnp.where(swap, final[:, 0:half], final[:, half:feat])
        for copy in last:
            copy.wait_recv()
    for copy, sent, _ in conditional:

        @pl.when(sent)
        def _(copy=copy):
            copy.wait_send()

    for copy in sends:
        copy.wait_send()


def body(hidden_in, norm_gain, query_weight, key_weight, value_weight, output_weight, offset_bias):
    n_sp = lax.axis_size("sp")
    n_tp = lax.axis_size("tp")
    chips = n_tp // 2
    layers = norm_gain.shape[0]
    width = norm_gain.shape[1]
    tokens, _ = hidden_in.shape
    tok = tokens // 2
    feat = width // chips
    any_space = pl.BlockSpec(memory_space=pltpu.HBM)
    vmem = pl.BlockSpec(memory_space=pltpu.VMEM)
    dma = pltpu.SemaphoreType.DMA
    bf16 = jnp.bfloat16
    table = offset_bias.transpose(0, 2, 1, 3)
    return pl.pallas_call(
        functools.partial(kernel, n_sp, n_tp, layers),
        out_shape=jax.ShapeDtypeStruct(hidden_in.shape, bf16),
        in_specs=[any_space] * 7,
        out_specs=vmem,
        scratch_shapes=[
            pltpu.VMEM(norm_gain.shape, jnp.float32),
            pltpu.VMEM(table.shape, jnp.float32),
            pltpu.VMEM((tokens, feat // 2), bf16),
            pltpu.VMEM((tok, feat // 2), bf16),
            pltpu.VMEM((layers, chips, tok, feat), bf16),
            pltpu.VMEM((layers, chips, tok, 128), bf16),
            pltpu.VMEM((layers, 768, 256), bf16),
            pltpu.VMEM((layers, 384, width), bf16),
            pltpu.VMEM((layers, chips, 384, feat), bf16),
            pltpu.VMEM((layers, 1024, feat), bf16),
            pltpu.VMEM((3, layers, 16, 128), jnp.float32),
            pltpu.VMEM((layers, 2, 2, GRID_W, ROW_SPAN * GRID_W), jnp.float32),
            dma((layers, 3)),
            dma((layers,)),
            dma((4,)),
            dma((4 + 4 * layers,)),
            dma((4 + 4 * layers,)),
            dma((2, 2, chips)),
            dma((2, 2, chips)),
            dma((layers, 2, chips)),
            dma((layers, 2, chips)),
            dma((layers, 2, chips)),
            dma((layers, 2, chips)),
            dma((layers, 2, 5)),
            dma((layers, 2, 5)),
        ],
        compiler_params=pltpu.CompilerParams(
            collective_id=0, has_side_effects=True, vmem_limit_bytes=67043328
        ),
        name="layers",
    )(hidden_in, norm_gain, query_weight, key_weight, value_weight, output_weight, table)


def solution(mesh):
    return jax.shard_map(
        body,
        mesh=mesh,
        in_specs=(
            P(("grp", "sp"), "tp"),
            P(),
            P(None, "tp", None),
            P(None, "tp", None),
            P(None, "tp", None),
            P(None, None, "tp"),
            P(None, "tp", None, None),
        ),
        out_specs=P(("grp", "sp"), "tp"),
        check_vma=False,
    )
```

```python
import functools

import jax
import jax.numpy as jnp
from jax import lax
from jax.experimental import pallas as pl
from jax.experimental.pallas import tpu as pltpu
from jax.sharding import PartitionSpec as P

HEAD_DIM = 64
GRID_W = 64
ROW_SPAN = 8
COL_SPAN = 16
EPS = 1e-06
NEG = -1e30
MESH = pl.DeviceIdType.MESH
ORDER = (4, 3, 5, 2, 6, 1, 7)
ARRIVE = (1, 7, 2, 6, 3, 5, 4)
HELD = (0, 5, 3)
HANDED = ((0, 1, 1), (0, -1, 7), (5, 1, 6), (5, -1, 4), (3, -1, 2))


def kernel(
    n_sp,
    n_tp,
    layers,
    hid_ref,
    gain_hbm,
    wq_ref,
    wk_ref,
    wv_ref,
    wo_ref,
    ob_hbm,
    out_ref,
    gain_ref,
    ob_ref,
    xst,
    last_half,
    xs,
    atts,
    kv,
    wraw,
    wg,
    wout,
    tab,
    bias,
    own_w_sem,
    own_o_sem,
    own_x_sem,
    d2d_s,
    d2d_r,
    f_s,
    f_r,
    e_s,
    e_r,
    x_s,
    x_r,
    a_s,
    a_r,
    h_s,
    h_r,
):
    chips = n_tp // 2
    tok = xs.shape[2]
    feat = xs.shape[3]
    half = feat // 2
    tp = lax.axis_index("tp")
    sp = lax.axis_index("sp")
    core = lax.rem(tp, 2)
    chip = lax.div(tp, 2)
    mate = tp + 1 - 2 * core
    up = lax.rem(sp + 1, n_sp)
    down = lax.rem(sp + n_sp - 1, n_sp)

    def peer(j):
        return {"tp": lax.rem(tp + 2 * j + n_tp, n_tp)}

    def rows_at(start, size, align):
        return pl.ds(pl.multiple_of(start, align), size)

    greet = [{"tp": lax.rem(tp + j, n_tp)} for j in range(1, n_tp)]
    greet += [{"sp": z, "tp": t} for z in (up, down) for t in (tp, mate)]
    barrier = pltpu.get_barrier_semaphore()
    for device in greet:
        pl.semaphore_signal(barrier, inc=1, device_id=device, device_id_type=MESH)

    my_lanes = rows_at(core * half, half, half)
    own_x = [
        pltpu.make_async_copy(hid_ref, xst, own_x_sem.at[0]),
        pltpu.make_async_copy(
            hid_ref.at[rows_at(core * tok, tok, tok), :], xs.at[0, 0, :, my_lanes], own_x_sem.at[1]
        ),
    ]
    own_g = pltpu.make_async_copy(gain_hbm, gain_ref, own_x_sem.at[2])
    own_b = pltpu.make_async_copy(ob_hbm, ob_ref, own_x_sem.at[3])
    for copy in own_x + [own_b, own_g]:
        copy.start()
    w_rows = (
        rows_at(HEAD_DIM * (1 - core), HEAD_DIM, HEAD_DIM),
        rows_at(192 + 64 * core, HEAD_DIM, HEAD_DIM),
        rows_at(128 + 192 * core, HEAD_DIM, HEAD_DIM),
    )
    own_w = []
    own_o = []
    for layer in range(layers):
        for i, w_ref in enumerate((wq_ref, wk_ref, wv_ref)):
            copy = pltpu.make_async_copy(
                w_ref.at[layer], wraw.at[layer, w_rows[i], :], own_w_sem.at[layer, i]
            )
            copy.start()
            own_w.append(copy)
    for layer in range(layers):
        copy = pltpu.make_async_copy(
            wo_ref.at[layer], wout.at[layer, 0, :, my_lanes], own_o_sem.at[layer]
        )
        copy.start()
        own_o.append(copy)

    tab[1] = jnp.zeros(tab.shape[1:], jnp.float32)
    own_b.wait()
    for layer in range(layers):
        for line in range(2 * ROW_SPAN - 1):
            tab[1, layer, line : line + 1, 0:31] = ob_ref[layer, line]
    for layer in range(layers):
        raw = tab[1, layer]
        low = pltpu.roll(raw, 128 - 15, 1)
        high = pltpu.roll(pltpu.roll(raw, 64 - 15, 1), 15, 0)
        tab[0, layer] = low + high

    pl.semaphore_wait(barrier, len(greet))

    sends = []

    def send(src, dst, s_sem, r_sem, device):
        copy = pltpu.make_async_remote_copy(
            src_ref=src,
            dst_ref=dst,
            send_sem=s_sem,
            recv_sem=r_sem,
            device_id=device,
            device_id_type=MESH,
        )
        copy.start()
        sends.append(copy)
        return copy

    own_x[0].wait()
    first_gather = [{}, {}]
    for i in range(2):
        spot = pl.ds(GRID_W * i, GRID_W)
        given = xst.at[rows_at((1 - core) * tok + GRID_W * i, GRID_W, GRID_W), :]
        kept = xst.at[rows_at(core * tok + GRID_W * i, GRID_W, GRID_W), :]
        for j in ORDER + (0,):
            far = (2 * j + 1 - 2 * core + n_tp) if j else (1 - 2 * core + n_tp)
            there = xs.at[0, j, spot, my_lanes]
            pair = []
            if j:
                pair.append(send(kept, there, f_s.at[i, 0, j], f_r.at[i, 0, j], peer(j)))
            device = {"tp": lax.rem(tp + far, n_tp)}
            pair.append(send(given, there, f_s.at[i, 1, j], f_r.at[i, 1, j], device))
            first_gather[i][j] = pair
    t_mate = send(tab.at[0], tab.at[2], d2d_s.at[1], d2d_r.at[1], {"tp": mate})
    w_mate = []
    sem = 2
    for layer in range(layers):
        for i, w_ref in enumerate((wq_ref, wk_ref, wv_ref)):
            w_mate.append(
                send(
                    w_ref.at[layer],
                    wraw.at[layer, w_rows[i], :],
                    d2d_s.at[sem],
                    d2d_r.at[sem],
                    {"tp": mate},
                )
            )
            sem += 1
    o_mate = []
    for layer in range(layers):
        o_mate.append(
            send(
                wo_ref.at[layer],
                wout.at[layer, 0, :, my_lanes],
                d2d_s.at[sem],
                d2d_r.at[sem],
                {"tp": mate},
            )
        )
        sem += 1

    def scale_layer(layer):
        for copy in own_w[3 * layer : 3 * layer + 3]:
            copy.wait()
        for copy in w_mate[3 * layer : 3 * layer + 3]:
            copy.wait_recv()

        def one(j, carry):
            source = lax.rem(chip - j + chips, chips)
            lanes = rows_at(source * feat, feat, feat)
            gain = gain_ref[pl.ds(layer, 1), lanes]
            scale = HEAD_DIM ** (-0.5)
            wg[layer, j, 0:128, :] = (
                wraw[layer, 0:128, lanes].astype(jnp.float32) * (gain * scale)
            ).astype(jnp.bfloat16)
            wg[layer, j, 128:384, :] = (
                wraw[layer, 128:384, lanes].astype(jnp.float32) * gain
            ).astype(jnp.bfloat16)
            return carry

        lax.fori_loop(0, chips, one, 0)

    all_rows = n_sp * 4
    starts = []
    offsets = []
    for i in range(2):
        row = sp * 4 + core * 2 + i
        first = jnp.clip(row - ROW_SPAN // 2, 0, all_rows - ROW_SPAN)
        starts.append(first - sp * 4 + 4)
        offsets.append(first - row + ROW_SPAN - 1)

    def make_bias():
        t_mate.wait_recv()
        lane = lax.broadcasted_iota(jnp.int32, (GRID_W, 128), 1)
        key_col = jnp.where(lane < GRID_W, lane, lane - GRID_W)
        query_col = lax.broadcasted_iota(jnp.int32, (GRID_W, 128), 0)
        window = jnp.clip(query_col - COL_SPAN // 2, 0, GRID_W - COL_SPAN)
        inside = (key_col >= window) & (key_col < window + COL_SPAN)

        def one(layer, carry):
            for head in range(2):
                which = jnp.where(core == head, 0, 2)
                for i in range(2):
                    for pair in range(4):
                        line = tab[which, layer, pl.ds(offsets[i] + 2 * pair, 1), :]
                        wide = jnp.broadcast_to(line, (GRID_W, 128))
                        rolled = pltpu.roll(wide, 0, 1, stride=1, stride_axis=0)
                        bias[layer, head, i, :, 128 * pair : 128 * pair + 128] = jnp.where(
                            inside, rolled, NEG
                        )
            return carry

        lax.fori_loop(0, layers, one, 0)

    own_g.wait()
    scale_layer(0)
    make_bias()
    scale_layer(1)

    lane_low = lax.broadcasted_iota(jnp.int32, (GRID_W, 128), 1) < HEAD_DIM
    not_last = sp < n_sp - 1
    not_first = sp > 0
    places = [rows_at(256 + core * tok + GRID_W * i, GRID_W, GRID_W) for i in range(2)]

    def halo_copies(layer, i):
        mine = kv.at[layer, places[i], :]
        above = kv.at[layer, rows_at(core * tok + GRID_W * i, GRID_W, GRID_W), :]
        below = kv.at[layer, rows_at(512 + core * tok + GRID_W * i, GRID_W, GRID_W), :]
        to_first = sp == 1
        to_last = sp == n_sp - 2
        at_first = sp == 0
        at_last = sp == n_sp - 1
        low = core == 0
        high = core == 1
        if i == 0:
            down_same, down_same_got = not_first, not_last
        else:
            down_same, down_same_got = to_first, at_first
        plan = (
            (above, up, tp, not_last, not_first),
            (below, down, tp, down_same, down_same_got),
            (
                above,
                up,
                mate,
                not_last & (high | to_last),
                not_first & (low | at_last),
            ),
            (
                below,
                down,
                mate,
                not_first & (low | to_first),
                not_last & (high | at_first),
            ),
        )
        copies = []
        for n, (spot, z, t, sent, got) in enumerate(plan):
            copy = pltpu.make_async_remote_copy(
                src_ref=mine,
                dst_ref=spot,
                send_sem=h_s.at[layer, i, n + 1],
                recv_sem=h_r.at[layer, i, n + 1],
                device_id={"sp": z, "tp": t},
                device_id_type=MESH,
            )
            copies.append((copy, sent, got))
        return mine, copies

    conditional = []
    x_gather = [[], []]
    for layer in range(layers):
        queries = []
        mates = []
        halos = []
        for i in range(2):
            spot = slice(GRID_W * i, GRID_W * (i + 1))
            if layer == 0:
                order = [(j, first_gather[i][j]) for j in (0,) + ARRIVE]
            else:
                order = [(j, ()) for j in HELD] + x_gather[i]
            made = None
            squares = None
            for j, copies in order:
                if layer == 0 and i == 0 and j == 0:
                    own_x[1].wait()
                for copy in copies:
                    copy.wait_recv()
                block = xs[layer, j, spot]
                wide = block.astype(jnp.float32)
                square = wide * wide
                part = lax.dot_general(
                    block,
                    wg[layer, j],
                    (((1,), (1,)), ((), ())),
                    preferred_element_type=jnp.float32,
                )
                made = part if made is None else made + part
                squares = square if squares is None else squares + square
            if i == 0 and layer + 1 < layers:
                shipped = []
                for n, away in ((1, -3), (2, 3)):
                    shipped.append(
                        send(
                            wo_ref.at[layer],
                            wout.at[layer, n, :, my_lanes],
                            e_s.at[layer, 0, n - 1],
                            e_r.at[layer, 0, n - 1],
                            peer(away),
                        )
                    )
            mean = jnp.sum(squares, axis=1, keepdims=True) * (1.0 / (feat * chips))
            normed = made * lax.rsqrt(mean + EPS)
            queries.append(normed[:, 0:128].astype(jnp.bfloat16))
            kv[layer, places[i], :] = normed[:, 128:384].astype(jnp.bfloat16)
            mine, copies = halo_copies(layer, i)
            mates.append(send(mine, mine, h_s.at[layer, i, 0], h_r.at[layer, i, 0], {"tp": mate}))
            for copy, sent, _ in copies:

                @pl.when(sent)
                def _(copy=copy):
                    copy.start()

            halos += copies
            conditional += copies
        if layer == 0:
            for other in range(2, layers):
                scale_layer(other)
        for copy in mates:
            copy.wait_recv()
        for copy, _, got in halos:

            @pl.when(got)
            def _(copy=copy):
                copy.wait_recv()

        gather = [[None] * chips for _ in range(2)]
        for i in range(2):
            spot = pl.ds(GRID_W * i, GRID_W)
            outs = []
            for head in range(2):
                pick = lane_low if head == 1 else jnp.logical_not(lane_low)
                query = jnp.where(pick, queries[i], 0)
                pairs = kv[
                    layer,
                    rows_at(starts[i] * GRID_W, ROW_SPAN * GRID_W, GRID_W),
                    128 * head : 128 * head + 128,
                ]
                scores = lax.dot_general(
                    query, pairs, (((1,), (1,)), ((), ())), preferred_element_type=jnp.float32
                )
                scores = scores + bias[layer, head, i]
                peak = jnp.max(scores, axis=1, keepdims=True)
                lifted = jnp.exp(scores - peak)
                total = jnp.sum(lifted, axis=1, keepdims=True)
                mixed = jnp.dot(
                    lifted.astype(jnp.bfloat16), pairs, preferred_element_type=jnp.float32
                )
                outs.append(mixed / total)
            both = jnp.where(lane_low, outs[0], outs[1])
            atts[layer, 0, spot, :] = both.astype(jnp.bfloat16)
            for j in ORDER:
                gather[i][j] = send(
                    atts.at[layer, 0, spot, :],
                    atts.at[layer, j, spot, :],
                    a_s.at[layer, i, j],
                    a_r.at[layer, i, j],
                    peer(j),
                )

        own_o[layer].wait()
        o_mate[layer].wait_recv()
        held = HELD[:1]
        if layer + 1 < layers:
            held = HELD
            relayed = []
            for n in (1, 2):
                shipped[n - 1].wait_recv()
                spot = wout.at[layer, n, :, my_lanes]
                relayed.append(
                    send(
                        spot,
                        spot,
                        e_s.at[layer, 1, n - 1],
                        e_r.at[layer, 1, n - 1],
                        {"tp": mate},
                    )
                )
            for copy in relayed:
                copy.wait_recv()
        last = []
        for i in range(2):
            spot = pl.ds(GRID_W * i, GRID_W)
            streams = [xs[layer, slot, spot].astype(jnp.float32) for slot in held]
            for j in (0,) + ARRIVE:
                if j:
                    gather[i][j].wait_recv()
                source = lax.rem(chip - j + chips, chips)
                block = atts[layer, j, spot]
                for n in range(len(held)):
                    streams[n] = streams[n] + jnp.dot(
                        block,
                        wout[layer, n, rows_at(source * 128, 128, 128), :],
                        preferred_element_type=jnp.float32,
                    )
            finals = [stream.astype(jnp.bfloat16) for stream in streams]
            final = finals[0]
            if layer + 1 < layers:
                for slot, block in zip(held, finals, strict=True):
                    xs[layer + 1, slot, spot, :] = block
                x_gather[i] = []
                for slot, far, there in HANDED:
                    copy = send(
                        xs.at[layer + 1, slot, spot, :],
                        xs.at[layer + 1, there, spot, :],
                        x_s.at[layer, i, there],
                        x_r.at[layer, i, there],
                        peer(far),
                    )
                    x_gather[i].append((there, (copy,)))
            else:
                swap = core == 0
                last_half[spot, :] = jnp.where(swap, final[:, half:feat], final[:, 0:half])
                place = rows_at(core * tok + GRID_W * i, GRID_W, GRID_W)
                last.append(
                    send(
                        last_half.at[spot, :],
                        out_ref.at[place, :],
                        d2d_s.at[sem],
                        d2d_r.at[sem],
                        {"tp": mate},
                    )
                )
                sem += 1
                out_ref[place, :] = jnp.where(swap, final[:, 0:half], final[:, half:feat])
        for copy in last:
            copy.wait_recv()
    for copy, sent, _ in conditional:

        @pl.when(sent)
        def _(copy=copy):
            copy.wait_send()

    for copy in sends:
        copy.wait_send()


def body(hidden_in, norm_gain, query_weight, key_weight, value_weight, output_weight, offset_bias):
    n_sp = lax.axis_size("sp")
    n_tp = lax.axis_size("tp")
    chips = n_tp // 2
    layers = norm_gain.shape[0]
    width = norm_gain.shape[1]
    tokens, _ = hidden_in.shape
    tok = tokens // 2
    feat = width // chips
    any_space = pl.BlockSpec(memory_space=pltpu.HBM)
    vmem = pl.BlockSpec(memory_space=pltpu.VMEM)
    dma = pltpu.SemaphoreType.DMA
    bf16 = jnp.bfloat16
    table = offset_bias.transpose(0, 2, 1, 3)
    return pl.pallas_call(
        functools.partial(kernel, n_sp, n_tp, layers),
        out_shape=jax.ShapeDtypeStruct(hidden_in.shape, bf16),
        in_specs=[any_space] * 7,
        out_specs=vmem,
        scratch_shapes=[
            pltpu.VMEM(norm_gain.shape, jnp.float32),
            pltpu.VMEM(table.shape, jnp.float32),
            pltpu.VMEM((tokens, feat // 2), bf16),
            pltpu.VMEM((tok, feat // 2), bf16),
            pltpu.VMEM((layers, chips, tok, feat), bf16),
            pltpu.VMEM((layers, chips, tok, 128), bf16),
            pltpu.VMEM((layers, 768, 256), bf16),
            pltpu.VMEM((layers, 384, width), bf16),
            pltpu.VMEM((layers, chips, 384, feat), bf16),
            pltpu.VMEM((layers, 3, 1024, feat), bf16),
            pltpu.VMEM((3, layers, 16, 128), jnp.float32),
            pltpu.VMEM((layers, 2, 2, GRID_W, ROW_SPAN * GRID_W), jnp.float32),
            dma((layers, 3)),
            dma((layers,)),
            dma((4,)),
            dma((4 + 4 * layers,)),
            dma((4 + 4 * layers,)),
            dma((2, 2, chips)),
            dma((2, 2, chips)),
            dma((layers, 2, 2)),
            dma((layers, 2, 2)),
            dma((layers, 2, chips)),
            dma((layers, 2, chips)),
            dma((layers, 2, chips)),
            dma((layers, 2, chips)),
            dma((layers, 2, 5)),
            dma((layers, 2, 5)),
        ],
        compiler_params=pltpu.CompilerParams(
            collective_id=0, has_side_effects=True, vmem_limit_bytes=67043328
        ),
        name="layers",
    )(hidden_in, norm_gain, query_weight, key_weight, value_weight, output_weight, table)


def solution(mesh):
    return jax.shard_map(
        body,
        mesh=mesh,
        in_specs=(
            P(("grp", "sp"), "tp"),
            P(),
            P(None, "tp", None),
            P(None, "tp", None),
            P(None, "tp", None),
            P(None, None, "tp"),
            P(None, "tp", None, None),
        ),
        out_specs=P(("grp", "sp"), "tp"),
        check_vma=False,
    )
```

```python
import functools

import jax
import jax.numpy as jnp
from jax import lax
from jax.experimental import pallas as pl
from jax.experimental.pallas import tpu as pltpu
from jax.sharding import PartitionSpec as P

HEAD_DIM = 64
GRID_W = 64
ROW_SPAN = 8
COL_SPAN = 16
EPS = 1e-06
NEG = -1e30
MESH = pl.DeviceIdType.MESH
ORDER = (2, 6, 1, 7)
ARRIVE = (1, 7, 2, 6, 3, 5, 4)
HAND = (((2, 2, 4), (2, 1, 3), (6, -1, 5)), ((6, -2, 4), (6, -1, 5), (2, 1, 3)))


def kernel(
    n_sp,
    n_tp,
    layers,
    hid_ref,
    gain_hbm,
    wq_ref,
    wk_ref,
    wv_ref,
    wo_ref,
    ob_hbm,
    out_ref,
    gain_ref,
    ob_ref,
    xst,
    last_half,
    xs,
    atts,
    kv,
    wraw,
    wg,
    wout,
    tab,
    bias,
    own_w_sem,
    own_o_sem,
    own_x_sem,
    d2d_s,
    d2d_r,
    f_s,
    f_r,
    x_s,
    x_r,
    a_s,
    a_r,
    h_s,
    h_r,
):
    chips = n_tp // 2
    tok = xs.shape[2]
    feat = xs.shape[3]
    half = feat // 2
    tp = lax.axis_index("tp")
    sp = lax.axis_index("sp")
    core = lax.rem(tp, 2)
    chip = lax.div(tp, 2)
    mate = tp + 1 - 2 * core
    up = lax.rem(sp + 1, n_sp)
    down = lax.rem(sp + n_sp - 1, n_sp)

    def peer(j):
        return {"tp": lax.rem(tp + 2 * j + n_tp, n_tp)}

    def rows_at(start, size, align):
        return pl.ds(pl.multiple_of(start, align), size)

    greet = [{"tp": lax.rem(tp + j, n_tp)} for j in range(1, n_tp)]
    greet += [{"sp": z, "tp": t} for z in (up, down) for t in (tp, mate)]
    barrier = pltpu.get_barrier_semaphore()
    for device in greet:
        pl.semaphore_signal(barrier, inc=1, device_id=device, device_id_type=MESH)

    my_lanes = rows_at(core * half, half, half)
    own_x = [
        pltpu.make_async_copy(hid_ref, xst, own_x_sem.at[0]),
        pltpu.make_async_copy(
            hid_ref.at[rows_at(core * tok, tok, tok), :], xs.at[0, 0, :, my_lanes], own_x_sem.at[1]
        ),
    ]
    own_g = pltpu.make_async_copy(gain_hbm, gain_ref, own_x_sem.at[2])
    own_b = pltpu.make_async_copy(ob_hbm, ob_ref, own_x_sem.at[3])
    for copy in own_x + [own_b, own_g]:
        copy.start()
    w_rows = (
        rows_at(HEAD_DIM * (1 - core), HEAD_DIM, HEAD_DIM),
        rows_at(192 + 64 * core, HEAD_DIM, HEAD_DIM),
        rows_at(128 + 192 * core, HEAD_DIM, HEAD_DIM),
    )
    own_w = []
    own_o = []
    for layer in range(layers):
        for i, w_ref in enumerate((wq_ref, wk_ref, wv_ref)):
            copy = pltpu.make_async_copy(
                w_ref.at[layer], wraw.at[layer, w_rows[i], :], own_w_sem.at[layer, i]
            )
            copy.start()
            own_w.append(copy)
    for layer in range(layers):
        copy = pltpu.make_async_copy(
            wo_ref.at[layer], wout.at[layer, :, my_lanes], own_o_sem.at[layer]
        )
        copy.start()
        own_o.append(copy)

    tab[1] = jnp.zeros(tab.shape[1:], jnp.float32)
    own_b.wait()
    for layer in range(layers):
        for line in range(2 * ROW_SPAN - 1):
            tab[1, layer, line : line + 1, 0:31] = ob_ref[layer, line]
    for layer in range(layers):
        raw = tab[1, layer]
        low = pltpu.roll(raw, 128 - 15, 1)
        high = pltpu.roll(pltpu.roll(raw, 64 - 15, 1), 15, 0)
        tab[0, layer] = low + high

    pl.semaphore_wait(barrier, len(greet))

    sends = []

    def send(src, dst, s_sem, r_sem, device):
        copy = pltpu.make_async_remote_copy(
            src_ref=src,
            dst_ref=dst,
            send_sem=s_sem,
            recv_sem=r_sem,
            device_id=device,
            device_id_type=MESH,
        )
        copy.start()
        sends.append(copy)
        return copy

    own_x[0].wait()
    first_gather = [{}, {}]
    for i in range(2):
        spot = pl.ds(GRID_W * i, GRID_W)
        given = xst.at[rows_at((1 - core) * tok + GRID_W * i, GRID_W, GRID_W), :]
        kept = xst.at[rows_at(core * tok + GRID_W * i, GRID_W, GRID_W), :]
        for j in ORDER + (0,):
            far = (2 * j + 1 - 2 * core + n_tp) if j else (1 - 2 * core + n_tp)
            there = xs.at[0, j, spot, my_lanes]
            pair = []
            if j:
                pair.append(send(kept, there, f_s.at[i, 0, j], f_r.at[i, 0, j], peer(j)))
            device = {"tp": lax.rem(tp + far, n_tp)}
            pair.append(send(given, there, f_s.at[i, 1, j], f_r.at[i, 1, j], device))
            first_gather[i][j] = pair
    t_mate = send(tab.at[0], tab.at[2], d2d_s.at[1], d2d_r.at[1], {"tp": mate})
    w_mate = []
    sem = 2
    for layer in range(layers):
        for i, w_ref in enumerate((wq_ref, wk_ref, wv_ref)):
            w_mate.append(
                send(
                    w_ref.at[layer],
                    wraw.at[layer, w_rows[i], :],
                    d2d_s.at[sem],
                    d2d_r.at[sem],
                    {"tp": mate},
                )
            )
            sem += 1
    o_mate = []
    for layer in range(layers):
        o_mate.append(
            send(
                wo_ref.at[layer],
                wout.at[layer, :, my_lanes],
                d2d_s.at[sem],
                d2d_r.at[sem],
                {"tp": mate},
            )
        )
        sem += 1

    def scale_layer(layer):
        for copy in own_w[3 * layer : 3 * layer + 3]:
            copy.wait()
        for copy in w_mate[3 * layer : 3 * layer + 3]:
            copy.wait_recv()

        def one(j, carry):
            source = lax.rem(chip - j + chips, chips)
            lanes = rows_at(source * feat, feat, feat)
            gain = gain_ref[pl.ds(layer, 1), lanes]
            scale = HEAD_DIM ** (-0.5)
            wg[layer, j, 0:128, :] = (
                wraw[layer, 0:128, lanes].astype(jnp.float32) * (gain * scale)
            ).astype(jnp.bfloat16)
            wg[layer, j, 128:384, :] = (
                wraw[layer, 128:384, lanes].astype(jnp.float32) * gain
            ).astype(jnp.bfloat16)
            return carry

        lax.fori_loop(0, chips, one, 0)

    all_rows = n_sp * 4
    starts = []
    offsets = []
    for i in range(2):
        row = sp * 4 + core * 2 + i
        first = jnp.clip(row - ROW_SPAN // 2, 0, all_rows - ROW_SPAN)
        starts.append(first - sp * 4 + 4)
        offsets.append(first - row + ROW_SPAN - 1)

    def make_bias():
        t_mate.wait_recv()
        lane = lax.broadcasted_iota(jnp.int32, (GRID_W, 128), 1)
        key_col = jnp.where(lane < GRID_W, lane, lane - GRID_W)
        query_col = lax.broadcasted_iota(jnp.int32, (GRID_W, 128), 0)
        window = jnp.clip(query_col - COL_SPAN // 2, 0, GRID_W - COL_SPAN)
        inside = (key_col >= window) & (key_col < window + COL_SPAN)

        def one(layer, carry):
            for head in range(2):
                which = jnp.where(core == head, 0, 2)
                for i in range(2):
                    for pair in range(4):
                        line = tab[which, layer, pl.ds(offsets[i] + 2 * pair, 1), :]
                        wide = jnp.broadcast_to(line, (GRID_W, 128))
                        rolled = pltpu.roll(wide, 0, 1, stride=1, stride_axis=0)
                        bias[layer, head, i, :, 128 * pair : 128 * pair + 128] = jnp.where(
                            inside, rolled, NEG
                        )
            return carry

        lax.fori_loop(0, layers, one, 0)

    own_g.wait()
    scale_layer(0)
    make_bias()
    scale_layer(1)

    lane_low = lax.broadcasted_iota(jnp.int32, (GRID_W, 128), 1) < HEAD_DIM
    not_last = sp < n_sp - 1
    not_first = sp > 0
    places = [rows_at(256 + core * tok + GRID_W * i, GRID_W, GRID_W) for i in range(2)]

    def halo_copies(layer, i):
        mine = kv.at[layer, places[i], :]
        above = kv.at[layer, rows_at(core * tok + GRID_W * i, GRID_W, GRID_W), :]
        below = kv.at[layer, rows_at(512 + core * tok + GRID_W * i, GRID_W, GRID_W), :]
        to_first = sp == 1
        to_last = sp == n_sp - 2
        at_first = sp == 0
        at_last = sp == n_sp - 1
        low = core == 0
        high = core == 1
        if i == 0:
            down_same, down_same_got = not_first, not_last
        else:
            down_same, down_same_got = to_first, at_first
        plan = (
            (above, up, tp, not_last, not_first),
            (below, down, tp, down_same, down_same_got),
            (
                above,
                up,
                mate,
                not_last & (high | to_last),
                not_first & (low | at_last),
            ),
            (
                below,
                down,
                mate,
                not_first & (low | to_first),
                not_last & (high | at_first),
            ),
        )
        copies = []
        for n, (spot, z, t, sent, got) in enumerate(plan):
            copy = pltpu.make_async_remote_copy(
                src_ref=mine,
                dst_ref=spot,
                send_sem=h_s.at[layer, i, n + 1],
                recv_sem=h_r.at[layer, i, n + 1],
                device_id={"sp": z, "tp": t},
                device_id_type=MESH,
            )
            copies.append((copy, sent, got))
        return mine, copies

    def arrive(coming, slot):
        for copy in coming.pop(slot, ()):
            copy.wait_recv()

    def hand_on(array, spot, coming, s_sems, r_sems, i):
        for came, far, there in HAND[i]:
            arrive(coming, came)
            coming[there] = [
                send(
                    array.at[came, spot, :],
                    array.at[there, spot, :],
                    s_sems.at[i, there],
                    r_sems.at[i, there],
                    peer(far),
                )
            ]

    conditional = []
    x_gather = first_gather
    for layer in range(layers):
        queries = []
        mates = []
        halos = []
        for i in range(2):
            spot = pl.ds(GRID_W * i, GRID_W)
            hand_on(xs.at[layer], spot, x_gather[i], x_s.at[layer], x_r.at[layer], i)
        for i in range(2):
            spot = slice(GRID_W * i, GRID_W * (i + 1))
            made = None
            squares = None
            for j in (0,) + ARRIVE:
                if layer == 0 and i == 0 and j == 0:
                    own_x[1].wait()
                arrive(x_gather[i], j)
                block = xs[layer, j, spot]
                wide = block.astype(jnp.float32)
                square = wide * wide
                part = lax.dot_general(
                    block,
                    wg[layer, j],
                    (((1,), (1,)), ((), ())),
                    preferred_element_type=jnp.float32,
                )
                made = part if made is None else made + part
                squares = square if squares is None else squares + square
            mean = jnp.sum(squares, axis=1, keepdims=True) * (1.0 / (feat * chips))
            normed = made * lax.rsqrt(mean + EPS)
            queries.append(normed[:, 0:128].astype(jnp.bfloat16))
            kv[layer, places[i], :] = normed[:, 128:384].astype(jnp.bfloat16)
            mine, copies = halo_copies(layer, i)
            mates.append(send(mine, mine, h_s.at[layer, i, 0], h_r.at[layer, i, 0], {"tp": mate}))
            for copy, sent, _ in copies:

                @pl.when(sent)
                def _(copy=copy):
                    copy.start()

            halos += copies
            conditional += copies
        if layer == 0:
            for other in range(2, layers):
                scale_layer(other)
        for copy in mates:
            copy.wait_recv()
        for copy, _, got in halos:

            @pl.when(got)
            def _(copy=copy):
                copy.wait_recv()

        gather = [{}, {}]
        x_gather = [{}, {}]
        for i in range(2):
            spot = pl.ds(GRID_W * i, GRID_W)
            outs = []
            for head in range(2):
                pick = lane_low if head == 1 else jnp.logical_not(lane_low)
                query = jnp.where(pick, queries[i], 0)
                pairs = kv[
                    layer,
                    rows_at(starts[i] * GRID_W, ROW_SPAN * GRID_W, GRID_W),
                    128 * head : 128 * head + 128,
                ]
                scores = lax.dot_general(
                    query, pairs, (((1,), (1,)), ((), ())), preferred_element_type=jnp.float32
                )
                scores = scores + bias[layer, head, i]
                peak = jnp.max(scores, axis=1, keepdims=True)
                lifted = jnp.exp(scores - peak)
                total = jnp.sum(lifted, axis=1, keepdims=True)
                mixed = jnp.dot(
                    lifted.astype(jnp.bfloat16), pairs, preferred_element_type=jnp.float32
                )
                outs.append(mixed / total)
            both = jnp.where(lane_low, outs[0], outs[1])
            atts[layer, 0, spot, :] = both.astype(jnp.bfloat16)
            for j in ORDER:
                copy = send(
                    atts.at[layer, 0, spot, :],
                    atts.at[layer, j, spot, :],
                    a_s.at[layer, i, j],
                    a_r.at[layer, i, j],
                    peer(j),
                )
                gather[i][j] = [copy]
        for i in range(2):
            spot = pl.ds(GRID_W * i, GRID_W)
            hand_on(atts.at[layer], spot, gather[i], a_s.at[layer], a_r.at[layer], i)

        own_o[layer].wait()
        o_mate[layer].wait_recv()
        last = []
        for i in range(2):
            spot = pl.ds(GRID_W * i, GRID_W)
            stream = xs[layer, 0, spot].astype(jnp.float32)
            for j in (0,) + ARRIVE:
                arrive(gather[i], j)
                source = lax.rem(chip - j + chips, chips)
                stream = stream + jnp.dot(
                    atts[layer, j, spot],
                    wout[layer, rows_at(source * 128, 128, 128), :],
                    preferred_element_type=jnp.float32,
                )
            final = stream.astype(jnp.bfloat16)
            if layer + 1 < layers:
                xs[layer + 1, 0, spot, :] = final
                for j in ORDER:
                    copy = send(
                        xs.at[layer + 1, 0, spot, :],
                        xs.at[layer + 1, j, spot, :],
                        x_s.at[layer + 1, i, j],
                        x_r.at[layer + 1, i, j],
                        peer(j),
                    )
                    x_gather[i][j] = [copy]
            else:
                swap = core == 0
                last_half[spot, :] = jnp.where(swap, final[:, half:feat], final[:, 0:half])
                place = rows_at(core * tok + GRID_W * i, GRID_W, GRID_W)
                last.append(
                    send(
                        last_half.at[spot, :],
                        out_ref.at[place, :],
                        d2d_s.at[sem],
                        d2d_r.at[sem],
                        {"tp": mate},
                    )
                )
                sem += 1
                out_ref[place, :] = jnp.where(swap, final[:, 0:half], final[:, half:feat])
        for copy in last:
            copy.wait_recv()
    for copy, sent, _ in conditional:

        @pl.when(sent)
        def _(copy=copy):
            copy.wait_send()

    for copy in sends:
        copy.wait_send()


def body(hidden_in, norm_gain, query_weight, key_weight, value_weight, output_weight, offset_bias):
    n_sp = lax.axis_size("sp")
    n_tp = lax.axis_size("tp")
    chips = n_tp // 2
    layers = norm_gain.shape[0]
    width = norm_gain.shape[1]
    tokens, _ = hidden_in.shape
    tok = tokens // 2
    feat = width // chips
    any_space = pl.BlockSpec(memory_space=pltpu.HBM)
    vmem = pl.BlockSpec(memory_space=pltpu.VMEM)
    dma = pltpu.SemaphoreType.DMA
    bf16 = jnp.bfloat16
    table = offset_bias.transpose(0, 2, 1, 3)
    return pl.pallas_call(
        functools.partial(kernel, n_sp, n_tp, layers),
        out_shape=jax.ShapeDtypeStruct(hidden_in.shape, bf16),
        in_specs=[any_space] * 7,
        out_specs=vmem,
        scratch_shapes=[
            pltpu.VMEM(norm_gain.shape, jnp.float32),
            pltpu.VMEM(table.shape, jnp.float32),
            pltpu.VMEM((tokens, feat // 2), bf16),
            pltpu.VMEM((tok, feat // 2), bf16),
            pltpu.VMEM((layers, chips, tok, feat), bf16),
            pltpu.VMEM((layers, chips, tok, 128), bf16),
            pltpu.VMEM((layers, 768, 256), bf16),
            pltpu.VMEM((layers, 384, width), bf16),
            pltpu.VMEM((layers, chips, 384, feat), bf16),
            pltpu.VMEM((layers, 1024, feat), bf16),
            pltpu.VMEM((3, layers, 16, 128), jnp.float32),
            pltpu.VMEM((layers, 2, 2, GRID_W, ROW_SPAN * GRID_W), jnp.float32),
            dma((layers, 3)),
            dma((layers,)),
            dma((4,)),
            dma((4 + 4 * layers,)),
            dma((4 + 4 * layers,)),
            dma((2, 2, chips)),
            dma((2, 2, chips)),
            dma((layers, 2, chips)),
            dma((layers, 2, chips)),
            dma((layers, 2, chips)),
            dma((layers, 2, chips)),
            dma((layers, 2, 5)),
            dma((layers, 2, 5)),
        ],
        compiler_params=pltpu.CompilerParams(
            collective_id=0, has_side_effects=True, vmem_limit_bytes=67043328
        ),
        name="layers",
    )(hidden_in, norm_gain, query_weight, key_weight, value_weight, output_weight, table)


def solution(mesh):
    return jax.shard_map(
        body,
        mesh=mesh,
        in_specs=(
            P(("grp", "sp"), "tp"),
            P(),
            P(None, "tp", None),
            P(None, "tp", None),
            P(None, "tp", None),
            P(None, None, "tp"),
            P(None, "tp", None, None),
        ),
        out_specs=P(("grp", "sp"), "tp"),
        check_vma=False,
    )
```

```python
import functools

import jax
import jax.numpy as jnp
from jax import lax
from jax.experimental import pallas as pl
from jax.experimental.pallas import tpu as pltpu
from jax.sharding import PartitionSpec as P

HEAD_DIM = 64
GRID_W = 64
ROW_SPAN = 8
COL_SPAN = 16
EPS = 1e-06
NEG = -1e30
MESH = pl.DeviceIdType.MESH
ORDER = (2, 6, 1, 7)
ARRIVE = (1, 7, 2, 6, 3, 5, 4)
HALF = GRID_W // 2
HAND = (
    (2, 2, 4, (0, HALF), 4),
    (2, 1, 3, (0, GRID_W), 3),
    (6, -2, 4, (HALF, HALF), 0),
    (6, -1, 5, (0, GRID_W), 5),
)


def kernel(
    n_sp,
    n_tp,
    layers,
    hid_ref,
    gain_hbm,
    wq_ref,
    wk_ref,
    wv_ref,
    wo_ref,
    ob_hbm,
    out_ref,
    gain_ref,
    ob_ref,
    xst,
    last_half,
    xs,
    atts,
    kv,
    wraw,
    wg,
    wout,
    tab,
    bias,
    own_w_sem,
    own_o_sem,
    own_x_sem,
    d2d_s,
    d2d_r,
    f_s,
    f_r,
    x_s,
    x_r,
    a_s,
    a_r,
    h_s,
    h_r,
):
    chips = n_tp // 2
    tok = xs.shape[2]
    feat = xs.shape[3]
    half = feat // 2
    tp = lax.axis_index("tp")
    sp = lax.axis_index("sp")
    core = lax.rem(tp, 2)
    chip = lax.div(tp, 2)
    mate = tp + 1 - 2 * core
    up = lax.rem(sp + 1, n_sp)
    down = lax.rem(sp + n_sp - 1, n_sp)

    def peer(j):
        return {"tp": lax.rem(tp + 2 * j + n_tp, n_tp)}

    def rows_at(start, size, align):
        return pl.ds(pl.multiple_of(start, align), size)

    greet = [peer(j) for j in ORDER] + [{"tp": mate}]
    greet += [{"tp": lax.rem(mate + 2 * j, n_tp)} for j in ORDER]
    greet += [{"sp": z, "tp": t} for z in (up, down) for t in (tp, mate)]
    barrier = pltpu.get_barrier_semaphore()
    for device in greet:
        pl.semaphore_signal(barrier, inc=1, device_id=device, device_id_type=MESH)

    my_lanes = rows_at(core * half, half, half)
    own_x = [
        pltpu.make_async_copy(hid_ref, xst, own_x_sem.at[0]),
        pltpu.make_async_copy(
            hid_ref.at[rows_at(core * tok, tok, tok), :], xs.at[0, 0, :, my_lanes], own_x_sem.at[1]
        ),
    ]
    own_g = pltpu.make_async_copy(gain_hbm, gain_ref, own_x_sem.at[2])
    own_b = pltpu.make_async_copy(ob_hbm, ob_ref, own_x_sem.at[3])
    for copy in own_x + [own_b, own_g]:
        copy.start()
    w_rows = (
        rows_at(HEAD_DIM * (1 - core), HEAD_DIM, HEAD_DIM),
        rows_at(192 + 64 * core, HEAD_DIM, HEAD_DIM),
        rows_at(128 + 192 * core, HEAD_DIM, HEAD_DIM),
    )
    own_w = []
    own_o = []
    for layer in range(layers):
        for i, w_ref in enumerate((wq_ref, wk_ref, wv_ref)):
            copy = pltpu.make_async_copy(
                w_ref.at[layer], wraw.at[layer, w_rows[i], :], own_w_sem.at[layer, i]
            )
            copy.start()
            own_w.append(copy)
    for layer in range(layers):
        copy = pltpu.make_async_copy(
            wo_ref.at[layer], wout.at[layer, :, my_lanes], own_o_sem.at[layer]
        )
        copy.start()
        own_o.append(copy)

    tab[1] = jnp.zeros(tab.shape[1:], jnp.float32)
    own_b.wait()
    for layer in range(layers):
        for line in range(2 * ROW_SPAN - 1):
            tab[1, layer, line : line + 1, 0:31] = ob_ref[layer, line]
    for layer in range(layers):
        raw = tab[1, layer]
        low = pltpu.roll(raw, 128 - 15, 1)
        high = pltpu.roll(pltpu.roll(raw, 64 - 15, 1), 15, 0)
        tab[0, layer] = low + high

    pl.semaphore_wait(barrier, len(greet))

    sends = []

    def send(src, dst, s_sem, r_sem, device):
        copy = pltpu.make_async_remote_copy(
            src_ref=src,
            dst_ref=dst,
            send_sem=s_sem,
            recv_sem=r_sem,
            device_id=device,
            device_id_type=MESH,
        )
        copy.start()
        sends.append(copy)
        return copy

    own_x[0].wait()
    first_gather = [{}, {}]
    for i in range(2):
        spot = pl.ds(GRID_W * i, GRID_W)
        given = xst.at[rows_at((1 - core) * tok + GRID_W * i, GRID_W, GRID_W), :]
        kept = xst.at[rows_at(core * tok + GRID_W * i, GRID_W, GRID_W), :]
        for j in ORDER + (0,):
            far = (2 * j + 1 - 2 * core + n_tp) if j else (1 - 2 * core + n_tp)
            there = xs.at[0, j, spot, my_lanes]
            pair = []
            if j:
                pair.append(send(kept, there, f_s.at[i, 0, j], f_r.at[i, 0, j], peer(j)))
            device = {"tp": lax.rem(tp + far, n_tp)}
            pair.append(send(given, there, f_s.at[i, 1, j], f_r.at[i, 1, j], device))
            first_gather[i][j] = pair
    t_mate = send(tab.at[0], tab.at[2], d2d_s.at[1], d2d_r.at[1], {"tp": mate})
    w_mate = []
    sem = 2
    for layer in range(layers):
        for i, w_ref in enumerate((wq_ref, wk_ref, wv_ref)):
            w_mate.append(
                send(
                    w_ref.at[layer],
                    wraw.at[layer, w_rows[i], :],
                    d2d_s.at[sem],
                    d2d_r.at[sem],
                    {"tp": mate},
                )
            )
            sem += 1
    o_mate = []
    for layer in range(layers):
        o_mate.append(
            send(
                wo_ref.at[layer],
                wout.at[layer, :, my_lanes],
                d2d_s.at[sem],
                d2d_r.at[sem],
                {"tp": mate},
            )
        )
        sem += 1

    def scale_layer(layer):
        for copy in own_w[3 * layer : 3 * layer + 3]:
            copy.wait()
        for copy in w_mate[3 * layer : 3 * layer + 3]:
            copy.wait_recv()

        def one(j, carry):
            source = lax.rem(chip - j + chips, chips)
            lanes = rows_at(source * feat, feat, feat)
            gain = gain_ref[pl.ds(layer, 1), lanes]
            scale = HEAD_DIM ** (-0.5)
            wg[layer, j, 0:128, :] = (
                wraw[layer, 0:128, lanes].astype(jnp.float32) * (gain * scale)
            ).astype(jnp.bfloat16)
            wg[layer, j, 128:384, :] = (
                wraw[layer, 128:384, lanes].astype(jnp.float32) * gain
            ).astype(jnp.bfloat16)
            return carry

        lax.fori_loop(0, chips, one, 0)

    all_rows = n_sp * 4
    starts = []
    offsets = []
    for i in range(2):
        row = sp * 4 + core * 2 + i
        first = jnp.clip(row - ROW_SPAN // 2, 0, all_rows - ROW_SPAN)
        starts.append(first - sp * 4 + 4)
        offsets.append(first - row + ROW_SPAN - 1)

    def make_bias():
        t_mate.wait_recv()
        lane = lax.broadcasted_iota(jnp.int32, (GRID_W, 128), 1)
        key_col = jnp.where(lane < GRID_W, lane, lane - GRID_W)
        query_col = lax.broadcasted_iota(jnp.int32, (GRID_W, 128), 0)
        window = jnp.clip(query_col - COL_SPAN // 2, 0, GRID_W - COL_SPAN)
        inside = (key_col >= window) & (key_col < window + COL_SPAN)

        def one(layer, carry):
            for head in range(2):
                which = jnp.where(core == head, 0, 2)
                for i in range(2):
                    for pair in range(4):
                        line = tab[which, layer, pl.ds(offsets[i] + 2 * pair, 1), :]
                        wide = jnp.broadcast_to(line, (GRID_W, 128))
                        rolled = pltpu.roll(wide, 0, 1, stride=1, stride_axis=0)
                        bias[layer, head, i, :, 128 * pair : 128 * pair + 128] = jnp.where(
                            inside, rolled, NEG
                        )
            return carry

        lax.fori_loop(0, layers, one, 0)

    own_g.wait()
    scale_layer(0)
    make_bias()
    scale_layer(1)

    lane_low = lax.broadcasted_iota(jnp.int32, (GRID_W, 128), 1) < HEAD_DIM
    not_last = sp < n_sp - 1
    not_first = sp > 0
    places = [rows_at(256 + core * tok + GRID_W * i, GRID_W, GRID_W) for i in range(2)]

    def halo_copies(layer, i):
        mine = kv.at[layer, places[i], :]
        above = kv.at[layer, rows_at(core * tok + GRID_W * i, GRID_W, GRID_W), :]
        below = kv.at[layer, rows_at(512 + core * tok + GRID_W * i, GRID_W, GRID_W), :]
        to_first = sp == 1
        to_last = sp == n_sp - 2
        at_first = sp == 0
        at_last = sp == n_sp - 1
        low = core == 0
        high = core == 1
        if i == 0:
            down_same, down_same_got = not_first, not_last
        else:
            down_same, down_same_got = to_first, at_first
        plan = (
            (above, up, tp, not_last, not_first),
            (below, down, tp, down_same, down_same_got),
            (
                above,
                up,
                mate,
                not_last & (high | to_last),
                not_first & (low | at_last),
            ),
            (
                below,
                down,
                mate,
                not_first & (low | to_first),
                not_last & (high | at_first),
            ),
        )
        copies = []
        for n, (spot, z, t, sent, got) in enumerate(plan):
            copy = pltpu.make_async_remote_copy(
                src_ref=mine,
                dst_ref=spot,
                send_sem=h_s.at[layer, i, n + 1],
                recv_sem=h_r.at[layer, i, n + 1],
                device_id={"sp": z, "tp": t},
                device_id_type=MESH,
            )
            copies.append((copy, sent, got))
        return mine, copies

    def arrive(coming, slot):
        for copy in coming.pop(slot, ()):
            copy.wait_recv()

    def hand_on(array, row, coming, s_sems, r_sems):
        for came, far, there, (first, size), sem in HAND:
            arrive(coming, came)
            spot = pl.ds(GRID_W * row + first, size)
            copy = send(
                array.at[came, spot, :],
                array.at[there, spot, :],
                s_sems.at[row, sem],
                r_sems.at[row, sem],
                peer(far),
            )
            coming.setdefault(there, []).append(copy)

    conditional = []
    x_gather = first_gather
    for layer in range(layers):
        queries = []
        mates = []
        halos = []
        for i in range(2):
            hand_on(xs.at[layer], i, x_gather[i], x_s.at[layer], x_r.at[layer])
        for i in range(2):
            spot = slice(GRID_W * i, GRID_W * (i + 1))
            made = None
            squares = None
            for j in (0,) + ARRIVE:
                if layer == 0 and i == 0 and j == 0:
                    own_x[1].wait()
                arrive(x_gather[i], j)
                block = xs[layer, j, spot]
                wide = block.astype(jnp.float32)
                square = wide * wide
                part = lax.dot_general(
                    block,
                    wg[layer, j],
                    (((1,), (1,)), ((), ())),
                    preferred_element_type=jnp.float32,
                )
                made = part if made is None else made + part
                squares = square if squares is None else squares + square
            mean = jnp.sum(squares, axis=1, keepdims=True) * (1.0 / (feat * chips))
            normed = made * lax.rsqrt(mean + EPS)
            queries.append(normed[:, 0:128].astype(jnp.bfloat16))
            kv[layer, places[i], :] = normed[:, 128:384].astype(jnp.bfloat16)
            mine, copies = halo_copies(layer, i)
            mates.append(send(mine, mine, h_s.at[layer, i, 0], h_r.at[layer, i, 0], {"tp": mate}))
            for copy, sent, _ in copies:

                @pl.when(sent)
                def _(copy=copy):
                    copy.start()

            halos += copies
            conditional += copies
        if layer == 0:
            for other in range(2, layers):
                scale_layer(other)
        for copy in mates:
            copy.wait_recv()
        for copy, _, got in halos:

            @pl.when(got)
            def _(copy=copy):
                copy.wait_recv()

        gather = [{}, {}]
        x_gather = [{}, {}]
        for i in range(2):
            spot = pl.ds(GRID_W * i, GRID_W)
            outs = []
            for head in range(2):
                pick = lane_low if head == 1 else jnp.logical_not(lane_low)
                query = jnp.where(pick, queries[i], 0)
                pairs = kv[
                    layer,
                    rows_at(starts[i] * GRID_W, ROW_SPAN * GRID_W, GRID_W),
                    128 * head : 128 * head + 128,
                ]
                scores = lax.dot_general(
                    query, pairs, (((1,), (1,)), ((), ())), preferred_element_type=jnp.float32
                )
                scores = scores + bias[layer, head, i]
                peak = jnp.max(scores, axis=1, keepdims=True)
                lifted = jnp.exp(scores - peak)
                total = jnp.sum(lifted, axis=1, keepdims=True)
                mixed = jnp.dot(
                    lifted.astype(jnp.bfloat16), pairs, preferred_element_type=jnp.float32
                )
                outs.append(mixed / total)
            both = jnp.where(lane_low, outs[0], outs[1])
            atts[layer, 0, spot, :] = both.astype(jnp.bfloat16)
            for j in ORDER:
                copy = send(
                    atts.at[layer, 0, spot, :],
                    atts.at[layer, j, spot, :],
                    a_s.at[layer, i, j],
                    a_r.at[layer, i, j],
                    peer(j),
                )
                gather[i][j] = [copy]
        before = list(sends[: -2 * len(ORDER)])
        del sends[: len(before)]
        for i in range(2):
            hand_on(atts.at[layer], i, gather[i], a_s.at[layer], a_r.at[layer])
        for copy in before:
            copy.wait_send()

        own_o[layer].wait()
        o_mate[layer].wait_recv()
        last = []
        for i in range(2):
            spot = pl.ds(GRID_W * i, GRID_W)
            stream = xs[layer, 0, spot].astype(jnp.float32)
            for j in (0,) + ARRIVE:
                arrive(gather[i], j)
                source = lax.rem(chip - j + chips, chips)
                stream = stream + jnp.dot(
                    atts[layer, j, spot],
                    wout[layer, rows_at(source * 128, 128, 128), :],
                    preferred_element_type=jnp.float32,
                )
            final = stream.astype(jnp.bfloat16)
            if layer + 1 < layers:
                xs[layer + 1, 0, spot, :] = final
                for j in ORDER:
                    copy = send(
                        xs.at[layer + 1, 0, spot, :],
                        xs.at[layer + 1, j, spot, :],
                        x_s.at[layer + 1, i, j],
                        x_r.at[layer + 1, i, j],
                        peer(j),
                    )
                    x_gather[i][j] = [copy]
            else:
                swap = core == 0
                last_half[spot, :] = jnp.where(swap, final[:, half:feat], final[:, 0:half])
                place = rows_at(core * tok + GRID_W * i, GRID_W, GRID_W)
                last.append(
                    send(
                        last_half.at[spot, :],
                        out_ref.at[place, :],
                        d2d_s.at[sem],
                        d2d_r.at[sem],
                        {"tp": mate},
                    )
                )
                sem += 1
                out_ref[place, :] = jnp.where(swap, final[:, 0:half], final[:, half:feat])
        for copy in last:
            copy.wait_recv()
    for copy, sent, _ in conditional:

        @pl.when(sent)
        def _(copy=copy):
            copy.wait_send()

    for copy in sends:
        copy.wait_send()


def body(hidden_in, norm_gain, query_weight, key_weight, value_weight, output_weight, offset_bias):
    n_sp = lax.axis_size("sp")
    n_tp = lax.axis_size("tp")
    chips = n_tp // 2
    layers = norm_gain.shape[0]
    width = norm_gain.shape[1]
    tokens, _ = hidden_in.shape
    tok = tokens // 2
    feat = width // chips
    any_space = pl.BlockSpec(memory_space=pltpu.HBM)
    vmem = pl.BlockSpec(memory_space=pltpu.VMEM)
    dma = pltpu.SemaphoreType.DMA
    bf16 = jnp.bfloat16
    table = offset_bias.transpose(0, 2, 1, 3)
    return pl.pallas_call(
        functools.partial(kernel, n_sp, n_tp, layers),
        out_shape=jax.ShapeDtypeStruct(hidden_in.shape, bf16),
        in_specs=[any_space] * 7,
        out_specs=vmem,
        scratch_shapes=[
            pltpu.VMEM(norm_gain.shape, jnp.float32),
            pltpu.VMEM(table.shape, jnp.float32),
            pltpu.VMEM((tokens, feat // 2), bf16),
            pltpu.VMEM((tok, feat // 2), bf16),
            pltpu.VMEM((layers, chips, tok, feat), bf16),
            pltpu.VMEM((layers, chips, tok, 128), bf16),
            pltpu.VMEM((layers, 768, 256), bf16),
            pltpu.VMEM((layers, 384, width), bf16),
            pltpu.VMEM((layers, chips, 384, feat), bf16),
            pltpu.VMEM((layers, 1024, feat), bf16),
            pltpu.VMEM((3, layers, 16, 128), jnp.float32),
            pltpu.VMEM((layers, 2, 2, GRID_W, ROW_SPAN * GRID_W), jnp.float32),
            dma((layers, 3)),
            dma((layers,)),
            dma((4,)),
            dma((4 + 4 * layers,)),
            dma((4 + 4 * layers,)),
            dma((2, 2, chips)),
            dma((2, 2, chips)),
            dma((layers, 2, chips)),
            dma((layers, 2, chips)),
            dma((layers, 2, chips)),
            dma((layers, 2, chips)),
            dma((layers, 2, 5)),
            dma((layers, 2, 5)),
        ],
        compiler_params=pltpu.CompilerParams(
            collective_id=0, has_side_effects=True, vmem_limit_bytes=67043328
        ),
        name="layers",
    )(hidden_in, norm_gain, query_weight, key_weight, value_weight, output_weight, table)


def solution(mesh):
    return jax.shard_map(
        body,
        mesh=mesh,
        in_specs=(
            P(("grp", "sp"), "tp"),
            P(),
            P(None, "tp", None),
            P(None, "tp", None),
            P(None, "tp", None),
            P(None, None, "tp"),
            P(None, "tp", None, None),
        ),
        out_specs=P(("grp", "sp"), "tp"),
        check_vma=False,
    )
```

```python
import functools

import jax
import jax.numpy as jnp
from jax import lax
from jax.experimental import pallas as pl
from jax.experimental.pallas import tpu as pltpu
from jax.sharding import PartitionSpec as P

HEAD_DIM = 64
GRID_W = 64
ROW_SPAN = 8
COL_SPAN = 16
EPS = 1e-06
NEG = -1e30
MESH = pl.DeviceIdType.MESH
ORDER = (2, 6, 1, 7)
ARRIVE = (1, 7, 2, 6, 3, 5, 4)
HALF = GRID_W // 2
HAND = (
    (2, 2, 4, (0, HALF), 4),
    (2, 1, 3, (0, GRID_W), 3),
    (6, -2, 4, (HALF, HALF), 0),
    (6, -1, 5, (0, GRID_W), 5),
)


def kernel(
    n_sp,
    n_tp,
    layers,
    hid_ref,
    gain_hbm,
    wq_ref,
    wk_ref,
    wv_ref,
    wo_ref,
    ob_hbm,
    out_ref,
    gain_ref,
    ob_ref,
    xst,
    last_half,
    kept_half,
    xs,
    atts,
    kv,
    wraw,
    wg,
    wout,
    tab,
    bias,
    own_w_sem,
    own_o_sem,
    own_x_sem,
    d2d_s,
    d2d_r,
    f_s,
    f_r,
    x_s,
    x_r,
    a_s,
    a_r,
    h_s,
    h_r,
):
    chips = n_tp // 2
    tok = xs.shape[2]
    feat = xs.shape[3]
    half = feat // 2
    tp = lax.axis_index("tp")
    sp = lax.axis_index("sp")
    core = lax.rem(tp, 2)
    chip = lax.div(tp, 2)
    mate = tp + 1 - 2 * core
    up = lax.rem(sp + 1, n_sp)
    down = lax.rem(sp + n_sp - 1, n_sp)

    def peer(j):
        return {"tp": lax.rem(tp + 2 * j + n_tp, n_tp)}

    def rows_at(start, size, align):
        return pl.ds(pl.multiple_of(start, align), size)

    greet = [peer(j) for j in ORDER] + [{"tp": mate}]
    greet += [{"tp": lax.rem(mate + 2 * j, n_tp)} for j in ORDER]
    greet += [{"sp": z, "tp": t} for z in (up, down) for t in (tp, mate)]
    barrier = pltpu.get_barrier_semaphore()
    for device in greet:
        pl.semaphore_signal(barrier, inc=1, device_id=device, device_id_type=MESH)

    my_lanes = rows_at(core * half, half, half)
    own_x = [
        pltpu.make_async_copy(hid_ref, xst, own_x_sem.at[0]),
        pltpu.make_async_copy(
            hid_ref.at[rows_at(core * tok, tok, tok), :], xs.at[0, 0, :, my_lanes], own_x_sem.at[1]
        ),
    ]
    own_g = pltpu.make_async_copy(gain_hbm, gain_ref, own_x_sem.at[2])
    own_b = pltpu.make_async_copy(ob_hbm, ob_ref, own_x_sem.at[3])
    for copy in own_x + [own_b, own_g]:
        copy.start()
    w_rows = (
        rows_at(HEAD_DIM * (1 - core), HEAD_DIM, HEAD_DIM),
        rows_at(192 + 64 * core, HEAD_DIM, HEAD_DIM),
        rows_at(128 + 192 * core, HEAD_DIM, HEAD_DIM),
    )
    own_w = []
    own_o = []
    for layer in range(layers):
        for i, w_ref in enumerate((wq_ref, wk_ref, wv_ref)):
            copy = pltpu.make_async_copy(
                w_ref.at[layer], wraw.at[layer, w_rows[i], :], own_w_sem.at[layer, i]
            )
            copy.start()
            own_w.append(copy)
    for layer in range(layers):
        copy = pltpu.make_async_copy(
            wo_ref.at[layer], wout.at[layer, :, my_lanes], own_o_sem.at[layer]
        )
        copy.start()
        own_o.append(copy)

    tab[1] = jnp.zeros(tab.shape[1:], jnp.float32)
    own_b.wait()
    for layer in range(layers):
        for line in range(2 * ROW_SPAN - 1):
            tab[1, layer, line : line + 1, 0:31] = ob_ref[layer, line]
    for layer in range(layers):
        raw = tab[1, layer]
        low = pltpu.roll(raw, 128 - 15, 1)
        high = pltpu.roll(pltpu.roll(raw, 64 - 15, 1), 15, 0)
        tab[0, layer] = low + high

    pl.semaphore_wait(barrier, len(greet))

    sends = []

    def send(src, dst, s_sem, r_sem, device):
        copy = pltpu.make_async_remote_copy(
            src_ref=src,
            dst_ref=dst,
            send_sem=s_sem,
            recv_sem=r_sem,
            device_id=device,
            device_id_type=MESH,
        )
        copy.start()
        sends.append(copy)
        return copy

    own_x[0].wait()
    first_gather = [{}, {}]
    for i in range(2):
        spot = pl.ds(GRID_W * i, GRID_W)
        given = xst.at[rows_at((1 - core) * tok + GRID_W * i, GRID_W, GRID_W), :]
        kept = xst.at[rows_at(core * tok + GRID_W * i, GRID_W, GRID_W), :]
        for j in ORDER + (0,):
            far = (2 * j + 1 - 2 * core + n_tp) if j else (1 - 2 * core + n_tp)
            there = xs.at[0, j, spot, my_lanes]
            pair = []
            if j:
                pair.append(send(kept, there, f_s.at[i, 0, j], f_r.at[i, 0, j], peer(j)))
            device = {"tp": lax.rem(tp + far, n_tp)}
            pair.append(send(given, there, f_s.at[i, 1, j], f_r.at[i, 1, j], device))
            first_gather[i][j] = pair
    t_mate = send(tab.at[0], tab.at[2], d2d_s.at[1], d2d_r.at[1], {"tp": mate})
    w_mate = []
    sem = 2
    for layer in range(layers):
        for i, w_ref in enumerate((wq_ref, wk_ref, wv_ref)):
            w_mate.append(
                send(
                    w_ref.at[layer],
                    wraw.at[layer, w_rows[i], :],
                    d2d_s.at[sem],
                    d2d_r.at[sem],
                    {"tp": mate},
                )
            )
            sem += 1
    o_mate = []
    for layer in range(layers):
        o_mate.append(
            send(
                wo_ref.at[layer],
                wout.at[layer, :, my_lanes],
                d2d_s.at[sem],
                d2d_r.at[sem],
                {"tp": mate},
            )
        )
        sem += 1

    def scale_layer(layer):
        for copy in own_w[3 * layer : 3 * layer + 3]:
            copy.wait()
        for copy in w_mate[3 * layer : 3 * layer + 3]:
            copy.wait_recv()

        def one(j, carry):
            source = lax.rem(chip - j + chips, chips)
            lanes = rows_at(source * feat, feat, feat)
            gain = gain_ref[pl.ds(layer, 1), lanes]
            scale = HEAD_DIM ** (-0.5)
            wg[layer, j, 0:128, :] = (
                wraw[layer, 0:128, lanes].astype(jnp.float32) * (gain * scale)
            ).astype(jnp.bfloat16)
            wg[layer, j, 128:384, :] = (
                wraw[layer, 128:384, lanes].astype(jnp.float32) * gain
            ).astype(jnp.bfloat16)
            return carry

        lax.fori_loop(0, chips, one, 0)

    all_rows = n_sp * 4
    starts = []
    offsets = []
    for i in range(2):
        row = sp * 4 + core * 2 + i
        first = jnp.clip(row - ROW_SPAN // 2, 0, all_rows - ROW_SPAN)
        starts.append(first - sp * 4 + 4)
        offsets.append(first - row + ROW_SPAN - 1)

    def make_bias():
        t_mate.wait_recv()
        lane = lax.broadcasted_iota(jnp.int32, (GRID_W, 128), 1)
        key_col = jnp.where(lane < GRID_W, lane, lane - GRID_W)
        query_col = lax.broadcasted_iota(jnp.int32, (GRID_W, 128), 0)
        window = jnp.clip(query_col - COL_SPAN // 2, 0, GRID_W - COL_SPAN)
        inside = (key_col >= window) & (key_col < window + COL_SPAN)

        def one(layer, carry):
            for head in range(2):
                which = jnp.where(core == head, 0, 2)
                for i in range(2):
                    for pair in range(4):
                        line = tab[which, layer, pl.ds(offsets[i] + 2 * pair, 1), :]
                        wide = jnp.broadcast_to(line, (GRID_W, 128))
                        rolled = pltpu.roll(wide, 0, 1, stride=1, stride_axis=0)
                        bias[layer, head, i, :, 128 * pair : 128 * pair + 128] = jnp.where(
                            inside, rolled, NEG
                        )
            return carry

        lax.fori_loop(0, layers, one, 0)


    lane_low = lax.broadcasted_iota(jnp.int32, (GRID_W, 128), 1) < HEAD_DIM
    not_last = sp < n_sp - 1
    not_first = sp > 0
    places = [rows_at(256 + core * tok + GRID_W * i, GRID_W, GRID_W) for i in range(2)]

    def halo_copies(layer, i):
        mine = kv.at[layer, places[i], :]
        above = kv.at[layer, rows_at(core * tok + GRID_W * i, GRID_W, GRID_W), :]
        below = kv.at[layer, rows_at(512 + core * tok + GRID_W * i, GRID_W, GRID_W), :]
        to_first = sp == 1
        to_last = sp == n_sp - 2
        at_first = sp == 0
        at_last = sp == n_sp - 1
        low = core == 0
        high = core == 1
        if i == 0:
            down_same, down_same_got = not_first, not_last
        else:
            down_same, down_same_got = to_first, at_first
        plan = (
            (above, up, tp, not_last, not_first),
            (below, down, tp, down_same, down_same_got),
            (
                above,
                up,
                mate,
                not_last & (high | to_last),
                not_first & (low | at_last),
            ),
            (
                below,
                down,
                mate,
                not_first & (low | to_first),
                not_last & (high | at_first),
            ),
        )
        copies = []
        for n, (spot, z, t, sent, got) in enumerate(plan):
            copy = pltpu.make_async_remote_copy(
                src_ref=mine,
                dst_ref=spot,
                send_sem=h_s.at[layer, i, n + 1],
                recv_sem=h_r.at[layer, i, n + 1],
                device_id={"sp": z, "tp": t},
                device_id_type=MESH,
            )
            copies.append((copy, sent, got))
        return mine, copies

    def arrive(coming, slot):
        for copy in coming.pop(slot, ()):
            copy.wait_recv()

    def hand_on(array, row, coming, s_sems, r_sems):
        for came, far, there, (first, size), sem in HAND:
            arrive(coming, came)
            spot = pl.ds(GRID_W * row + first, size)
            copy = send(
                array.at[came, spot, :],
                array.at[there, spot, :],
                s_sems.at[row, sem],
                r_sems.at[row, sem],
                peer(far),
            )
            coming.setdefault(there, []).append(copy)

    conditional = []
    x_gather = first_gather
    for layer in range(layers):
        queries = []
        mates = []
        halos = []
        for i in range(2):
            hand_on(xs.at[layer], i, x_gather[i], x_s.at[layer], x_r.at[layer])
        if layer == 0:
            own_g.wait()
            own_x[1].wait()
            scale_layer(0)
            make_bias()
            scale_layer(1)
        for i in range(2):
            spot = slice(GRID_W * i, GRID_W * (i + 1))
            made = None
            squares = None
            for j in (0,) + ARRIVE:
                arrive(x_gather[i], j)
                block = xs[layer, j, spot]
                wide = block.astype(jnp.float32)
                square = wide * wide
                part = lax.dot_general(
                    block,
                    wg[layer, j],
                    (((1,), (1,)), ((), ())),
                    preferred_element_type=jnp.float32,
                )
                made = part if made is None else made + part
                squares = square if squares is None else squares + square
            mean = jnp.sum(squares, axis=1, keepdims=True) * (1.0 / (feat * chips))
            normed = made * lax.rsqrt(mean + EPS)
            queries.append(normed[:, 0:128].astype(jnp.bfloat16))
            kv[layer, places[i], :] = normed[:, 128:384].astype(jnp.bfloat16)
            mine, copies = halo_copies(layer, i)
            mates.append(send(mine, mine, h_s.at[layer, i, 0], h_r.at[layer, i, 0], {"tp": mate}))
            for copy, sent, _ in copies:

                @pl.when(sent)
                def _(copy=copy):
                    copy.start()

            halos += copies
            conditional += copies
        if layer == 0:
            for other in range(2, layers):
                scale_layer(other)
        for copy in mates:
            copy.wait_recv()
        for copy, _, got in halos:

            @pl.when(got)
            def _(copy=copy):
                copy.wait_recv()

        gather = [{}, {}]
        x_gather = [{}, {}]
        for i in range(2):
            spot = pl.ds(GRID_W * i, GRID_W)
            outs = []
            for head in range(2):
                pick = lane_low if head == 1 else jnp.logical_not(lane_low)
                query = jnp.where(pick, queries[i], 0)
                pairs = kv[
                    layer,
                    rows_at(starts[i] * GRID_W, ROW_SPAN * GRID_W, GRID_W),
                    128 * head : 128 * head + 128,
                ]
                scores = lax.dot_general(
                    query, pairs, (((1,), (1,)), ((), ())), preferred_element_type=jnp.float32
                )
                scores = scores + bias[layer, head, i]
                peak = jnp.max(scores, axis=1, keepdims=True)
                lifted = jnp.exp(scores - peak)
                total = jnp.sum(lifted, axis=1, keepdims=True)
                mixed = jnp.dot(
                    lifted.astype(jnp.bfloat16), pairs, preferred_element_type=jnp.float32
                )
                outs.append(mixed / total)
            both = jnp.where(lane_low, outs[0], outs[1])
            atts[layer, 0, spot, :] = both.astype(jnp.bfloat16)
            for j in ORDER:
                copy = send(
                    atts.at[layer, 0, spot, :],
                    atts.at[layer, j, spot, :],
                    a_s.at[layer, i, j],
                    a_r.at[layer, i, j],
                    peer(j),
                )
                gather[i][j] = [copy]
        before = list(sends[: -2 * len(ORDER)])
        del sends[: len(before)]
        for i in range(2):
            hand_on(atts.at[layer], i, gather[i], a_s.at[layer], a_r.at[layer])
        for copy in before:
            copy.wait_send()

        own_o[layer].wait()
        o_mate[layer].wait_recv()
        last = []
        kept = []
        for i in range(2):
            spot = pl.ds(GRID_W * i, GRID_W)
            stream = xs[layer, 0, spot].astype(jnp.float32)
            for j in (0,) + ARRIVE:
                arrive(gather[i], j)
                source = lax.rem(chip - j + chips, chips)
                stream = stream + jnp.dot(
                    atts[layer, j, spot],
                    wout[layer, rows_at(source * 128, 128, 128), :],
                    preferred_element_type=jnp.float32,
                )
            final = stream.astype(jnp.bfloat16)
            if layer + 1 < layers:
                xs[layer + 1, 0, spot, :] = final
                for j in ORDER:
                    copy = send(
                        xs.at[layer + 1, 0, spot, :],
                        xs.at[layer + 1, j, spot, :],
                        x_s.at[layer + 1, i, j],
                        x_r.at[layer + 1, i, j],
                        peer(j),
                    )
                    x_gather[i][j] = [copy]
            else:
                swap = core == 0
                last_half[spot, :] = jnp.where(swap, final[:, half:feat], final[:, 0:half])
                place = rows_at(core * tok + GRID_W * i, GRID_W, GRID_W)
                last.append(
                    send(
                        last_half.at[spot, :],
                        out_ref.at[place, :],
                        d2d_s.at[sem],
                        d2d_r.at[sem],
                        {"tp": mate},
                    )
                )
                sem += 1
                kept_half[spot, :] = jnp.where(swap, final[:, 0:half], final[:, half:feat])
                copy = pltpu.make_async_copy(
                    kept_half.at[spot, :], out_ref.at[place, :], own_x_sem.at[4 + i]
                )
                copy.start()
                kept.append(copy)
        for copy in last:
            copy.wait_recv()
        for copy in kept:
            copy.wait()
    for copy, sent, _ in conditional:

        @pl.when(sent)
        def _(copy=copy):
            copy.wait_send()

    for copy in sends:
        copy.wait_send()


def body(hidden_in, norm_gain, query_weight, key_weight, value_weight, output_weight, offset_bias):
    n_sp = lax.axis_size("sp")
    n_tp = lax.axis_size("tp")
    chips = n_tp // 2
    layers = norm_gain.shape[0]
    width = norm_gain.shape[1]
    tokens, _ = hidden_in.shape
    tok = tokens // 2
    feat = width // chips
    any_space = pl.BlockSpec(memory_space=pltpu.HBM)
    dma = pltpu.SemaphoreType.DMA
    bf16 = jnp.bfloat16
    table = offset_bias.transpose(0, 2, 1, 3)
    return pl.pallas_call(
        functools.partial(kernel, n_sp, n_tp, layers),
        out_shape=jax.ShapeDtypeStruct(hidden_in.shape, bf16),
        in_specs=[any_space] * 7,
        out_specs=any_space,
        scratch_shapes=[
            pltpu.VMEM(norm_gain.shape, jnp.float32),
            pltpu.VMEM(table.shape, jnp.float32),
            pltpu.VMEM((tokens, feat // 2), bf16),
            pltpu.VMEM((tok, feat // 2), bf16),
            pltpu.VMEM((tok, feat // 2), bf16),
            pltpu.VMEM((layers, chips, tok, feat), bf16),
            pltpu.VMEM((layers, chips, tok, 128), bf16),
            pltpu.VMEM((layers, 768, 256), bf16),
            pltpu.VMEM((layers, 384, width), bf16),
            pltpu.VMEM((layers, chips, 384, feat), bf16),
            pltpu.VMEM((layers, 1024, feat), bf16),
            pltpu.VMEM((3, layers, 16, 128), jnp.float32),
            pltpu.VMEM((layers, 2, 2, GRID_W, ROW_SPAN * GRID_W), jnp.float32),
            dma((layers, 3)),
            dma((layers,)),
            dma((6,)),
            dma((4 + 4 * layers,)),
            dma((4 + 4 * layers,)),
            dma((2, 2, chips)),
            dma((2, 2, chips)),
            dma((layers, 2, chips)),
            dma((layers, 2, chips)),
            dma((layers, 2, chips)),
            dma((layers, 2, chips)),
            dma((layers, 2, 5)),
            dma((layers, 2, 5)),
        ],
        compiler_params=pltpu.CompilerParams(
            collective_id=0, has_side_effects=True, vmem_limit_bytes=67043328
        ),
        name="layers",
    )(hidden_in, norm_gain, query_weight, key_weight, value_weight, output_weight, table)


def solution(mesh):
    return jax.shard_map(
        body,
        mesh=mesh,
        in_specs=(
            P(("grp", "sp"), "tp"),
            P(),
            P(None, "tp", None),
            P(None, "tp", None),
            P(None, "tp", None),
            P(None, None, "tp"),
            P(None, "tp", None, None),
        ),
        out_specs=P(("grp", "sp"), "tp"),
        check_vma=False,
    )
```

```python
import functools

import jax
import jax.numpy as jnp
from jax import lax
from jax.experimental import pallas as pl
from jax.experimental.pallas import tpu as pltpu
from jax.sharding import PartitionSpec as P

HEAD_DIM = 64
GRID_W = 64
ROW_SPAN = 8
COL_SPAN = 16
EPS = 1e-06
NEG = -1e30
MESH = pl.DeviceIdType.MESH
ORDER = (2, 6, 1, 7)
ARRIVE = (1, 7, 2, 6, 3, 5, 4)
HALF = GRID_W // 2
HAND = (
    (2, 2, 4, (0, HALF), 4),
    (2, 1, 3, (0, GRID_W), 3),
    (6, -2, 4, (HALF, HALF), 0),
    (6, -1, 5, (0, GRID_W), 5),
)


def kernel(
    n_sp,
    n_tp,
    layers,
    hid_ref,
    gain_hbm,
    wq_ref,
    wk_ref,
    wv_ref,
    wo_ref,
    ob_hbm,
    out_ref,
    gain_ref,
    ob_ref,
    xst,
    last_half,
    kept_half,
    xs,
    atts,
    kv,
    wraw,
    wg,
    wout,
    tab,
    bias,
    own_w_sem,
    own_o_sem,
    own_x_sem,
    d2d_s,
    d2d_r,
    f_s,
    f_r,
    x_s,
    x_r,
    a_s,
    a_r,
    h_s,
    h_r,
):
    chips = n_tp // 2
    tok = xs.shape[2]
    feat = xs.shape[3]
    half = feat // 2
    tp = lax.axis_index("tp")
    sp = lax.axis_index("sp")
    core = lax.rem(tp, 2)
    chip = lax.div(tp, 2)
    mate = tp + 1 - 2 * core
    up = lax.rem(sp + 1, n_sp)
    down = lax.rem(sp + n_sp - 1, n_sp)

    def peer(j):
        return {"tp": lax.rem(tp + 2 * j + n_tp, n_tp)}

    def rows_at(start, size, align):
        return pl.ds(pl.multiple_of(start, align), size)

    greet = [peer(j) for j in ORDER] + [{"tp": mate}]
    greet += [{"tp": lax.rem(mate + 2 * j, n_tp)} for j in ORDER]
    greet += [{"sp": z, "tp": t} for z in (up, down) for t in (tp, mate)]
    barrier = pltpu.get_barrier_semaphore()
    for device in greet:
        pl.semaphore_signal(barrier, inc=1, device_id=device, device_id_type=MESH)

    my_lanes = rows_at(core * half, half, half)
    own_x = [
        pltpu.make_async_copy(hid_ref, xst, own_x_sem.at[0]),
        pltpu.make_async_copy(
            hid_ref.at[rows_at(core * tok, tok, tok), :], xs.at[0, 0, :, my_lanes], own_x_sem.at[1]
        ),
    ]
    own_g = pltpu.make_async_copy(gain_hbm, gain_ref, own_x_sem.at[2])
    own_b = pltpu.make_async_copy(ob_hbm, ob_ref, own_x_sem.at[3])
    for copy in own_x + [own_b, own_g]:
        copy.start()
    w_rows = (
        rows_at(HEAD_DIM * (1 - core), HEAD_DIM, HEAD_DIM),
        rows_at(192 + 64 * core, HEAD_DIM, HEAD_DIM),
        rows_at(128 + 192 * core, HEAD_DIM, HEAD_DIM),
    )
    own_w = []
    own_o = []
    for layer in range(layers):
        for i, w_ref in enumerate((wq_ref, wk_ref, wv_ref)):
            copy = pltpu.make_async_copy(
                w_ref.at[layer], wraw.at[layer, w_rows[i], :], own_w_sem.at[layer, i]
            )
            copy.start()
            own_w.append(copy)
    for layer in range(layers):
        copy = pltpu.make_async_copy(
            wo_ref.at[layer], wout.at[layer, :, my_lanes], own_o_sem.at[layer]
        )
        copy.start()
        own_o.append(copy)

    tab[1] = jnp.zeros(tab.shape[1:], jnp.float32)
    own_b.wait()
    for layer in range(layers):
        for line in range(2 * ROW_SPAN - 1):
            tab[1, layer, line : line + 1, 0:31] = ob_ref[layer, line]
    for layer in range(layers):
        raw = tab[1, layer]
        low = pltpu.roll(raw, 128 - 15, 1)
        high = pltpu.roll(pltpu.roll(raw, 64 - 15, 1), 15, 0)
        tab[0, layer] = low + high

    pl.semaphore_wait(barrier, len(greet))

    sends = []

    def send(src, dst, s_sem, r_sem, device):
        copy = pltpu.make_async_remote_copy(
            src_ref=src,
            dst_ref=dst,
            send_sem=s_sem,
            recv_sem=r_sem,
            device_id=device,
            device_id_type=MESH,
        )
        copy.start()
        sends.append(copy)
        return copy

    own_x[0].wait()
    first_gather = [{}, {}]
    for i in range(2):
        spot = pl.ds(GRID_W * i, GRID_W)
        given = xst.at[rows_at((1 - core) * tok + GRID_W * i, GRID_W, GRID_W), :]
        kept = xst.at[rows_at(core * tok + GRID_W * i, GRID_W, GRID_W), :]
        for j in ORDER + (0,):
            far = (2 * j + 1 - 2 * core + n_tp) if j else (1 - 2 * core + n_tp)
            there = xs.at[0, j, spot, my_lanes]
            pair = []
            if j:
                pair.append(send(kept, there, f_s.at[i, 0, j], f_r.at[i, 0, j], peer(j)))
            device = {"tp": lax.rem(tp + far, n_tp)}
            pair.append(send(given, there, f_s.at[i, 1, j], f_r.at[i, 1, j], device))
            first_gather[i][j] = pair
    t_mate = send(tab.at[0], tab.at[2], d2d_s.at[1], d2d_r.at[1], {"tp": mate})
    w_mate = []
    o_mate = []

    def give_weights(layer):
        sem = 2 + 4 * layer
        pairs = [
            (w_ref.at[layer], wraw.at[layer, rows, :])
            for w_ref, rows in zip((wq_ref, wk_ref, wv_ref), w_rows, strict=True)
        ]
        pairs.append((wo_ref.at[layer], wout.at[layer, :, my_lanes]))
        for i, (mine, there) in enumerate(pairs):
            copy = send(mine, there, d2d_s.at[sem + i], d2d_r.at[sem + i], {"tp": mate})
            (w_mate if i < 3 else o_mate).append(copy)

    give_weights(0)

    def scale_layer(layer):
        for copy in own_w[3 * layer : 3 * layer + 3]:
            copy.wait()
        for copy in w_mate[3 * layer : 3 * layer + 3]:
            copy.wait_recv()

        def one(j, carry):
            source = lax.rem(chip - j + chips, chips)
            lanes = rows_at(source * feat, feat, feat)
            gain = gain_ref[pl.ds(layer, 1), lanes]
            scale = HEAD_DIM ** (-0.5)
            wg[layer, j, 0:128, :] = (
                wraw[layer, 0:128, lanes].astype(jnp.float32) * (gain * scale)
            ).astype(jnp.bfloat16)
            wg[layer, j, 128:384, :] = (
                wraw[layer, 128:384, lanes].astype(jnp.float32) * gain
            ).astype(jnp.bfloat16)
            return carry

        lax.fori_loop(0, chips, one, 0)

    all_rows = n_sp * 4
    starts = []
    offsets = []
    for i in range(2):
        row = sp * 4 + core * 2 + i
        first = jnp.clip(row - ROW_SPAN // 2, 0, all_rows - ROW_SPAN)
        starts.append(first - sp * 4 + 4)
        offsets.append(first - row + ROW_SPAN - 1)

    def make_bias():
        t_mate.wait_recv()
        lane = lax.broadcasted_iota(jnp.int32, (GRID_W, 128), 1)
        key_col = jnp.where(lane < GRID_W, lane, lane - GRID_W)
        query_col = lax.broadcasted_iota(jnp.int32, (GRID_W, 128), 0)
        window = jnp.clip(query_col - COL_SPAN // 2, 0, GRID_W - COL_SPAN)
        inside = (key_col >= window) & (key_col < window + COL_SPAN)

        def one(layer, carry):
            for head in range(2):
                which = jnp.where(core == head, 0, 2)
                for i in range(2):
                    for pair in range(4):
                        line = tab[which, layer, pl.ds(offsets[i] + 2 * pair, 1), :]
                        wide = jnp.broadcast_to(line, (GRID_W, 128))
                        rolled = pltpu.roll(wide, 0, 1, stride=1, stride_axis=0)
                        bias[layer, head, i, :, 128 * pair : 128 * pair + 128] = jnp.where(
                            inside, rolled, NEG
                        )
            return carry

        lax.fori_loop(0, layers, one, 0)


    lane_low = lax.broadcasted_iota(jnp.int32, (GRID_W, 128), 1) < HEAD_DIM
    not_last = sp < n_sp - 1
    not_first = sp > 0
    places = [rows_at(256 + core * tok + GRID_W * i, GRID_W, GRID_W) for i in range(2)]

    def halo_copies(layer, i):
        mine = kv.at[layer, places[i], :]
        above = kv.at[layer, rows_at(core * tok + GRID_W * i, GRID_W, GRID_W), :]
        below = kv.at[layer, rows_at(512 + core * tok + GRID_W * i, GRID_W, GRID_W), :]
        to_first = sp == 1
        to_last = sp == n_sp - 2
        at_first = sp == 0
        at_last = sp == n_sp - 1
        low = core == 0
        high = core == 1
        if i == 0:
            down_same, down_same_got = not_first, not_last
        else:
            down_same, down_same_got = to_first, at_first
        plan = (
            (above, up, tp, not_last, not_first),
            (below, down, tp, down_same, down_same_got),
            (
                above,
                up,
                mate,
                not_last & (high | to_last),
                not_first & (low | at_last),
            ),
            (
                below,
                down,
                mate,
                not_first & (low | to_first),
                not_last & (high | at_first),
            ),
        )
        copies = []
        for n, (spot, z, t, sent, got) in enumerate(plan):
            copy = pltpu.make_async_remote_copy(
                src_ref=mine,
                dst_ref=spot,
                send_sem=h_s.at[layer, i, n + 1],
                recv_sem=h_r.at[layer, i, n + 1],
                device_id={"sp": z, "tp": t},
                device_id_type=MESH,
            )
            copies.append((copy, sent, got))
        return mine, copies

    def arrive(coming, slot):
        for copy in coming.pop(slot, ()):
            copy.wait_recv()

    def hand_on(array, row, coming, s_sems, r_sems):
        for came, far, there, (first, size), sem in HAND:
            arrive(coming, came)
            spot = pl.ds(GRID_W * row + first, size)
            copy = send(
                array.at[came, spot, :],
                array.at[there, spot, :],
                s_sems.at[row, sem],
                r_sems.at[row, sem],
                peer(far),
            )
            coming.setdefault(there, []).append(copy)

    conditional = []
    x_gather = first_gather
    for layer in range(layers):
        queries = []
        mates = []
        halos = []
        for i in range(2):
            hand_on(xs.at[layer], i, x_gather[i], x_s.at[layer], x_r.at[layer])
        if layer == 0:
            own_g.wait()
            own_x[1].wait()
            make_bias()
        scale_layer(layer)
        for i in range(2):
            spot = slice(GRID_W * i, GRID_W * (i + 1))
            made = None
            squares = None
            for j in (0,) + ARRIVE:
                arrive(x_gather[i], j)
                block = xs[layer, j, spot]
                wide = block.astype(jnp.float32)
                square = wide * wide
                part = lax.dot_general(
                    block,
                    wg[layer, j],
                    (((1,), (1,)), ((), ())),
                    preferred_element_type=jnp.float32,
                )
                made = part if made is None else made + part
                squares = square if squares is None else squares + square
            mean = jnp.sum(squares, axis=1, keepdims=True) * (1.0 / (feat * chips))
            normed = made * lax.rsqrt(mean + EPS)
            queries.append(normed[:, 0:128].astype(jnp.bfloat16))
            kv[layer, places[i], :] = normed[:, 128:384].astype(jnp.bfloat16)
            mine, copies = halo_copies(layer, i)
            mates.append(send(mine, mine, h_s.at[layer, i, 0], h_r.at[layer, i, 0], {"tp": mate}))
            for copy, sent, _ in copies:

                @pl.when(sent)
                def _(copy=copy):
                    copy.start()

            halos += copies
            conditional += copies
        for copy in mates:
            copy.wait_recv()
        for copy, _, got in halos:

            @pl.when(got)
            def _(copy=copy):
                copy.wait_recv()

        gather = [{}, {}]
        x_gather = [{}, {}]
        for i in range(2):
            spot = pl.ds(GRID_W * i, GRID_W)
            outs = []
            for head in range(2):
                pick = lane_low if head == 1 else jnp.logical_not(lane_low)
                query = jnp.where(pick, queries[i], 0)
                pairs = kv[
                    layer,
                    rows_at(starts[i] * GRID_W, ROW_SPAN * GRID_W, GRID_W),
                    128 * head : 128 * head + 128,
                ]
                scores = lax.dot_general(
                    query, pairs, (((1,), (1,)), ((), ())), preferred_element_type=jnp.float32
                )
                scores = scores + bias[layer, head, i]
                peak = jnp.max(scores, axis=1, keepdims=True)
                lifted = jnp.exp(scores - peak)
                total = jnp.sum(lifted, axis=1, keepdims=True)
                mixed = jnp.dot(
                    lifted.astype(jnp.bfloat16), pairs, preferred_element_type=jnp.float32
                )
                outs.append(mixed / total)
            both = jnp.where(lane_low, outs[0], outs[1])
            atts[layer, 0, spot, :] = both.astype(jnp.bfloat16)
            for j in ORDER:
                copy = send(
                    atts.at[layer, 0, spot, :],
                    atts.at[layer, j, spot, :],
                    a_s.at[layer, i, j],
                    a_r.at[layer, i, j],
                    peer(j),
                )
                gather[i][j] = [copy]
        before = list(sends[: -2 * len(ORDER)])
        del sends[: len(before)]
        for i in range(2):
            hand_on(atts.at[layer], i, gather[i], a_s.at[layer], a_r.at[layer])
        if layer + 1 < layers:
            give_weights(layer + 1)
        for copy in before:
            copy.wait_send()

        own_o[layer].wait()
        o_mate[layer].wait_recv()
        last = []
        kept = []
        for i in range(2):
            spot = pl.ds(GRID_W * i, GRID_W)
            stream = xs[layer, 0, spot].astype(jnp.float32)
            for j in (0,) + ARRIVE:
                arrive(gather[i], j)
                source = lax.rem(chip - j + chips, chips)
                stream = stream + jnp.dot(
                    atts[layer, j, spot],
                    wout[layer, rows_at(source * 128, 128, 128), :],
                    preferred_element_type=jnp.float32,
                )
            final = stream.astype(jnp.bfloat16)
            if layer + 1 < layers:
                xs[layer + 1, 0, spot, :] = final
                for j in ORDER:
                    copy = send(
                        xs.at[layer + 1, 0, spot, :],
                        xs.at[layer + 1, j, spot, :],
                        x_s.at[layer + 1, i, j],
                        x_r.at[layer + 1, i, j],
                        peer(j),
                    )
                    x_gather[i][j] = [copy]
            else:
                swap = core == 0
                last_half[spot, :] = jnp.where(swap, final[:, half:feat], final[:, 0:half])
                place = rows_at(core * tok + GRID_W * i, GRID_W, GRID_W)
                last.append(
                    send(
                        last_half.at[spot, :],
                        out_ref.at[place, :],
                        d2d_s.at[2 + 4 * layers + i],
                        d2d_r.at[2 + 4 * layers + i],
                        {"tp": mate},
                    )
                )
                kept_half[spot, :] = jnp.where(swap, final[:, 0:half], final[:, half:feat])
                copy = pltpu.make_async_copy(
                    kept_half.at[spot, :], out_ref.at[place, :], own_x_sem.at[4 + i]
                )
                copy.start()
                kept.append(copy)
        for copy in last:
            copy.wait_recv()
        for copy in kept:
            copy.wait()
    for copy, sent, _ in conditional:

        @pl.when(sent)
        def _(copy=copy):
            copy.wait_send()

    for copy in sends:
        copy.wait_send()


def body(hidden_in, norm_gain, query_weight, key_weight, value_weight, output_weight, offset_bias):
    n_sp = lax.axis_size("sp")
    n_tp = lax.axis_size("tp")
    chips = n_tp // 2
    layers = norm_gain.shape[0]
    width = norm_gain.shape[1]
    tokens, _ = hidden_in.shape
    tok = tokens // 2
    feat = width // chips
    any_space = pl.BlockSpec(memory_space=pltpu.HBM)
    dma = pltpu.SemaphoreType.DMA
    bf16 = jnp.bfloat16
    table = offset_bias.transpose(0, 2, 1, 3)
    return pl.pallas_call(
        functools.partial(kernel, n_sp, n_tp, layers),
        out_shape=jax.ShapeDtypeStruct(hidden_in.shape, bf16),
        in_specs=[any_space] * 7,
        out_specs=any_space,
        scratch_shapes=[
            pltpu.VMEM(norm_gain.shape, jnp.float32),
            pltpu.VMEM(table.shape, jnp.float32),
            pltpu.VMEM((tokens, feat // 2), bf16),
            pltpu.VMEM((tok, feat // 2), bf16),
            pltpu.VMEM((tok, feat // 2), bf16),
            pltpu.VMEM((layers, chips, tok, feat), bf16),
            pltpu.VMEM((layers, chips, tok, 128), bf16),
            pltpu.VMEM((layers, 768, 256), bf16),
            pltpu.VMEM((layers, 384, width), bf16),
            pltpu.VMEM((layers, chips, 384, feat), bf16),
            pltpu.VMEM((layers, 1024, feat), bf16),
            pltpu.VMEM((3, layers, 16, 128), jnp.float32),
            pltpu.VMEM((layers, 2, 2, GRID_W, ROW_SPAN * GRID_W), jnp.float32),
            dma((layers, 3)),
            dma((layers,)),
            dma((6,)),
            dma((4 + 4 * layers,)),
            dma((4 + 4 * layers,)),
            dma((2, 2, chips)),
            dma((2, 2, chips)),
            dma((layers, 2, chips)),
            dma((layers, 2, chips)),
            dma((layers, 2, chips)),
            dma((layers, 2, chips)),
            dma((layers, 2, 5)),
            dma((layers, 2, 5)),
        ],
        compiler_params=pltpu.CompilerParams(
            collective_id=0, has_side_effects=True, vmem_limit_bytes=67043328
        ),
        name="layers",
    )(hidden_in, norm_gain, query_weight, key_weight, value_weight, output_weight, table)


def solution(mesh):
    return jax.shard_map(
        body,
        mesh=mesh,
        in_specs=(
            P(("grp", "sp"), "tp"),
            P(),
            P(None, "tp", None),
            P(None, "tp", None),
            P(None, "tp", None),
            P(None, None, "tp"),
            P(None, "tp", None, None),
        ),
        out_specs=P(("grp", "sp"), "tp"),
        check_vma=False,
    )
```

```python
import functools

import jax
import jax.numpy as jnp
from jax import lax
from jax.experimental import pallas as pl
from jax.experimental.pallas import tpu as pltpu
from jax.sharding import PartitionSpec as P

HEAD_DIM = 64
GRID_W = 64
ROW_SPAN = 8
COL_SPAN = 16
EPS = 1e-06
NEG = -1e30
MESH = pl.DeviceIdType.MESH
ORDER = (4, 2, 6, 1, 7)
ARRIVE = (1, 7, 2, 6, 3, 5, 4)
HAND = ((2, 1, 3), (6, -1, 5))


def kernel(
    n_sp,
    n_tp,
    layers,
    hid_ref,
    gain_hbm,
    wq_ref,
    wk_ref,
    wv_ref,
    wo_ref,
    ob_hbm,
    out_ref,
    gain_ref,
    ob_ref,
    xst,
    last_half,
    kept_half,
    xs,
    atts,
    kv,
    wraw,
    wg,
    wout,
    tab,
    bias,
    own_w_sem,
    own_o_sem,
    own_x_sem,
    d2d_s,
    d2d_r,
    f_s,
    f_r,
    x_s,
    x_r,
    a_s,
    a_r,
    h_s,
    h_r,
):
    chips = n_tp // 2
    tok = xs.shape[2]
    feat = xs.shape[3]
    half = feat // 2
    tp = lax.axis_index("tp")
    sp = lax.axis_index("sp")
    core = lax.rem(tp, 2)
    chip = lax.div(tp, 2)
    mate = tp + 1 - 2 * core
    up = lax.rem(sp + 1, n_sp)
    down = lax.rem(sp + n_sp - 1, n_sp)

    def peer(j):
        return {"tp": lax.rem(tp + 2 * j + n_tp, n_tp)}

    def rows_at(start, size, align):
        return pl.ds(pl.multiple_of(start, align), size)

    greet = [peer(j) for j in ORDER] + [{"tp": mate}]
    greet += [{"tp": lax.rem(mate + 2 * j, n_tp)} for j in ORDER]
    greet += [{"sp": z, "tp": t} for z in (up, down) for t in (tp, mate)]
    barrier = pltpu.get_barrier_semaphore()
    for device in greet:
        pl.semaphore_signal(barrier, inc=1, device_id=device, device_id_type=MESH)

    my_lanes = rows_at(core * half, half, half)
    own_x = [
        pltpu.make_async_copy(hid_ref, xst, own_x_sem.at[0]),
        pltpu.make_async_copy(
            hid_ref.at[rows_at(core * tok, tok, tok), :], xs.at[0, 0, :, my_lanes], own_x_sem.at[1]
        ),
    ]
    own_g = pltpu.make_async_copy(gain_hbm, gain_ref, own_x_sem.at[2])
    own_b = pltpu.make_async_copy(ob_hbm, ob_ref, own_x_sem.at[3])
    for copy in own_x + [own_b, own_g]:
        copy.start()
    w_rows = (
        rows_at(HEAD_DIM * (1 - core), HEAD_DIM, HEAD_DIM),
        rows_at(192 + 64 * core, HEAD_DIM, HEAD_DIM),
        rows_at(128 + 192 * core, HEAD_DIM, HEAD_DIM),
    )
    own_w = []
    own_o = []
    for layer in range(layers):
        for i, w_ref in enumerate((wq_ref, wk_ref, wv_ref)):
            copy = pltpu.make_async_copy(
                w_ref.at[layer], wraw.at[layer, w_rows[i], :], own_w_sem.at[layer, i]
            )
            copy.start()
            own_w.append(copy)
    for layer in range(layers):
        copy = pltpu.make_async_copy(
            wo_ref.at[layer], wout.at[layer, :, my_lanes], own_o_sem.at[layer]
        )
        copy.start()
        own_o.append(copy)

    tab[1] = jnp.zeros(tab.shape[1:], jnp.float32)
    own_b.wait()
    for layer in range(layers):
        for line in range(2 * ROW_SPAN - 1):
            tab[1, layer, line : line + 1, 0:31] = ob_ref[layer, line]
    for layer in range(layers):
        raw = tab[1, layer]
        low = pltpu.roll(raw, 128 - 15, 1)
        high = pltpu.roll(pltpu.roll(raw, 64 - 15, 1), 15, 0)
        tab[0, layer] = low + high

    pl.semaphore_wait(barrier, len(greet))

    sends = []

    def send(src, dst, s_sem, r_sem, device):
        copy = pltpu.make_async_remote_copy(
            src_ref=src,
            dst_ref=dst,
            send_sem=s_sem,
            recv_sem=r_sem,
            device_id=device,
            device_id_type=MESH,
        )
        copy.start()
        sends.append(copy)
        return copy

    own_x[0].wait()
    first_gather = [{}, {}]
    for i in range(2):
        spot = pl.ds(GRID_W * i, GRID_W)
        given = xst.at[rows_at((1 - core) * tok + GRID_W * i, GRID_W, GRID_W), :]
        kept = xst.at[rows_at(core * tok + GRID_W * i, GRID_W, GRID_W), :]
        for j in ORDER + (0,):
            far = (2 * j + 1 - 2 * core + n_tp) if j else (1 - 2 * core + n_tp)
            there = xs.at[0, j, spot, my_lanes]
            pair = []
            if j:
                pair.append(send(kept, there, f_s.at[i, 0, j], f_r.at[i, 0, j], peer(j)))
            device = {"tp": lax.rem(tp + far, n_tp)}
            pair.append(send(given, there, f_s.at[i, 1, j], f_r.at[i, 1, j], device))
            first_gather[i][j] = pair
    t_mate = send(tab.at[0], tab.at[2], d2d_s.at[1], d2d_r.at[1], {"tp": mate})
    w_mate = []
    o_mate = []

    def give_weights(layer):
        sem = 2 + 4 * layer
        pairs = [
            (w_ref.at[layer], wraw.at[layer, rows, :])
            for w_ref, rows in zip((wq_ref, wk_ref, wv_ref), w_rows, strict=True)
        ]
        pairs.append((wo_ref.at[layer], wout.at[layer, :, my_lanes]))
        for i, (mine, there) in enumerate(pairs):
            copy = send(mine, there, d2d_s.at[sem + i], d2d_r.at[sem + i], {"tp": mate})
            (w_mate if i < 3 else o_mate).append(copy)

    give_weights(0)

    def scale_layer(layer):
        for copy in own_w[3 * layer : 3 * layer + 3]:
            copy.wait()
        for copy in w_mate[3 * layer : 3 * layer + 3]:
            copy.wait_recv()

        def one(j, carry):
            source = lax.rem(chip - j + chips, chips)
            lanes = rows_at(source * feat, feat, feat)
            gain = gain_ref[pl.ds(layer, 1), lanes]
            scale = HEAD_DIM ** (-0.5)
            wg[layer, j, 0:128, :] = (
                wraw[layer, 0:128, lanes].astype(jnp.float32) * (gain * scale)
            ).astype(jnp.bfloat16)
            wg[layer, j, 128:384, :] = (
                wraw[layer, 128:384, lanes].astype(jnp.float32) * gain
            ).astype(jnp.bfloat16)
            return carry

        lax.fori_loop(0, chips, one, 0)

    all_rows = n_sp * 4
    starts = []
    offsets = []
    for i in range(2):
        row = sp * 4 + core * 2 + i
        first = jnp.clip(row - ROW_SPAN // 2, 0, all_rows - ROW_SPAN)
        starts.append(first - sp * 4 + 4)
        offsets.append(first - row + ROW_SPAN - 1)

    def make_bias():
        t_mate.wait_recv()
        lane = lax.broadcasted_iota(jnp.int32, (GRID_W, 128), 1)
        key_col = jnp.where(lane < GRID_W, lane, lane - GRID_W)
        query_col = lax.broadcasted_iota(jnp.int32, (GRID_W, 128), 0)
        window = jnp.clip(query_col - COL_SPAN // 2, 0, GRID_W - COL_SPAN)
        inside = (key_col >= window) & (key_col < window + COL_SPAN)

        def one(layer, carry):
            for head in range(2):
                which = jnp.where(core == head, 0, 2)
                for i in range(2):
                    for pair in range(4):
                        line = tab[which, layer, pl.ds(offsets[i] + 2 * pair, 1), :]
                        wide = jnp.broadcast_to(line, (GRID_W, 128))
                        rolled = pltpu.roll(wide, 0, 1, stride=1, stride_axis=0)
                        bias[layer, head, i, :, 128 * pair : 128 * pair + 128] = jnp.where(
                            inside, rolled, NEG
                        )
            return carry

        lax.fori_loop(0, layers, one, 0)


    lane_low = lax.broadcasted_iota(jnp.int32, (GRID_W, 128), 1) < HEAD_DIM
    not_last = sp < n_sp - 1
    not_first = sp > 0
    places = [rows_at(256 + core * tok + GRID_W * i, GRID_W, GRID_W) for i in range(2)]

    def halo_copies(layer, i):
        mine = kv.at[layer, places[i], :]
        above = kv.at[layer, rows_at(core * tok + GRID_W * i, GRID_W, GRID_W), :]
        below = kv.at[layer, rows_at(512 + core * tok + GRID_W * i, GRID_W, GRID_W), :]
        to_first = sp == 1
        to_last = sp == n_sp - 2
        at_first = sp == 0
        at_last = sp == n_sp - 1
        low = core == 0
        high = core == 1
        if i == 0:
            down_same, down_same_got = not_first, not_last
        else:
            down_same, down_same_got = to_first, at_first
        plan = (
            (above, up, tp, not_last, not_first),
            (below, down, tp, down_same, down_same_got),
            (
                above,
                up,
                mate,
                not_last & (high | to_last),
                not_first & (low | at_last),
            ),
            (
                below,
                down,
                mate,
                not_first & (low | to_first),
                not_last & (high | at_first),
            ),
        )
        copies = []
        for n, (spot, z, t, sent, got) in enumerate(plan):
            copy = pltpu.make_async_remote_copy(
                src_ref=mine,
                dst_ref=spot,
                send_sem=h_s.at[layer, i, n + 1],
                recv_sem=h_r.at[layer, i, n + 1],
                device_id={"sp": z, "tp": t},
                device_id_type=MESH,
            )
            copies.append((copy, sent, got))
        return mine, copies

    def arrive(coming, slot):
        for copy in coming.pop(slot, ()):
            copy.wait_recv()

    def hand_on(array, row, coming, s_sems, r_sems):
        spot = pl.ds(GRID_W * row, GRID_W)
        for came, far, there in HAND:
            arrive(coming, came)
            copy = send(
                array.at[came, spot, :],
                array.at[there, spot, :],
                s_sems.at[row, there],
                r_sems.at[row, there],
                peer(far),
            )
            coming[there] = [copy]

    conditional = []
    x_gather = first_gather
    for layer in range(layers):
        queries = []
        mates = []
        halos = []
        for i in range(2):
            hand_on(xs.at[layer], i, x_gather[i], x_s.at[layer], x_r.at[layer])
        if layer == 0:
            own_g.wait()
            own_x[1].wait()
            make_bias()
        scale_layer(layer)
        for i in range(2):
            spot = slice(GRID_W * i, GRID_W * (i + 1))
            made = None
            squares = None
            for j in (0,) + ARRIVE:
                arrive(x_gather[i], j)
                block = xs[layer, j, spot]
                wide = block.astype(jnp.float32)
                square = wide * wide
                part = lax.dot_general(
                    block,
                    wg[layer, j],
                    (((1,), (1,)), ((), ())),
                    preferred_element_type=jnp.float32,
                )
                made = part if made is None else made + part
                squares = square if squares is None else squares + square
            mean = jnp.sum(squares, axis=1, keepdims=True) * (1.0 / (feat * chips))
            normed = made * lax.rsqrt(mean + EPS)
            queries.append(normed[:, 0:128].astype(jnp.bfloat16))
            kv[layer, places[i], :] = normed[:, 128:384].astype(jnp.bfloat16)
            mine, copies = halo_copies(layer, i)
            mates.append(send(mine, mine, h_s.at[layer, i, 0], h_r.at[layer, i, 0], {"tp": mate}))
            for copy, sent, _ in copies:

                @pl.when(sent)
                def _(copy=copy):
                    copy.start()

            halos += copies
            conditional += copies
        for copy in mates:
            copy.wait_recv()
        for copy, _, got in halos:

            @pl.when(got)
            def _(copy=copy):
                copy.wait_recv()

        gather = [{}, {}]
        x_gather = [{}, {}]
        for i in range(2):
            spot = pl.ds(GRID_W * i, GRID_W)
            outs = []
            for head in range(2):
                pick = lane_low if head == 1 else jnp.logical_not(lane_low)
                query = jnp.where(pick, queries[i], 0)
                pairs = kv[
                    layer,
                    rows_at(starts[i] * GRID_W, ROW_SPAN * GRID_W, GRID_W),
                    128 * head : 128 * head + 128,
                ]
                scores = lax.dot_general(
                    query, pairs, (((1,), (1,)), ((), ())), preferred_element_type=jnp.float32
                )
                scores = scores + bias[layer, head, i]
                peak = jnp.max(scores, axis=1, keepdims=True)
                lifted = jnp.exp(scores - peak)
                total = jnp.sum(lifted, axis=1, keepdims=True)
                mixed = jnp.dot(
                    lifted.astype(jnp.bfloat16), pairs, preferred_element_type=jnp.float32
                )
                outs.append(mixed / total)
            both = jnp.where(lane_low, outs[0], outs[1])
            atts[layer, 0, spot, :] = both.astype(jnp.bfloat16)
            for j in ORDER:
                copy = send(
                    atts.at[layer, 0, spot, :],
                    atts.at[layer, j, spot, :],
                    a_s.at[layer, i, j],
                    a_r.at[layer, i, j],
                    peer(j),
                )
                gather[i][j] = [copy]
        before = list(sends[: -2 * len(ORDER)])
        del sends[: len(before)]
        for i in range(2):
            hand_on(atts.at[layer], i, gather[i], a_s.at[layer], a_r.at[layer])
        if layer + 1 < layers:
            give_weights(layer + 1)
        for copy in before:
            copy.wait_send()

        own_o[layer].wait()
        o_mate[layer].wait_recv()
        last = []
        kept = []
        for i in range(2):
            spot = pl.ds(GRID_W * i, GRID_W)
            stream = xs[layer, 0, spot].astype(jnp.float32)
            for j in (0,) + ARRIVE:
                arrive(gather[i], j)
                source = lax.rem(chip - j + chips, chips)
                stream = stream + jnp.dot(
                    atts[layer, j, spot],
                    wout[layer, rows_at(source * 128, 128, 128), :],
                    preferred_element_type=jnp.float32,
                )
            final = stream.astype(jnp.bfloat16)
            if layer + 1 < layers:
                xs[layer + 1, 0, spot, :] = final
                for j in ORDER:
                    copy = send(
                        xs.at[layer + 1, 0, spot, :],
                        xs.at[layer + 1, j, spot, :],
                        x_s.at[layer + 1, i, j],
                        x_r.at[layer + 1, i, j],
                        peer(j),
                    )
                    x_gather[i][j] = [copy]
            else:
                swap = core == 0
                last_half[spot, :] = jnp.where(swap, final[:, half:feat], final[:, 0:half])
                place = rows_at(core * tok + GRID_W * i, GRID_W, GRID_W)
                last.append(
                    send(
                        last_half.at[spot, :],
                        out_ref.at[place, :],
                        d2d_s.at[2 + 4 * layers + i],
                        d2d_r.at[2 + 4 * layers + i],
                        {"tp": mate},
                    )
                )
                kept_half[spot, :] = jnp.where(swap, final[:, 0:half], final[:, half:feat])
                copy = pltpu.make_async_copy(
                    kept_half.at[spot, :], out_ref.at[place, :], own_x_sem.at[4 + i]
                )
                copy.start()
                kept.append(copy)
        for copy in last:
            copy.wait_recv()
        for copy in kept:
            copy.wait()
    for copy, sent, _ in conditional:

        @pl.when(sent)
        def _(copy=copy):
            copy.wait_send()

    for copy in sends:
        copy.wait_send()


def body(hidden_in, norm_gain, query_weight, key_weight, value_weight, output_weight, offset_bias):
    n_sp = lax.axis_size("sp")
    n_tp = lax.axis_size("tp")
    chips = n_tp // 2
    layers = norm_gain.shape[0]
    width = norm_gain.shape[1]
    tokens, _ = hidden_in.shape
    tok = tokens // 2
    feat = width // chips
    any_space = pl.BlockSpec(memory_space=pltpu.HBM)
    dma = pltpu.SemaphoreType.DMA
    bf16 = jnp.bfloat16
    table = offset_bias.transpose(0, 2, 1, 3)
    return pl.pallas_call(
        functools.partial(kernel, n_sp, n_tp, layers),
        out_shape=jax.ShapeDtypeStruct(hidden_in.shape, bf16),
        in_specs=[any_space] * 7,
        out_specs=any_space,
        scratch_shapes=[
            pltpu.VMEM(norm_gain.shape, jnp.float32),
            pltpu.VMEM(table.shape, jnp.float32),
            pltpu.VMEM((tokens, feat // 2), bf16),
            pltpu.VMEM((tok, feat // 2), bf16),
            pltpu.VMEM((tok, feat // 2), bf16),
            pltpu.VMEM((layers, chips, tok, feat), bf16),
            pltpu.VMEM((layers, chips, tok, 128), bf16),
            pltpu.VMEM((layers, 768, 256), bf16),
            pltpu.VMEM((layers, 384, width), bf16),
            pltpu.VMEM((layers, chips, 384, feat), bf16),
            pltpu.VMEM((layers, 1024, feat), bf16),
            pltpu.VMEM((3, layers, 16, 128), jnp.float32),
            pltpu.VMEM((layers, 2, 2, GRID_W, ROW_SPAN * GRID_W), jnp.float32),
            dma((layers, 3)),
            dma((layers,)),
            dma((6,)),
            dma((4 + 4 * layers,)),
            dma((4 + 4 * layers,)),
            dma((2, 2, chips)),
            dma((2, 2, chips)),
            dma((layers, 2, chips)),
            dma((layers, 2, chips)),
            dma((layers, 2, chips)),
            dma((layers, 2, chips)),
            dma((layers, 2, 5)),
            dma((layers, 2, 5)),
        ],
        compiler_params=pltpu.CompilerParams(
            collective_id=0, has_side_effects=True, vmem_limit_bytes=67043328
        ),
        name="layers",
    )(hidden_in, norm_gain, query_weight, key_weight, value_weight, output_weight, table)


def solution(mesh):
    return jax.shard_map(
        body,
        mesh=mesh,
        in_specs=(
            P(("grp", "sp"), "tp"),
            P(),
            P(None, "tp", None),
            P(None, "tp", None),
            P(None, "tp", None),
            P(None, None, "tp"),
            P(None, "tp", None, None),
        ),
        out_specs=P(("grp", "sp"), "tp"),
        check_vma=False,
    )
```

```python
import functools

import jax
import jax.numpy as jnp
from jax import lax
from jax.experimental import pallas as pl
from jax.experimental.pallas import tpu as pltpu
from jax.sharding import PartitionSpec as P

HEAD_DIM = 64
GRID_W = 64
ROW_SPAN = 8
COL_SPAN = 16
EPS = 1e-06
NEG = -1e30
MESH = pl.DeviceIdType.MESH
ORDER = (2, 6, 1, 7)
ARRIVE = (1, 7, 2, 6, 3, 5, 4)
HALF = GRID_W // 2
HAND = (
    (2, 2, 4, (0, HALF), 4),
    (2, 1, 3, (0, GRID_W), 3),
    (6, -2, 4, (HALF, HALF), 0),
    (6, -1, 5, (0, GRID_W), 5),
)


def kernel(
    n_sp,
    n_tp,
    layers,
    hid_ref,
    gain_hbm,
    wq_ref,
    wk_ref,
    wv_ref,
    wo_ref,
    ob_hbm,
    out_ref,
    gain_ref,
    ob_ref,
    xst,
    last_half,
    kept_half,
    xs,
    atts,
    kv,
    wraw,
    wg,
    wout,
    tab,
    bias,
    own_w_sem,
    own_o_sem,
    own_x_sem,
    d2d_s,
    d2d_r,
    f_s,
    f_r,
    x_s,
    x_r,
    a_s,
    a_r,
    h_s,
    h_r,
):
    chips = n_tp // 2
    tok = xs.shape[3]
    feat = xs.shape[4]
    half = feat // 2
    tp = lax.axis_index("tp")
    sp = lax.axis_index("sp")
    core = lax.rem(tp, 2)
    chip = lax.div(tp, 2)
    mate = tp + 1 - 2 * core
    up = lax.rem(sp + 1, n_sp)
    down = lax.rem(sp + n_sp - 1, n_sp)

    def peer(j):
        return {"tp": lax.rem(tp + 2 * j + n_tp, n_tp)}

    def place_of(j, owner):
        at = owner if j in (1, chips - 1) else 1
        return {"tp": 2 * lax.rem(chip + j, chips) + at}

    def rows_at(start, size, align):
        return pl.ds(pl.multiple_of(start, align), size)

    greet = [peer(j) for j in ORDER] + [{"tp": mate}]
    greet += [{"tp": lax.rem(mate + 2 * j, n_tp)} for j in ORDER]
    greet += [{"sp": z, "tp": t} for z in (up, down) for t in (tp, mate)]
    barrier = pltpu.get_barrier_semaphore()
    for device in greet:
        pl.semaphore_signal(barrier, inc=1, device_id=device, device_id_type=MESH)

    my_lanes = rows_at(core * half, half, half)
    own_x = [
        pltpu.make_async_copy(hid_ref, xst, own_x_sem.at[0]),
        pltpu.make_async_copy(
            hid_ref.at[rows_at(core * tok, tok, tok), :], xs.at[0, core, 0, :, my_lanes], own_x_sem.at[1]
        ),
    ]
    own_g = pltpu.make_async_copy(gain_hbm, gain_ref, own_x_sem.at[2])
    own_b = pltpu.make_async_copy(ob_hbm, ob_ref, own_x_sem.at[3])
    for copy in own_x + [own_b, own_g]:
        copy.start()
    w_rows = (
        rows_at(HEAD_DIM * (1 - core), HEAD_DIM, HEAD_DIM),
        rows_at(192 + 64 * core, HEAD_DIM, HEAD_DIM),
        rows_at(128 + 192 * core, HEAD_DIM, HEAD_DIM),
    )
    own_w = []
    own_o = []
    for layer in range(layers):
        for i, w_ref in enumerate((wq_ref, wk_ref, wv_ref)):
            copy = pltpu.make_async_copy(
                w_ref.at[layer], wraw.at[layer, w_rows[i], :], own_w_sem.at[layer, i]
            )
            copy.start()
            own_w.append(copy)
    for layer in range(layers):
        copy = pltpu.make_async_copy(
            wo_ref.at[layer], wout.at[layer, :, my_lanes], own_o_sem.at[layer]
        )
        copy.start()
        own_o.append(copy)

    tab[1] = jnp.zeros(tab.shape[1:], jnp.float32)
    own_b.wait()
    for layer in range(layers):
        for line in range(2 * ROW_SPAN - 1):
            tab[1, layer, line : line + 1, 0:31] = ob_ref[layer, line]
    for layer in range(layers):
        raw = tab[1, layer]
        low = pltpu.roll(raw, 128 - 15, 1)
        high = pltpu.roll(pltpu.roll(raw, 64 - 15, 1), 15, 0)
        tab[0, layer] = low + high

    pl.semaphore_wait(barrier, len(greet))

    sends = []

    def send(src, dst, s_sem, r_sem, device):
        copy = pltpu.make_async_remote_copy(
            src_ref=src,
            dst_ref=dst,
            send_sem=s_sem,
            recv_sem=r_sem,
            device_id=device,
            device_id_type=MESH,
        )
        copy.start()
        sends.append(copy)
        return copy

    own_x[0].wait()
    for i in range(2):
        spot = pl.ds(GRID_W * i, GRID_W)
        for j in ORDER:
            for owner in range(2):
                send(
                    xst.at[pl.ds(owner * tok + GRID_W * i, GRID_W), :],
                    xs.at[0, owner, j, spot, my_lanes],
                    f_s.at[owner, i, j],
                    f_r.at[owner, i, core, j],
                    place_of(j, owner),
                )
        send(
            xst.at[rows_at((1 - core) * tok + GRID_W * i, GRID_W, GRID_W), :],
            xs.at[0, 1 - core, 0, spot, my_lanes],
            f_s.at[0, i, 0],
            f_r.at[1 - core, i, core, 0],
            {"tp": mate},
        )
    t_mate = send(tab.at[0], tab.at[2], d2d_s.at[1], d2d_r.at[1], {"tp": mate})
    w_mate = []
    o_mate = []

    def give_weights(layer):
        sem = 2 + 4 * layer
        pairs = [
            (w_ref.at[layer], wraw.at[layer, rows, :])
            for w_ref, rows in zip((wq_ref, wk_ref, wv_ref), w_rows, strict=True)
        ]
        pairs.append((wo_ref.at[layer], wout.at[layer, :, my_lanes]))
        for i, (mine, there) in enumerate(pairs):
            copy = send(mine, there, d2d_s.at[sem + i], d2d_r.at[sem + i], {"tp": mate})
            (w_mate if i < 3 else o_mate).append(copy)

    give_weights(0)

    def scale_layer(layer):
        for copy in own_w[3 * layer : 3 * layer + 3]:
            copy.wait()
        for copy in w_mate[3 * layer : 3 * layer + 3]:
            copy.wait_recv()

        def one(j, carry):
            source = lax.rem(chip - j + chips, chips)
            lanes = rows_at(source * feat, feat, feat)
            gain = gain_ref[pl.ds(layer, 1), lanes]
            scale = HEAD_DIM ** (-0.5)
            wg[layer, j, 0:128, :] = (
                wraw[layer, 0:128, lanes].astype(jnp.float32) * (gain * scale)
            ).astype(jnp.bfloat16)
            wg[layer, j, 128:384, :] = (
                wraw[layer, 128:384, lanes].astype(jnp.float32) * gain
            ).astype(jnp.bfloat16)
            return carry

        lax.fori_loop(0, chips, one, 0)

    all_rows = n_sp * 4
    starts = []
    offsets = []
    for i in range(2):
        row = sp * 4 + core * 2 + i
        first = jnp.clip(row - ROW_SPAN // 2, 0, all_rows - ROW_SPAN)
        starts.append(first - sp * 4 + 4)
        offsets.append(first - row + ROW_SPAN - 1)

    def make_bias():
        t_mate.wait_recv()
        lane = lax.broadcasted_iota(jnp.int32, (GRID_W, 128), 1)
        key_col = jnp.where(lane < GRID_W, lane, lane - GRID_W)
        query_col = lax.broadcasted_iota(jnp.int32, (GRID_W, 128), 0)
        window = jnp.clip(query_col - COL_SPAN // 2, 0, GRID_W - COL_SPAN)
        inside = (key_col >= window) & (key_col < window + COL_SPAN)

        def one(layer, carry):
            for head in range(2):
                which = jnp.where(core == head, 0, 2)
                for i in range(2):
                    for pair in range(4):
                        line = tab[which, layer, pl.ds(offsets[i] + 2 * pair, 1), :]
                        wide = jnp.broadcast_to(line, (GRID_W, 128))
                        rolled = pltpu.roll(wide, 0, 1, stride=1, stride_axis=0)
                        bias[layer, head, i, :, 128 * pair : 128 * pair + 128] = jnp.where(
                            inside, rolled, NEG
                        )
            return carry

        lax.fori_loop(0, layers, one, 0)


    lane_low = lax.broadcasted_iota(jnp.int32, (GRID_W, 128), 1) < HEAD_DIM
    not_last = sp < n_sp - 1
    not_first = sp > 0
    places = [rows_at(256 + core * tok + GRID_W * i, GRID_W, GRID_W) for i in range(2)]

    def halo_copies(layer, i):
        mine = kv.at[layer, places[i], :]
        above = kv.at[layer, rows_at(core * tok + GRID_W * i, GRID_W, GRID_W), :]
        below = kv.at[layer, rows_at(512 + core * tok + GRID_W * i, GRID_W, GRID_W), :]
        to_first = sp == 1
        to_last = sp == n_sp - 2
        at_first = sp == 0
        at_last = sp == n_sp - 1
        low = core == 0
        high = core == 1
        if i == 0:
            down_same, down_same_got = not_first, not_last
        else:
            down_same, down_same_got = to_first, at_first
        plan = (
            (above, up, tp, not_last, not_first),
            (below, down, tp, down_same, down_same_got),
            (
                above,
                up,
                mate,
                not_last & (high | to_last),
                not_first & (low | at_last),
            ),
            (
                below,
                down,
                mate,
                not_first & (low | to_first),
                not_last & (high | at_first),
            ),
        )
        copies = []
        for n, (spot, z, t, sent, got) in enumerate(plan):
            copy = pltpu.make_async_remote_copy(
                src_ref=mine,
                dst_ref=spot,
                send_sem=h_s.at[layer, i, n + 1],
                recv_sem=h_r.at[layer, i, n + 1],
                device_id={"sp": z, "tp": t},
                device_id_type=MESH,
            )
            copies.append((copy, sent, got))
        return mine, copies

    def part_of(array, owner, slot, row, first=0, size=GRID_W):
        return array.at[owner, slot, pl.ds(GRID_W * row + first, size), :]

    def remote(src, dst, s_sem, r_sem, device):
        return pltpu.make_async_remote_copy(
            src_ref=src,
            dst_ref=dst,
            send_sem=s_sem,
            recv_sem=r_sem,
            device_id=device,
            device_id_type=MESH,
        )

    def landed(there, sem):
        remote(there, there, d2d_s.at[0], sem, {"tp": mate}).wait_recv()

    def halves_landed(owner, slot, row, sources):
        for source in sources:
            lanes = rows_at(source * half, half, half)
            landed(
                xs.at[0, owner, slot, pl.ds(GRID_W * row, GRID_W), lanes],
                f_r.at[owner, row, source, slot],
            )

    def give(array, s_sems, r_sems, row):
        for j in ORDER:
            send(
                part_of(array, core, 0, row),
                part_of(array, core, j, row),
                s_sems.at[0, row, j],
                r_sems.at[core, row, j],
                place_of(j, core),
            )

    def relay(array, s_sems, r_sems, row, owner, n):
        came, far, there, (at, size), sem = HAND[n]
        return remote(
            part_of(array, owner, came, row, at, size),
            part_of(array, owner, there, row, at, size),
            s_sems.at[owner, row, 8 + n],
            r_sems.at[owner, row, sem],
            {"tp": 2 * lax.rem(chip + far + chips, chips) + owner},
        )

    def share(array, s_sems, r_sems, row, came):
        own = part_of(array, 0, came, row)
        return remote(
            own, own, s_sems.at[0, row, 12 + came // 4], r_sems.at[0, row, came], {"tp": mate}
        )

    handed = []

    def hand_on(array, s_sems, r_sems, row, first=False):
        @pl.when(core == 1)
        def _():
            for owner in (1, 0):
                for came in (2, 6):
                    if first:
                        halves_landed(owner, came, row, range(2))
                    else:
                        landed(part_of(array, owner, came, row), r_sems.at[owner, row, came])
                    for n, hand in enumerate(HAND):
                        if hand[0] == came:
                            make = functools.partial(relay, array, s_sems, r_sems, row, owner, n)
                            make().start()
                            handed.append(make)
                    if owner == 0:
                        make = functools.partial(share, array, s_sems, r_sems, row, came)
                        make().start()
                        handed.append(make)

    def arrive(array, r_sems, slot, row, first=False):
        if slot == 0:
            if first:
                halves_landed(core, 0, row, (1 - core,))
        elif slot in (2, 6):

            @pl.when(core == 0)
            def _():
                landed(part_of(array, 0, slot, row), r_sems.at[0, row, slot])
        elif slot == 4:
            landed(part_of(array, core, 4, row, 0, HALF), r_sems.at[core, row, 4])
            landed(part_of(array, core, 4, row, HALF, HALF), r_sems.at[core, row, 0])
        elif first and slot in (1, 7):
            halves_landed(core, slot, row, range(2))
        else:
            landed(part_of(array, core, slot, row), r_sems.at[core, row, slot])

    conditional = []
    for layer in range(layers):
        queries = []
        mates = []
        halos = []
        for i in range(2):
            hand_on(xs.at[layer], x_s.at[layer], x_r.at[layer], i, layer == 0)
        if layer == 0:
            own_g.wait()
            own_x[1].wait()
            make_bias()
        scale_layer(layer)
        for i in range(2):
            spot = slice(GRID_W * i, GRID_W * (i + 1))
            made = None
            squares = None
            for j in (0,) + ARRIVE:
                arrive(xs.at[layer], x_r.at[layer], j, i, layer == 0)
                block = xs[layer, core, j, spot]
                wide = block.astype(jnp.float32)
                square = wide * wide
                part = lax.dot_general(
                    block,
                    wg[layer, j],
                    (((1,), (1,)), ((), ())),
                    preferred_element_type=jnp.float32,
                )
                made = part if made is None else made + part
                squares = square if squares is None else squares + square
            mean = jnp.sum(squares, axis=1, keepdims=True) * (1.0 / (feat * chips))
            normed = made * lax.rsqrt(mean + EPS)
            queries.append(normed[:, 0:128].astype(jnp.bfloat16))
            kv[layer, places[i], :] = normed[:, 128:384].astype(jnp.bfloat16)
            mine, copies = halo_copies(layer, i)
            mates.append(send(mine, mine, h_s.at[layer, i, 0], h_r.at[layer, i, 0], {"tp": mate}))
            for copy, sent, _ in copies:

                @pl.when(sent)
                def _(copy=copy):
                    copy.start()

            halos += copies
            conditional += copies
        for copy in mates:
            copy.wait_recv()
        for copy, _, got in halos:

            @pl.when(got)
            def _(copy=copy):
                copy.wait_recv()

        for i in range(2):
            spot = pl.ds(GRID_W * i, GRID_W)
            outs = []
            for head in range(2):
                pick = lane_low if head == 1 else jnp.logical_not(lane_low)
                query = jnp.where(pick, queries[i], 0)
                pairs = kv[
                    layer,
                    rows_at(starts[i] * GRID_W, ROW_SPAN * GRID_W, GRID_W),
                    128 * head : 128 * head + 128,
                ]
                scores = lax.dot_general(
                    query, pairs, (((1,), (1,)), ((), ())), preferred_element_type=jnp.float32
                )
                scores = scores + bias[layer, head, i]
                peak = jnp.max(scores, axis=1, keepdims=True)
                lifted = jnp.exp(scores - peak)
                total = jnp.sum(lifted, axis=1, keepdims=True)
                mixed = jnp.dot(
                    lifted.astype(jnp.bfloat16), pairs, preferred_element_type=jnp.float32
                )
                outs.append(mixed / total)
            both = jnp.where(lane_low, outs[0], outs[1])
            atts[layer, core, 0, spot, :] = both.astype(jnp.bfloat16)
            give(atts.at[layer], a_s.at[layer], a_r.at[layer], i)
        before = list(sends[: -2 * len(ORDER)])
        del sends[: len(before)]
        for i in range(2):
            hand_on(atts.at[layer], a_s.at[layer], a_r.at[layer], i)
        if layer + 1 < layers:
            give_weights(layer + 1)
        for copy in before:
            copy.wait_send()

        own_o[layer].wait()
        o_mate[layer].wait_recv()
        last = []
        kept = []
        for i in range(2):
            spot = pl.ds(GRID_W * i, GRID_W)
            stream = xs[layer, core, 0, spot].astype(jnp.float32)
            for j in (0,) + ARRIVE:
                arrive(atts.at[layer], a_r.at[layer], j, i)
                source = lax.rem(chip - j + chips, chips)
                stream = stream + jnp.dot(
                    atts[layer, core, j, spot],
                    wout[layer, rows_at(source * 128, 128, 128), :],
                    preferred_element_type=jnp.float32,
                )
            final = stream.astype(jnp.bfloat16)
            if layer + 1 < layers:
                xs[layer + 1, core, 0, spot, :] = final
                give(xs.at[layer + 1], x_s.at[layer + 1], x_r.at[layer + 1], i)
            else:
                swap = core == 0
                last_half[spot, :] = jnp.where(swap, final[:, half:feat], final[:, 0:half])
                place = rows_at(core * tok + GRID_W * i, GRID_W, GRID_W)
                last.append(
                    send(
                        last_half.at[spot, :],
                        out_ref.at[place, :],
                        d2d_s.at[2 + 4 * layers + i],
                        d2d_r.at[2 + 4 * layers + i],
                        {"tp": mate},
                    )
                )
                kept_half[spot, :] = jnp.where(swap, final[:, 0:half], final[:, half:feat])
                copy = pltpu.make_async_copy(
                    kept_half.at[spot, :], out_ref.at[place, :], own_x_sem.at[4 + i]
                )
                copy.start()
                kept.append(copy)
        for copy in last:
            copy.wait_recv()
        for copy in kept:
            copy.wait()
    for copy, sent, _ in conditional:

        @pl.when(sent)
        def _(copy=copy):
            copy.wait_send()

    for copy in sends:
        copy.wait_send()

    @pl.when(core == 1)
    def _():
        for make in handed:
            make().wait_send()


def body(hidden_in, norm_gain, query_weight, key_weight, value_weight, output_weight, offset_bias):
    n_sp = lax.axis_size("sp")
    n_tp = lax.axis_size("tp")
    chips = n_tp // 2
    layers = norm_gain.shape[0]
    width = norm_gain.shape[1]
    tokens, _ = hidden_in.shape
    tok = tokens // 2
    feat = width // chips
    any_space = pl.BlockSpec(memory_space=pltpu.HBM)
    dma = pltpu.SemaphoreType.DMA
    bf16 = jnp.bfloat16
    table = offset_bias.transpose(0, 2, 1, 3)
    return pl.pallas_call(
        functools.partial(kernel, n_sp, n_tp, layers),
        out_shape=jax.ShapeDtypeStruct(hidden_in.shape, bf16),
        in_specs=[any_space] * 7,
        out_specs=any_space,
        scratch_shapes=[
            pltpu.VMEM(norm_gain.shape, jnp.float32),
            pltpu.VMEM(table.shape, jnp.float32),
            pltpu.VMEM((tokens, feat // 2), bf16),
            pltpu.VMEM((tok, feat // 2), bf16),
            pltpu.VMEM((tok, feat // 2), bf16),
            pltpu.VMEM((layers, 2, chips, tok, feat), bf16),
            pltpu.VMEM((layers, 2, chips, tok, 128), bf16),
            pltpu.VMEM((layers, 768, 256), bf16),
            pltpu.VMEM((layers, 384, width), bf16),
            pltpu.VMEM((layers, chips, 384, feat), bf16),
            pltpu.VMEM((layers, 1024, feat), bf16),
            pltpu.VMEM((3, layers, 16, 128), jnp.float32),
            pltpu.VMEM((layers, 2, 2, GRID_W, ROW_SPAN * GRID_W), jnp.float32),
            dma((layers, 3)),
            dma((layers,)),
            dma((6,)),
            dma((4 + 4 * layers,)),
            dma((4 + 4 * layers,)),
            dma((2, 2, chips)),
            dma((2, 2, 2, chips)),
            dma((layers, 2, 2, 16)),
            dma((layers, 2, 2, chips)),
            dma((layers, 2, 2, 16)),
            dma((layers, 2, 2, chips)),
            dma((layers, 2, 5)),
            dma((layers, 2, 5)),
        ],
        compiler_params=pltpu.CompilerParams(
            collective_id=0, has_side_effects=True, vmem_limit_bytes=67043328
        ),
        name="layers",
    )(hidden_in, norm_gain, query_weight, key_weight, value_weight, output_weight, table)


def solution(mesh):
    return jax.shard_map(
        body,
        mesh=mesh,
        in_specs=(
            P(("grp", "sp"), "tp"),
            P(),
            P(None, "tp", None),
            P(None, "tp", None),
            P(None, "tp", None),
            P(None, None, "tp"),
            P(None, "tp", None, None),
        ),
        out_specs=P(("grp", "sp"), "tp"),
        check_vma=False,
    )
```

```python
import functools

import jax
import jax.numpy as jnp
from jax import lax
from jax.experimental import pallas as pl
from jax.experimental.pallas import tpu as pltpu
from jax.sharding import PartitionSpec as P

HEAD_DIM = 64
GRID_W = 64
ROW_SPAN = 8
COL_SPAN = 16
EPS = 1e-06
NEG = -1e30
MESH = pl.DeviceIdType.MESH
ORDER = (2, 6, 1, 7)
ARRIVE = (1, 7, 2, 6, 3, 5, 4)
HALF = GRID_W // 2
WHOLE = (0, GRID_W)
STAGES = (
    ((2, 1, 3, WHOLE, 3), (6, -1, 5, WHOLE, 5)),
    ((3, 1, 4, (0, HALF), 4), (5, -1, 4, (HALF, HALF), 0)),
)


def kernel(
    n_sp,
    n_tp,
    layers,
    hid_ref,
    gain_hbm,
    wq_ref,
    wk_ref,
    wv_ref,
    wo_ref,
    ob_hbm,
    out_ref,
    gain_ref,
    ob_ref,
    xst,
    last_half,
    kept_half,
    xs,
    atts,
    kv,
    wraw,
    wg,
    wout,
    tab,
    bias,
    own_w_sem,
    own_o_sem,
    own_x_sem,
    d2d_s,
    d2d_r,
    f_s,
    f_r,
    x_s,
    x_r,
    a_s,
    a_r,
    h_s,
    h_r,
):
    chips = n_tp // 2
    tok = xs.shape[2]
    feat = xs.shape[3]
    half = feat // 2
    tp = lax.axis_index("tp")
    sp = lax.axis_index("sp")
    core = lax.rem(tp, 2)
    chip = lax.div(tp, 2)
    mate = tp + 1 - 2 * core
    up = lax.rem(sp + 1, n_sp)
    down = lax.rem(sp + n_sp - 1, n_sp)

    def peer(j):
        return {"tp": lax.rem(tp + 2 * j + n_tp, n_tp)}

    def rows_at(start, size, align):
        return pl.ds(pl.multiple_of(start, align), size)

    greet = [peer(j) for j in ORDER] + [{"tp": mate}]
    greet += [{"tp": lax.rem(mate + 2 * j, n_tp)} for j in ORDER]
    greet += [{"sp": z, "tp": t} for z in (up, down) for t in (tp, mate)]
    barrier = pltpu.get_barrier_semaphore()
    for device in greet:
        pl.semaphore_signal(barrier, inc=1, device_id=device, device_id_type=MESH)

    my_lanes = rows_at(core * half, half, half)
    own_x = [
        pltpu.make_async_copy(hid_ref, xst, own_x_sem.at[0]),
        pltpu.make_async_copy(
            hid_ref.at[rows_at(core * tok, tok, tok), :], xs.at[0, 0, :, my_lanes], own_x_sem.at[1]
        ),
    ]
    own_g = pltpu.make_async_copy(gain_hbm, gain_ref, own_x_sem.at[2])
    own_b = pltpu.make_async_copy(ob_hbm, ob_ref, own_x_sem.at[3])
    for copy in own_x + [own_b, own_g]:
        copy.start()
    w_rows = (
        rows_at(HEAD_DIM * (1 - core), HEAD_DIM, HEAD_DIM),
        rows_at(192 + 64 * core, HEAD_DIM, HEAD_DIM),
        rows_at(128 + 192 * core, HEAD_DIM, HEAD_DIM),
    )
    own_w = []
    own_o = []
    for layer in range(layers):
        for i, w_ref in enumerate((wq_ref, wk_ref, wv_ref)):
            copy = pltpu.make_async_copy(
                w_ref.at[layer], wraw.at[layer, w_rows[i], :], own_w_sem.at[layer, i]
            )
            copy.start()
            own_w.append(copy)
    for layer in range(layers):
        copy = pltpu.make_async_copy(
            wo_ref.at[layer], wout.at[layer, :, my_lanes], own_o_sem.at[layer]
        )
        copy.start()
        own_o.append(copy)

    tab[1] = jnp.zeros(tab.shape[1:], jnp.float32)
    own_b.wait()
    for layer in range(layers):
        for line in range(2 * ROW_SPAN - 1):
            tab[1, layer, line : line + 1, 0:31] = ob_ref[layer, line]
    for layer in range(layers):
        raw = tab[1, layer]
        low = pltpu.roll(raw, 128 - 15, 1)
        high = pltpu.roll(pltpu.roll(raw, 64 - 15, 1), 15, 0)
        tab[0, layer] = low + high

    pl.semaphore_wait(barrier, len(greet))

    sends = []

    def send(src, dst, s_sem, r_sem, device):
        copy = pltpu.make_async_remote_copy(
            src_ref=src,
            dst_ref=dst,
            send_sem=s_sem,
            recv_sem=r_sem,
            device_id=device,
            device_id_type=MESH,
        )
        copy.start()
        sends.append(copy)
        return copy

    own_x[0].wait()
    first_gather = [{}, {}]
    for i in range(2):
        spot = pl.ds(GRID_W * i, GRID_W)
        given = xst.at[rows_at((1 - core) * tok + GRID_W * i, GRID_W, GRID_W), :]
        kept = xst.at[rows_at(core * tok + GRID_W * i, GRID_W, GRID_W), :]
        for j in ORDER + (0,):
            far = (2 * j + 1 - 2 * core + n_tp) if j else (1 - 2 * core + n_tp)
            there = xs.at[0, j, spot, my_lanes]
            pair = []
            if j:
                pair.append(send(kept, there, f_s.at[i, 0, j], f_r.at[i, 0, j], peer(j)))
            device = {"tp": lax.rem(tp + far, n_tp)}
            pair.append(send(given, there, f_s.at[i, 1, j], f_r.at[i, 1, j], device))
            first_gather[i][j] = pair
    t_mate = send(tab.at[0], tab.at[2], d2d_s.at[1], d2d_r.at[1], {"tp": mate})
    w_mate = []
    o_mate = []

    def give_weights(layer):
        sem = 2 + 4 * layer
        pairs = [
            (w_ref.at[layer], wraw.at[layer, rows, :])
            for w_ref, rows in zip((wq_ref, wk_ref, wv_ref), w_rows, strict=True)
        ]
        pairs.append((wo_ref.at[layer], wout.at[layer, :, my_lanes]))
        for i, (mine, there) in enumerate(pairs):
            copy = send(mine, there, d2d_s.at[sem + i], d2d_r.at[sem + i], {"tp": mate})
            (w_mate if i < 3 else o_mate).append(copy)

    give_weights(0)

    def scale_layer(layer):
        for copy in own_w[3 * layer : 3 * layer + 3]:
            copy.wait()
        for copy in w_mate[3 * layer : 3 * layer + 3]:
            copy.wait_recv()

        def one(j, carry):
            source = lax.rem(chip - j + chips, chips)
            lanes = rows_at(source * feat, feat, feat)
            gain = gain_ref[pl.ds(layer, 1), lanes]
            scale = HEAD_DIM ** (-0.5)
            wg[layer, j, 0:128, :] = (
                wraw[layer, 0:128, lanes].astype(jnp.float32) * (gain * scale)
            ).astype(jnp.bfloat16)
            wg[layer, j, 128:384, :] = (
                wraw[layer, 128:384, lanes].astype(jnp.float32) * gain
            ).astype(jnp.bfloat16)
            return carry

        lax.fori_loop(0, chips, one, 0)

    all_rows = n_sp * 4
    starts = []
    offsets = []
    for i in range(2):
        row = sp * 4 + core * 2 + i
        first = jnp.clip(row - ROW_SPAN // 2, 0, all_rows - ROW_SPAN)
        starts.append(first - sp * 4 + 4)
        offsets.append(first - row + ROW_SPAN - 1)

    def make_bias():
        t_mate.wait_recv()
        lane = lax.broadcasted_iota(jnp.int32, (GRID_W, 128), 1)
        key_col = jnp.where(lane < GRID_W, lane, lane - GRID_W)
        query_col = lax.broadcasted_iota(jnp.int32, (GRID_W, 128), 0)
        window = jnp.clip(query_col - COL_SPAN // 2, 0, GRID_W - COL_SPAN)
        inside = (key_col >= window) & (key_col < window + COL_SPAN)

        def one(layer, carry):
            for head in range(2):
                which = jnp.where(core == head, 0, 2)
                for i in range(2):
                    for pair in range(4):
                        line = tab[which, layer, pl.ds(offsets[i] + 2 * pair, 1), :]
                        wide = jnp.broadcast_to(line, (GRID_W, 128))
                        rolled = pltpu.roll(wide, 0, 1, stride=1, stride_axis=0)
                        bias[layer, head, i, :, 128 * pair : 128 * pair + 128] = jnp.where(
                            inside, rolled, NEG
                        )
            return carry

        lax.fori_loop(0, layers, one, 0)


    lane_low = lax.broadcasted_iota(jnp.int32, (GRID_W, 128), 1) < HEAD_DIM
    not_last = sp < n_sp - 1
    not_first = sp > 0
    places = [rows_at(256 + core * tok + GRID_W * i, GRID_W, GRID_W) for i in range(2)]

    def halo_copies(layer, i):
        mine = kv.at[layer, places[i], :]
        above = kv.at[layer, rows_at(core * tok + GRID_W * i, GRID_W, GRID_W), :]
        below = kv.at[layer, rows_at(512 + core * tok + GRID_W * i, GRID_W, GRID_W), :]
        to_first = sp == 1
        to_last = sp == n_sp - 2
        at_first = sp == 0
        at_last = sp == n_sp - 1
        low = core == 0
        high = core == 1
        if i == 0:
            down_same, down_same_got = not_first, not_last
        else:
            down_same, down_same_got = to_first, at_first
        plan = (
            (above, up, tp, not_last, not_first),
            (below, down, tp, down_same, down_same_got),
            (
                above,
                up,
                mate,
                not_last & (high | to_last),
                not_first & (low | at_last),
            ),
            (
                below,
                down,
                mate,
                not_first & (low | to_first),
                not_last & (high | at_first),
            ),
        )
        copies = []
        for n, (spot, z, t, sent, got) in enumerate(plan):
            copy = pltpu.make_async_remote_copy(
                src_ref=mine,
                dst_ref=spot,
                send_sem=h_s.at[layer, i, n + 1],
                recv_sem=h_r.at[layer, i, n + 1],
                device_id={"sp": z, "tp": t},
                device_id_type=MESH,
            )
            copies.append((copy, sent, got))
        return mine, copies

    def arrive(coming, slot):
        for copy in coming.pop(slot, ()):
            copy.wait_recv()

    def hand_on(array, coming, s_sems, r_sems):
        for stage in STAGES:
            for row in range(2):
                for came, far, there, (first, size), sem in stage:
                    arrive(coming[row], came)
                    spot = pl.ds(GRID_W * row + first, size)
                    copy = send(
                        array.at[came, spot, :],
                        array.at[there, spot, :],
                        s_sems.at[row, sem],
                        r_sems.at[row, sem],
                        peer(far),
                    )
                    coming[row].setdefault(there, []).append(copy)

    conditional = []
    x_gather = first_gather
    for layer in range(layers):
        queries = []
        mates = []
        halos = []
        hand_on(xs.at[layer], x_gather, x_s.at[layer], x_r.at[layer])
        if layer == 0:
            own_g.wait()
            own_x[1].wait()
            make_bias()
        scale_layer(layer)
        for i in range(2):
            spot = slice(GRID_W * i, GRID_W * (i + 1))
            made = None
            squares = None
            for j in (0,) + ARRIVE:
                arrive(x_gather[i], j)
                block = xs[layer, j, spot]
                wide = block.astype(jnp.float32)
                square = wide * wide
                part = lax.dot_general(
                    block,
                    wg[layer, j],
                    (((1,), (1,)), ((), ())),
                    preferred_element_type=jnp.float32,
                )
                made = part if made is None else made + part
                squares = square if squares is None else squares + square
            mean = jnp.sum(squares, axis=1, keepdims=True) * (1.0 / (feat * chips))
            normed = made * lax.rsqrt(mean + EPS)
            queries.append(normed[:, 0:128].astype(jnp.bfloat16))
            kv[layer, places[i], :] = normed[:, 128:384].astype(jnp.bfloat16)
            mine, copies = halo_copies(layer, i)
            mates.append(send(mine, mine, h_s.at[layer, i, 0], h_r.at[layer, i, 0], {"tp": mate}))
            for copy, sent, _ in copies:

                @pl.when(sent)
                def _(copy=copy):
                    copy.start()

            halos += copies
            conditional += copies
        for copy in mates:
            copy.wait_recv()
        for copy, _, got in halos:

            @pl.when(got)
            def _(copy=copy):
                copy.wait_recv()

        gather = [{}, {}]
        x_gather = [{}, {}]
        for i in range(2):
            spot = pl.ds(GRID_W * i, GRID_W)
            outs = []
            for head in range(2):
                pick = lane_low if head == 1 else jnp.logical_not(lane_low)
                query = jnp.where(pick, queries[i], 0)
                pairs = kv[
                    layer,
                    rows_at(starts[i] * GRID_W, ROW_SPAN * GRID_W, GRID_W),
                    128 * head : 128 * head + 128,
                ]
                scores = lax.dot_general(
                    query, pairs, (((1,), (1,)), ((), ())), preferred_element_type=jnp.float32
                )
                scores = scores + bias[layer, head, i]
                peak = jnp.max(scores, axis=1, keepdims=True)
                lifted = jnp.exp(scores - peak)
                total = jnp.sum(lifted, axis=1, keepdims=True)
                mixed = jnp.dot(
                    lifted.astype(jnp.bfloat16), pairs, preferred_element_type=jnp.float32
                )
                outs.append(mixed / total)
            both = jnp.where(lane_low, outs[0], outs[1])
            atts[layer, 0, spot, :] = both.astype(jnp.bfloat16)
            for j in ORDER:
                copy = send(
                    atts.at[layer, 0, spot, :],
                    atts.at[layer, j, spot, :],
                    a_s.at[layer, i, j],
                    a_r.at[layer, i, j],
                    peer(j),
                )
                gather[i][j] = [copy]
        before = list(sends[: -2 * len(ORDER)])
        del sends[: len(before)]
        hand_on(atts.at[layer], gather, a_s.at[layer], a_r.at[layer])
        if layer + 1 < layers:
            give_weights(layer + 1)
        for copy in before:
            copy.wait_send()

        own_o[layer].wait()
        o_mate[layer].wait_recv()
        last = []
        kept = []
        for i in range(2):
            spot = pl.ds(GRID_W * i, GRID_W)
            stream = xs[layer, 0, spot].astype(jnp.float32)
            for j in (0,) + ARRIVE:
                arrive(gather[i], j)
                source = lax.rem(chip - j + chips, chips)
                stream = stream + jnp.dot(
                    atts[layer, j, spot],
                    wout[layer, rows_at(source * 128, 128, 128), :],
                    preferred_element_type=jnp.float32,
                )
            final = stream.astype(jnp.bfloat16)
            if layer + 1 < layers:
                xs[layer + 1, 0, spot, :] = final
                for j in ORDER:
                    copy = send(
                        xs.at[layer + 1, 0, spot, :],
                        xs.at[layer + 1, j, spot, :],
                        x_s.at[layer + 1, i, j],
                        x_r.at[layer + 1, i, j],
                        peer(j),
                    )
                    x_gather[i][j] = [copy]
            else:
                swap = core == 0
                last_half[spot, :] = jnp.where(swap, final[:, half:feat], final[:, 0:half])
                place = rows_at(core * tok + GRID_W * i, GRID_W, GRID_W)
                last.append(
                    send(
                        last_half.at[spot, :],
                        out_ref.at[place, :],
                        d2d_s.at[2 + 4 * layers + i],
                        d2d_r.at[2 + 4 * layers + i],
                        {"tp": mate},
                    )
                )
                kept_half[spot, :] = jnp.where(swap, final[:, 0:half], final[:, half:feat])
                copy = pltpu.make_async_copy(
                    kept_half.at[spot, :], out_ref.at[place, :], own_x_sem.at[4 + i]
                )
                copy.start()
                kept.append(copy)
        for copy in last:
            copy.wait_recv()
        for copy in kept:
            copy.wait()
    for copy, sent, _ in conditional:

        @pl.when(sent)
        def _(copy=copy):
            copy.wait_send()

    for copy in sends:
        copy.wait_send()


def body(hidden_in, norm_gain, query_weight, key_weight, value_weight, output_weight, offset_bias):
    n_sp = lax.axis_size("sp")
    n_tp = lax.axis_size("tp")
    chips = n_tp // 2
    layers = norm_gain.shape[0]
    width = norm_gain.shape[1]
    tokens, _ = hidden_in.shape
    tok = tokens // 2
    feat = width // chips
    any_space = pl.BlockSpec(memory_space=pltpu.HBM)
    dma = pltpu.SemaphoreType.DMA
    bf16 = jnp.bfloat16
    table = offset_bias.transpose(0, 2, 1, 3)
    return pl.pallas_call(
        functools.partial(kernel, n_sp, n_tp, layers),
        out_shape=jax.ShapeDtypeStruct(hidden_in.shape, bf16),
        in_specs=[any_space] * 7,
        out_specs=any_space,
        scratch_shapes=[
            pltpu.VMEM(norm_gain.shape, jnp.float32),
            pltpu.VMEM(table.shape, jnp.float32),
            pltpu.VMEM((tokens, feat // 2), bf16),
            pltpu.VMEM((tok, feat // 2), bf16),
            pltpu.VMEM((tok, feat // 2), bf16),
            pltpu.VMEM((layers, chips, tok, feat), bf16),
            pltpu.VMEM((layers, chips, tok, 128), bf16),
            pltpu.VMEM((layers, 768, 256), bf16),
            pltpu.VMEM((layers, 384, width), bf16),
            pltpu.VMEM((layers, chips, 384, feat), bf16),
            pltpu.VMEM((layers, 1024, feat), bf16),
            pltpu.VMEM((3, layers, 16, 128), jnp.float32),
            pltpu.VMEM((layers, 2, 2, GRID_W, ROW_SPAN * GRID_W), jnp.float32),
            dma((layers, 3)),
            dma((layers,)),
            dma((6,)),
            dma((4 + 4 * layers,)),
            dma((4 + 4 * layers,)),
            dma((2, 2, chips)),
            dma((2, 2, chips)),
            dma((layers, 2, chips)),
            dma((layers, 2, chips)),
            dma((layers, 2, chips)),
            dma((layers, 2, chips)),
            dma((layers, 2, 5)),
            dma((layers, 2, 5)),
        ],
        compiler_params=pltpu.CompilerParams(
            collective_id=0, has_side_effects=True, vmem_limit_bytes=67043328
        ),
        name="layers",
    )(hidden_in, norm_gain, query_weight, key_weight, value_weight, output_weight, table)


def solution(mesh):
    return jax.shard_map(
        body,
        mesh=mesh,
        in_specs=(
            P(("grp", "sp"), "tp"),
            P(),
            P(None, "tp", None),
            P(None, "tp", None),
            P(None, "tp", None),
            P(None, None, "tp"),
            P(None, "tp", None, None),
        ),
        out_specs=P(("grp", "sp"), "tp"),
        check_vma=False,
    )
```

```python
import functools

import jax
import jax.numpy as jnp
from jax import lax
from jax.experimental import pallas as pl
from jax.experimental.pallas import tpu as pltpu
from jax.sharding import PartitionSpec as P

HEAD_DIM = 64
GRID_W = 64
ROW_SPAN = 8
COL_SPAN = 16
EPS = 1e-06
NEG = -1e30
MESH = pl.DeviceIdType.MESH
ORDER = (2, 6, 1, 7)
ARRIVE = (1, 7, 2, 6, 3, 5, 4)
HALF = GRID_W // 2
HAND = (
    (2, 2, 4, (0, HALF), 4),
    (2, 1, 3, (0, GRID_W), 3),
    (6, -2, 4, (HALF, HALF), 0),
    (6, -1, 5, (0, GRID_W), 5),
)


def kernel(
    n_sp,
    n_tp,
    layers,
    hid_ref,
    gain_hbm,
    wq_ref,
    wk_ref,
    wv_ref,
    wo_ref,
    ob_hbm,
    out_ref,
    gain_ref,
    ob_ref,
    xst,
    last_half,
    kept_half,
    xs,
    atts,
    kv,
    wraw,
    wg,
    wout,
    tab,
    bias,
    own_w_sem,
    own_o_sem,
    own_x_sem,
    d2d_s,
    d2d_r,
    f_s,
    f_r,
    x_s,
    x_r,
    a_s,
    a_r,
    h_s,
    h_r,
):
    chips = n_tp // 2
    tok = xs.shape[2]
    feat = xs.shape[3]
    half = feat // 2
    tp = lax.axis_index("tp")
    sp = lax.axis_index("sp")
    core = lax.rem(tp, 2)
    chip = lax.div(tp, 2)
    mate = tp + 1 - 2 * core
    up = lax.rem(sp + 1, n_sp)
    down = lax.rem(sp + n_sp - 1, n_sp)

    def peer(j):
        return {"tp": lax.rem(tp + 2 * j + n_tp, n_tp)}

    def rows_at(start, size, align):
        return pl.ds(pl.multiple_of(start, align), size)

    greet = [peer(j) for j in ORDER] + [{"tp": mate}]
    greet += [{"tp": lax.rem(mate + 2 * j, n_tp)} for j in ORDER]
    greet += [{"sp": z, "tp": t} for z in (up, down) for t in (tp, mate)]
    barrier = pltpu.get_barrier_semaphore()
    for device in greet:
        pl.semaphore_signal(barrier, inc=1, device_id=device, device_id_type=MESH)

    my_lanes = rows_at(core * half, half, half)
    own_x = [
        pltpu.make_async_copy(hid_ref, xst, own_x_sem.at[0]),
        pltpu.make_async_copy(
            hid_ref.at[rows_at(core * tok, tok, tok), :], xs.at[0, 0, :, my_lanes], own_x_sem.at[1]
        ),
    ]
    own_g = pltpu.make_async_copy(gain_hbm, gain_ref, own_x_sem.at[2])
    own_b = pltpu.make_async_copy(ob_hbm, ob_ref, own_x_sem.at[3])
    for copy in own_x + [own_b, own_g]:
        copy.start()
    w_rows = (
        rows_at(HEAD_DIM * (1 - core), HEAD_DIM, HEAD_DIM),
        rows_at(192 + 64 * core, HEAD_DIM, HEAD_DIM),
        rows_at(128 + 192 * core, HEAD_DIM, HEAD_DIM),
    )
    own_w = []
    own_o = []
    for layer in range(layers):
        for i, w_ref in enumerate((wq_ref, wk_ref, wv_ref)):
            copy = pltpu.make_async_copy(
                w_ref.at[layer], wraw.at[layer, w_rows[i], :], own_w_sem.at[layer, i]
            )
            copy.start()
            own_w.append(copy)
    for layer in range(layers):
        copy = pltpu.make_async_copy(
            wo_ref.at[layer], wout.at[layer, :, my_lanes], own_o_sem.at[layer]
        )
        copy.start()
        own_o.append(copy)

    tab[1] = jnp.zeros(tab.shape[1:], jnp.float32)
    own_b.wait()
    for layer in range(layers):
        for line in range(2 * ROW_SPAN - 1):
            tab[1, layer, line : line + 1, 0:31] = ob_ref[layer, line]
    for layer in range(layers):
        raw = tab[1, layer]
        low = pltpu.roll(raw, 128 - 15, 1)
        high = pltpu.roll(pltpu.roll(raw, 64 - 15, 1), 15, 0)
        tab[0, layer] = low + high

    pl.semaphore_wait(barrier, len(greet))

    sends = []

    def send(src, dst, s_sem, r_sem, device):
        copy = pltpu.make_async_remote_copy(
            src_ref=src,
            dst_ref=dst,
            send_sem=s_sem,
            recv_sem=r_sem,
            device_id=device,
            device_id_type=MESH,
        )
        copy.start()
        sends.append(copy)
        return copy

    own_x[0].wait()
    first_gather = [{}, {}]
    for i in range(2):
        spot = pl.ds(GRID_W * i, GRID_W)
        given = xst.at[rows_at((1 - core) * tok + GRID_W * i, GRID_W, GRID_W), :]
        kept = xst.at[rows_at(core * tok + GRID_W * i, GRID_W, GRID_W), :]
        for j in ORDER + (0,):
            far = (2 * j + 1 - 2 * core + n_tp) if j else (1 - 2 * core + n_tp)
            there = xs.at[0, j, spot, my_lanes]
            pair = []
            if j:
                pair.append(send(kept, there, f_s.at[i, 0, j], f_r.at[i, 0, j], peer(j)))
            device = {"tp": lax.rem(tp + far, n_tp)}
            pair.append(send(given, there, f_s.at[i, 1, j], f_r.at[i, 1, j], device))
            first_gather[i][j] = pair
    t_mate = send(tab.at[0], tab.at[2], d2d_s.at[1], d2d_r.at[1], {"tp": mate})
    w_mate = []
    o_mate = []

    def give_weights(layer):
        sem = 2 + 4 * layer
        pairs = [
            (w_ref.at[layer], wraw.at[layer, rows, :])
            for w_ref, rows in zip((wq_ref, wk_ref, wv_ref), w_rows, strict=True)
        ]
        pairs.append((wo_ref.at[layer], wout.at[layer, :, my_lanes]))
        for i, (mine, there) in enumerate(pairs):
            copy = send(mine, there, d2d_s.at[sem + i], d2d_r.at[sem + i], {"tp": mate})
            (w_mate if i < 3 else o_mate).append(copy)

    give_weights(0)

    def scale_layer(layer):
        for copy in own_w[3 * layer : 3 * layer + 3]:
            copy.wait()
        for copy in w_mate[3 * layer : 3 * layer + 3]:
            copy.wait_recv()

        def one(j, carry):
            source = lax.rem(chip - j + chips, chips)
            lanes = rows_at(source * feat, feat, feat)
            gain = gain_ref[pl.ds(layer, 1), lanes]
            scale = HEAD_DIM ** (-0.5)
            wg[layer, j, 0:128, :] = (
                wraw[layer, 0:128, lanes].astype(jnp.float32) * (gain * scale)
            ).astype(jnp.bfloat16)
            wg[layer, j, 128:384, :] = (
                wraw[layer, 128:384, lanes].astype(jnp.float32) * gain
            ).astype(jnp.bfloat16)
            return carry

        lax.fori_loop(0, chips, one, 0)

    all_rows = n_sp * 4
    starts = []
    offsets = []
    for i in range(2):
        row = sp * 4 + core * 2 + i
        first = jnp.clip(row - ROW_SPAN // 2, 0, all_rows - ROW_SPAN)
        starts.append(first - sp * 4 + 4)
        offsets.append(first - row + ROW_SPAN - 1)

    def make_bias():
        t_mate.wait_recv()
        lane = lax.broadcasted_iota(jnp.int32, (GRID_W, 128), 1)
        key_col = jnp.where(lane < GRID_W, lane, lane - GRID_W)
        query_col = lax.broadcasted_iota(jnp.int32, (GRID_W, 128), 0)
        window = jnp.clip(query_col - COL_SPAN // 2, 0, GRID_W - COL_SPAN)
        inside = (key_col >= window) & (key_col < window + COL_SPAN)

        def one(layer, carry):
            for head in range(2):
                which = jnp.where(core == head, 0, 2)
                for i in range(2):
                    for pair in range(4):
                        line = tab[which, layer, pl.ds(offsets[i] + 2 * pair, 1), :]
                        wide = jnp.broadcast_to(line, (GRID_W, 128))
                        rolled = pltpu.roll(wide, 0, 1, stride=1, stride_axis=0)
                        bias[layer, head, i, :, 128 * pair : 128 * pair + 128] = jnp.where(
                            inside, rolled, NEG
                        )
            return carry

        lax.fori_loop(0, layers, one, 0)


    lane_low = lax.broadcasted_iota(jnp.int32, (GRID_W, 128), 1) < HEAD_DIM
    not_last = sp < n_sp - 1
    not_first = sp > 0
    places = [rows_at(256 + core * tok + GRID_W * i, GRID_W, GRID_W) for i in range(2)]

    def halo_copies(layer, i):
        mine = kv.at[layer, places[i], :]
        above = kv.at[layer, rows_at(core * tok + GRID_W * i, GRID_W, GRID_W), :]
        below = kv.at[layer, rows_at(512 + core * tok + GRID_W * i, GRID_W, GRID_W), :]
        to_first = sp == 1
        to_last = sp == n_sp - 2
        at_first = sp == 0
        at_last = sp == n_sp - 1
        low = core == 0
        high = core == 1
        if i == 0:
            down_same, down_same_got = not_first, not_last
        else:
            down_same, down_same_got = to_first, at_first
        plan = (
            (above, up, tp, not_last, not_first),
            (below, down, tp, down_same, down_same_got),
            (
                above,
                up,
                mate,
                not_last & (high | to_last),
                not_first & (low | at_last),
            ),
            (
                below,
                down,
                mate,
                not_first & (low | to_first),
                not_last & (high | at_first),
            ),
        )
        copies = []
        for n, (spot, z, t, sent, got) in enumerate(plan):
            copy = pltpu.make_async_remote_copy(
                src_ref=mine,
                dst_ref=spot,
                send_sem=h_s.at[layer, i, n + 1],
                recv_sem=h_r.at[layer, i, n + 1],
                device_id={"sp": z, "tp": t},
                device_id_type=MESH,
            )
            copies.append((copy, sent, got))
        return mine, copies

    def arrive(coming, slot):
        for copy in coming.pop(slot, ()):
            copy.wait_recv()

    def hand_on(array, row, coming, s_sems, r_sems):
        for came, far, there, (first, size), sem in HAND:
            arrive(coming, came)
            spot = pl.ds(GRID_W * row + first, size)
            copy = send(
                array.at[came, spot, :],
                array.at[there, spot, :],
                s_sems.at[row, sem],
                r_sems.at[row, sem],
                peer(far),
            )
            coming.setdefault(there, []).append(copy)

    conditional = []
    x_gather = first_gather
    for layer in range(layers):
        queries = []
        mates = []
        halos = []
        for i in range(2):
            hand_on(xs.at[layer], i, x_gather[i], x_s.at[layer], x_r.at[layer])
        if layer == 0:
            own_g.wait()
            own_x[1].wait()
            make_bias()
        scale_layer(layer)
        for i in range(2):
            spot = slice(GRID_W * i, GRID_W * (i + 1))
            made = None
            squares = None
            for j in (0,) + ARRIVE:
                arrive(x_gather[i], j)
                block = xs[layer, j, spot]
                wide = block.astype(jnp.float32)
                square = wide * wide
                part = lax.dot_general(
                    block,
                    wg[layer, j],
                    (((1,), (1,)), ((), ())),
                    preferred_element_type=jnp.float32,
                )
                made = part if made is None else made + part
                squares = square if squares is None else squares + square
            mean = jnp.sum(squares, axis=1, keepdims=True) * (1.0 / (feat * chips))
            normed = made * lax.rsqrt(mean + EPS)
            queries.append(normed[:, 0:128].astype(jnp.bfloat16))
            kv[layer, places[i], :] = normed[:, 128:384].astype(jnp.bfloat16)
            mine, copies = halo_copies(layer, i)
            mates.append(send(mine, mine, h_s.at[layer, i, 0], h_r.at[layer, i, 0], {"tp": mate}))
            for copy, sent, _ in copies:

                @pl.when(sent)
                def _(copy=copy):
                    copy.start()

            halos += copies
            conditional += copies
        for copy in mates:
            copy.wait_recv()
        for copy, _, got in halos:

            @pl.when(got)
            def _(copy=copy):
                copy.wait_recv()

        gather = [{}, {}]
        x_gather = [{}, {}]
        cases = [(i, head) for i in range(2) for head in range(2)]
        pairs = [
            kv[
                layer,
                rows_at(starts[i] * GRID_W, ROW_SPAN * GRID_W, GRID_W),
                128 * head : 128 * head + 128,
            ]
            for i, head in cases
        ]
        scores = []
        for (i, head), pair in zip(cases, pairs, strict=True):
            pick = lane_low if head == 1 else jnp.logical_not(lane_low)
            query = jnp.where(pick, queries[i], 0)
            score = lax.dot_general(
                query, pair, (((1,), (1,)), ((), ())), preferred_element_type=jnp.float32
            )
            scores.append(score + bias[layer, head, i])
        peaks = [jnp.max(score, axis=1, keepdims=True) for score in scores]
        lifted = [jnp.exp(score - peak) for score, peak in zip(scores, peaks, strict=True)]
        totals = [jnp.sum(lift, axis=1, keepdims=True) for lift in lifted]
        mixed = [
            jnp.dot(lift.astype(jnp.bfloat16), pair, preferred_element_type=jnp.float32)
            for lift, pair in zip(lifted, pairs, strict=True)
        ]
        outs = [mix / total for mix, total in zip(mixed, totals, strict=True)]
        for i in range(2):
            both = jnp.where(lane_low, outs[2 * i], outs[2 * i + 1])
            atts[layer, 0, GRID_W * i : GRID_W * (i + 1), :] = both.astype(jnp.bfloat16)
        for i in range(2):
            spot = pl.ds(GRID_W * i, GRID_W)
            for j in ORDER:
                copy = send(
                    atts.at[layer, 0, spot, :],
                    atts.at[layer, j, spot, :],
                    a_s.at[layer, i, j],
                    a_r.at[layer, i, j],
                    peer(j),
                )
                gather[i][j] = [copy]
        before = list(sends[: -2 * len(ORDER)])
        del sends[: len(before)]
        for i in range(2):
            hand_on(atts.at[layer], i, gather[i], a_s.at[layer], a_r.at[layer])
        if layer + 1 < layers:
            give_weights(layer + 1)
        for copy in before:
            copy.wait_send()

        own_o[layer].wait()
        o_mate[layer].wait_recv()
        last = []
        kept = []
        for i in range(2):
            spot = pl.ds(GRID_W * i, GRID_W)
            stream = xs[layer, 0, spot].astype(jnp.float32)
            for j in (0,) + ARRIVE:
                arrive(gather[i], j)
                source = lax.rem(chip - j + chips, chips)
                stream = stream + jnp.dot(
                    atts[layer, j, spot],
                    wout[layer, rows_at(source * 128, 128, 128), :],
                    preferred_element_type=jnp.float32,
                )
            final = stream.astype(jnp.bfloat16)
            if layer + 1 < layers:
                xs[layer + 1, 0, spot, :] = final
                for j in ORDER:
                    copy = send(
                        xs.at[layer + 1, 0, spot, :],
                        xs.at[layer + 1, j, spot, :],
                        x_s.at[layer + 1, i, j],
                        x_r.at[layer + 1, i, j],
                        peer(j),
                    )
                    x_gather[i][j] = [copy]
            else:
                swap = core == 0
                last_half[spot, :] = jnp.where(swap, final[:, half:feat], final[:, 0:half])
                place = rows_at(core * tok + GRID_W * i, GRID_W, GRID_W)
                last.append(
                    send(
                        last_half.at[spot, :],
                        out_ref.at[place, :],
                        d2d_s.at[2 + 4 * layers + i],
                        d2d_r.at[2 + 4 * layers + i],
                        {"tp": mate},
                    )
                )
                kept_half[spot, :] = jnp.where(swap, final[:, 0:half], final[:, half:feat])
                copy = pltpu.make_async_copy(
                    kept_half.at[spot, :], out_ref.at[place, :], own_x_sem.at[4 + i]
                )
                copy.start()
                kept.append(copy)
        for copy in last:
            copy.wait_recv()
        for copy in kept:
            copy.wait()
    for copy, sent, _ in conditional:

        @pl.when(sent)
        def _(copy=copy):
            copy.wait_send()

    for copy in sends:
        copy.wait_send()


def body(hidden_in, norm_gain, query_weight, key_weight, value_weight, output_weight, offset_bias):
    n_sp = lax.axis_size("sp")
    n_tp = lax.axis_size("tp")
    chips = n_tp // 2
    layers = norm_gain.shape[0]
    width = norm_gain.shape[1]
    tokens, _ = hidden_in.shape
    tok = tokens // 2
    feat = width // chips
    any_space = pl.BlockSpec(memory_space=pltpu.HBM)
    dma = pltpu.SemaphoreType.DMA
    bf16 = jnp.bfloat16
    table = offset_bias.transpose(0, 2, 1, 3)
    return pl.pallas_call(
        functools.partial(kernel, n_sp, n_tp, layers),
        out_shape=jax.ShapeDtypeStruct(hidden_in.shape, bf16),
        in_specs=[any_space] * 7,
        out_specs=any_space,
        scratch_shapes=[
            pltpu.VMEM(norm_gain.shape, jnp.float32),
            pltpu.VMEM(table.shape, jnp.float32),
            pltpu.VMEM((tokens, feat // 2), bf16),
            pltpu.VMEM((tok, feat // 2), bf16),
            pltpu.VMEM((tok, feat // 2), bf16),
            pltpu.VMEM((layers, chips, tok, feat), bf16),
            pltpu.VMEM((layers, chips, tok, 128), bf16),
            pltpu.VMEM((layers, 768, 256), bf16),
            pltpu.VMEM((layers, 384, width), bf16),
            pltpu.VMEM((layers, chips, 384, feat), bf16),
            pltpu.VMEM((layers, 1024, feat), bf16),
            pltpu.VMEM((3, layers, 16, 128), jnp.float32),
            pltpu.VMEM((layers, 2, 2, GRID_W, ROW_SPAN * GRID_W), jnp.float32),
            dma((layers, 3)),
            dma((layers,)),
            dma((6,)),
            dma((4 + 4 * layers,)),
            dma((4 + 4 * layers,)),
            dma((2, 2, chips)),
            dma((2, 2, chips)),
            dma((layers, 2, chips)),
            dma((layers, 2, chips)),
            dma((layers, 2, chips)),
            dma((layers, 2, chips)),
            dma((layers, 2, 5)),
            dma((layers, 2, 5)),
        ],
        compiler_params=pltpu.CompilerParams(
            collective_id=0, has_side_effects=True, vmem_limit_bytes=67043328
        ),
        name="layers",
    )(hidden_in, norm_gain, query_weight, key_weight, value_weight, output_weight, table)


def solution(mesh):
    return jax.shard_map(
        body,
        mesh=mesh,
        in_specs=(
            P(("grp", "sp"), "tp"),
            P(),
            P(None, "tp", None),
            P(None, "tp", None),
            P(None, "tp", None),
            P(None, None, "tp"),
            P(None, "tp", None, None),
        ),
        out_specs=P(("grp", "sp"), "tp"),
        check_vma=False,
    )
```

```python
import functools

import jax
import jax.numpy as jnp
from jax import lax
from jax.experimental import pallas as pl
from jax.experimental.pallas import tpu as pltpu
from jax.sharding import PartitionSpec as P

HEAD_DIM = 64
GRID_W = 64
ROW_SPAN = 8
COL_SPAN = 16
EPS = 1e-06
NEG = -1e30
MESH = pl.DeviceIdType.MESH
ORDER = (2, 6, 1, 7)
QUEUE = ((0, 2), (0, 6), (1, 2), (1, 6), (0, 1), (0, 7), (1, 1), (1, 7))
ARRIVE = (1, 7, 2, 6, 3, 5, 4)
HALF = GRID_W // 2
HAND = (
    (2, 2, 4, (0, HALF), 4),
    (2, 1, 3, (0, GRID_W), 3),
    (6, -2, 4, (HALF, HALF), 0),
    (6, -1, 5, (0, GRID_W), 5),
)


def kernel(
    n_sp,
    n_tp,
    layers,
    hid_ref,
    gain_hbm,
    wq_ref,
    wk_ref,
    wv_ref,
    wo_ref,
    ob_hbm,
    out_ref,
    gain_ref,
    ob_ref,
    xst,
    last_half,
    kept_half,
    xs,
    atts,
    kv,
    wraw,
    wg,
    wout,
    tab,
    bias,
    own_w_sem,
    own_o_sem,
    own_x_sem,
    d2d_s,
    d2d_r,
    f_s,
    f_r,
    x_s,
    x_r,
    a_s,
    a_r,
    h_s,
    h_r,
):
    chips = n_tp // 2
    tok = xs.shape[2]
    feat = xs.shape[3]
    half = feat // 2
    tp = lax.axis_index("tp")
    sp = lax.axis_index("sp")
    core = lax.rem(tp, 2)
    chip = lax.div(tp, 2)
    mate = tp + 1 - 2 * core
    up = lax.rem(sp + 1, n_sp)
    down = lax.rem(sp + n_sp - 1, n_sp)

    def peer(j):
        return {"tp": lax.rem(tp + 2 * j + n_tp, n_tp)}

    def rows_at(start, size, align):
        return pl.ds(pl.multiple_of(start, align), size)

    greet = [peer(j) for j in ORDER] + [{"tp": mate}]
    greet += [{"tp": lax.rem(mate + 2 * j, n_tp)} for j in ORDER]
    greet += [{"sp": z, "tp": t} for z in (up, down) for t in (tp, mate)]
    barrier = pltpu.get_barrier_semaphore()
    for device in greet:
        pl.semaphore_signal(barrier, inc=1, device_id=device, device_id_type=MESH)

    my_lanes = rows_at(core * half, half, half)
    own_x = [
        pltpu.make_async_copy(hid_ref, xst, own_x_sem.at[0]),
        pltpu.make_async_copy(
            hid_ref.at[rows_at(core * tok, tok, tok), :], xs.at[0, 0, :, my_lanes], own_x_sem.at[1]
        ),
    ]
    own_g = pltpu.make_async_copy(gain_hbm, gain_ref, own_x_sem.at[2])
    own_b = pltpu.make_async_copy(ob_hbm, ob_ref, own_x_sem.at[3])
    for copy in own_x + [own_b, own_g]:
        copy.start()
    w_rows = (
        rows_at(HEAD_DIM * (1 - core), HEAD_DIM, HEAD_DIM),
        rows_at(192 + 64 * core, HEAD_DIM, HEAD_DIM),
        rows_at(128 + 192 * core, HEAD_DIM, HEAD_DIM),
    )
    own_w = []
    own_o = []
    for layer in range(layers):
        for i, w_ref in enumerate((wq_ref, wk_ref, wv_ref)):
            copy = pltpu.make_async_copy(
                w_ref.at[layer], wraw.at[layer, w_rows[i], :], own_w_sem.at[layer, i]
            )
            copy.start()
            own_w.append(copy)
    for layer in range(layers):
        copy = pltpu.make_async_copy(
            wo_ref.at[layer], wout.at[layer, :, my_lanes], own_o_sem.at[layer]
        )
        copy.start()
        own_o.append(copy)

    tab[1] = jnp.zeros(tab.shape[1:], jnp.float32)
    own_b.wait()
    for layer in range(layers):
        for line in range(2 * ROW_SPAN - 1):
            tab[1, layer, line : line + 1, 0:31] = ob_ref[layer, line]
    for layer in range(layers):
        raw = tab[1, layer]
        low = pltpu.roll(raw, 128 - 15, 1)
        high = pltpu.roll(pltpu.roll(raw, 64 - 15, 1), 15, 0)
        tab[0, layer] = low + high

    pl.semaphore_wait(barrier, len(greet))

    sends = []

    def send(src, dst, s_sem, r_sem, device):
        copy = pltpu.make_async_remote_copy(
            src_ref=src,
            dst_ref=dst,
            send_sem=s_sem,
            recv_sem=r_sem,
            device_id=device,
            device_id_type=MESH,
        )
        copy.start()
        sends.append(copy)
        return copy

    own_x[0].wait()
    first_gather = [{}, {}]
    for i, j in QUEUE + ((0, 0), (1, 0)):
        spot = pl.ds(GRID_W * i, GRID_W)
        given = xst.at[rows_at((1 - core) * tok + GRID_W * i, GRID_W, GRID_W), :]
        kept = xst.at[rows_at(core * tok + GRID_W * i, GRID_W, GRID_W), :]
        far = (2 * j + 1 - 2 * core + n_tp) if j else (1 - 2 * core + n_tp)
        there = xs.at[0, j, spot, my_lanes]
        pair = []
        if j:
            pair.append(send(kept, there, f_s.at[i, 0, j], f_r.at[i, 0, j], peer(j)))
        device = {"tp": lax.rem(tp + far, n_tp)}
        pair.append(send(given, there, f_s.at[i, 1, j], f_r.at[i, 1, j], device))
        first_gather[i][j] = pair
    t_mate = send(tab.at[0], tab.at[2], d2d_s.at[1], d2d_r.at[1], {"tp": mate})
    w_mate = []
    o_mate = []

    def give_weights(layer):
        sem = 2 + 4 * layer
        pairs = [
            (w_ref.at[layer], wraw.at[layer, rows, :])
            for w_ref, rows in zip((wq_ref, wk_ref, wv_ref), w_rows, strict=True)
        ]
        pairs.append((wo_ref.at[layer], wout.at[layer, :, my_lanes]))
        for i, (mine, there) in enumerate(pairs):
            copy = send(mine, there, d2d_s.at[sem + i], d2d_r.at[sem + i], {"tp": mate})
            (w_mate if i < 3 else o_mate).append(copy)

    give_weights(0)

    def scale_layer(layer):
        for copy in own_w[3 * layer : 3 * layer + 3]:
            copy.wait()
        for copy in w_mate[3 * layer : 3 * layer + 3]:
            copy.wait_recv()

        def one(j, carry):
            source = lax.rem(chip - j + chips, chips)
            lanes = rows_at(source * feat, feat, feat)
            gain = gain_ref[pl.ds(layer, 1), lanes]
            scale = HEAD_DIM ** (-0.5)
            wg[layer, j, 0:128, :] = (
                wraw[layer, 0:128, lanes].astype(jnp.float32) * (gain * scale)
            ).astype(jnp.bfloat16)
            wg[layer, j, 128:384, :] = (
                wraw[layer, 128:384, lanes].astype(jnp.float32) * gain
            ).astype(jnp.bfloat16)
            return carry

        lax.fori_loop(0, chips, one, 0)

    all_rows = n_sp * 4
    starts = []
    offsets = []
    for i in range(2):
        row = sp * 4 + core * 2 + i
        first = jnp.clip(row - ROW_SPAN // 2, 0, all_rows - ROW_SPAN)
        starts.append(first - sp * 4 + 4)
        offsets.append(first - row + ROW_SPAN - 1)

    def make_bias():
        t_mate.wait_recv()
        lane = lax.broadcasted_iota(jnp.int32, (GRID_W, 128), 1)
        key_col = jnp.where(lane < GRID_W, lane, lane - GRID_W)
        query_col = lax.broadcasted_iota(jnp.int32, (GRID_W, 128), 0)
        window = jnp.clip(query_col - COL_SPAN // 2, 0, GRID_W - COL_SPAN)
        inside = (key_col >= window) & (key_col < window + COL_SPAN)

        def one(layer, carry):
            for head in range(2):
                which = jnp.where(core == head, 0, 2)
                for i in range(2):
                    for pair in range(4):
                        line = tab[which, layer, pl.ds(offsets[i] + 2 * pair, 1), :]
                        wide = jnp.broadcast_to(line, (GRID_W, 128))
                        rolled = pltpu.roll(wide, 0, 1, stride=1, stride_axis=0)
                        bias[layer, head, i, :, 128 * pair : 128 * pair + 128] = jnp.where(
                            inside, rolled, NEG
                        )
            return carry

        lax.fori_loop(0, layers, one, 0)


    lane_low = lax.broadcasted_iota(jnp.int32, (GRID_W, 128), 1) < HEAD_DIM
    not_last = sp < n_sp - 1
    not_first = sp > 0
    places = [rows_at(256 + core * tok + GRID_W * i, GRID_W, GRID_W) for i in range(2)]

    def halo_copies(layer, i):
        mine = kv.at[layer, places[i], :]
        above = kv.at[layer, rows_at(core * tok + GRID_W * i, GRID_W, GRID_W), :]
        below = kv.at[layer, rows_at(512 + core * tok + GRID_W * i, GRID_W, GRID_W), :]
        to_first = sp == 1
        to_last = sp == n_sp - 2
        at_first = sp == 0
        at_last = sp == n_sp - 1
        low = core == 0
        high = core == 1
        if i == 0:
            down_same, down_same_got = not_first, not_last
        else:
            down_same, down_same_got = to_first, at_first
        plan = (
            (above, up, tp, not_last, not_first),
            (below, down, tp, down_same, down_same_got),
            (
                above,
                up,
                mate,
                not_last & (high | to_last),
                not_first & (low | at_last),
            ),
            (
                below,
                down,
                mate,
                not_first & (low | to_first),
                not_last & (high | at_first),
            ),
        )
        copies = []
        for n, (spot, z, t, sent, got) in enumerate(plan):
            copy = pltpu.make_async_remote_copy(
                src_ref=mine,
                dst_ref=spot,
                send_sem=h_s.at[layer, i, n + 1],
                recv_sem=h_r.at[layer, i, n + 1],
                device_id={"sp": z, "tp": t},
                device_id_type=MESH,
            )
            copies.append((copy, sent, got))
        return mine, copies

    def arrive(coming, slot):
        for copy in coming.pop(slot, ()):
            copy.wait_recv()

    def hand_on(array, row, coming, s_sems, r_sems):
        for came, far, there, (first, size), sem in HAND:
            arrive(coming, came)
            spot = pl.ds(GRID_W * row + first, size)
            copy = send(
                array.at[came, spot, :],
                array.at[there, spot, :],
                s_sems.at[row, sem],
                r_sems.at[row, sem],
                peer(far),
            )
            coming.setdefault(there, []).append(copy)

    conditional = []
    x_gather = first_gather
    for layer in range(layers):
        queries = []
        mates = []
        halos = []
        for i in range(2):
            hand_on(xs.at[layer], i, x_gather[i], x_s.at[layer], x_r.at[layer])
        if layer == 0:
            own_g.wait()
            own_x[1].wait()
            make_bias()
        scale_layer(layer)
        for i in range(2):
            spot = slice(GRID_W * i, GRID_W * (i + 1))
            made = None
            squares = None
            for j in (0,) + ARRIVE:
                arrive(x_gather[i], j)
                block = xs[layer, j, spot]
                wide = block.astype(jnp.float32)
                square = wide * wide
                part = lax.dot_general(
                    block,
                    wg[layer, j],
                    (((1,), (1,)), ((), ())),
                    preferred_element_type=jnp.float32,
                )
                made = part if made is None else made + part
                squares = square if squares is None else squares + square
            mean = jnp.sum(squares, axis=1, keepdims=True) * (1.0 / (feat * chips))
            normed = made * lax.rsqrt(mean + EPS)
            queries.append(normed[:, 0:128].astype(jnp.bfloat16))
            kv[layer, places[i], :] = normed[:, 128:384].astype(jnp.bfloat16)
            mine, copies = halo_copies(layer, i)
            mates.append(send(mine, mine, h_s.at[layer, i, 0], h_r.at[layer, i, 0], {"tp": mate}))
            for copy, sent, _ in copies:

                @pl.when(sent)
                def _(copy=copy):
                    copy.start()

            halos += copies
            conditional += copies
        for copy in mates:
            copy.wait_recv()
        for copy, _, got in halos:

            @pl.when(got)
            def _(copy=copy):
                copy.wait_recv()

        gather = [{}, {}]
        x_gather = [{}, {}]
        cases = [(i, head) for i in range(2) for head in range(2)]
        pairs = [
            kv[
                layer,
                rows_at(starts[i] * GRID_W, ROW_SPAN * GRID_W, GRID_W),
                128 * head : 128 * head + 128,
            ]
            for i, head in cases
        ]
        scores = []
        for (i, head), pair in zip(cases, pairs, strict=True):
            pick = lane_low if head == 1 else jnp.logical_not(lane_low)
            query = jnp.where(pick, queries[i], 0)
            score = lax.dot_general(
                query, pair, (((1,), (1,)), ((), ())), preferred_element_type=jnp.float32
            )
            scores.append(score + bias[layer, head, i])
        peaks = [jnp.max(score, axis=1, keepdims=True) for score in scores]
        lifted = [jnp.exp(score - peak) for score, peak in zip(scores, peaks, strict=True)]
        totals = [jnp.sum(lift, axis=1, keepdims=True) for lift in lifted]
        mixed = [
            jnp.dot(lift.astype(jnp.bfloat16), pair, preferred_element_type=jnp.float32)
            for lift, pair in zip(lifted, pairs, strict=True)
        ]
        outs = [mix / total for mix, total in zip(mixed, totals, strict=True)]
        for i in range(2):
            both = jnp.where(lane_low, outs[2 * i], outs[2 * i + 1])
            atts[layer, 0, GRID_W * i : GRID_W * (i + 1), :] = both.astype(jnp.bfloat16)
        for i, j in QUEUE:
            spot = pl.ds(GRID_W * i, GRID_W)
            copy = send(
                atts.at[layer, 0, spot, :],
                atts.at[layer, j, spot, :],
                a_s.at[layer, i, j],
                a_r.at[layer, i, j],
                peer(j),
            )
            gather[i][j] = [copy]
        before = list(sends[: -2 * len(ORDER)])
        del sends[: len(before)]
        for i in range(2):
            hand_on(atts.at[layer], i, gather[i], a_s.at[layer], a_r.at[layer])
        if layer + 1 < layers:
            give_weights(layer + 1)
        for copy in before:
            copy.wait_send()

        own_o[layer].wait()
        o_mate[layer].wait_recv()
        last = []
        kept = []
        for i in range(2):
            spot = pl.ds(GRID_W * i, GRID_W)
            stream = xs[layer, 0, spot].astype(jnp.float32)
            for j in (0,) + ARRIVE:
                arrive(gather[i], j)
                source = lax.rem(chip - j + chips, chips)
                stream = stream + jnp.dot(
                    atts[layer, j, spot],
                    wout[layer, rows_at(source * 128, 128, 128), :],
                    preferred_element_type=jnp.float32,
                )
            final = stream.astype(jnp.bfloat16)
            if layer + 1 < layers:
                xs[layer + 1, 0, spot, :] = final
                for j in ORDER:
                    copy = send(
                        xs.at[layer + 1, 0, spot, :],
                        xs.at[layer + 1, j, spot, :],
                        x_s.at[layer + 1, i, j],
                        x_r.at[layer + 1, i, j],
                        peer(j),
                    )
                    x_gather[i][j] = [copy]
            else:
                swap = core == 0
                last_half[spot, :] = jnp.where(swap, final[:, half:feat], final[:, 0:half])
                place = rows_at(core * tok + GRID_W * i, GRID_W, GRID_W)
                last.append(
                    send(
                        last_half.at[spot, :],
                        out_ref.at[place, :],
                        d2d_s.at[2 + 4 * layers + i],
                        d2d_r.at[2 + 4 * layers + i],
                        {"tp": mate},
                    )
                )
                kept_half[spot, :] = jnp.where(swap, final[:, 0:half], final[:, half:feat])
                copy = pltpu.make_async_copy(
                    kept_half.at[spot, :], out_ref.at[place, :], own_x_sem.at[4 + i]
                )
                copy.start()
                kept.append(copy)
        for copy in last:
            copy.wait_recv()
        for copy in kept:
            copy.wait()
    for copy, sent, _ in conditional:

        @pl.when(sent)
        def _(copy=copy):
            copy.wait_send()

    for copy in sends:
        copy.wait_send()


def body(hidden_in, norm_gain, query_weight, key_weight, value_weight, output_weight, offset_bias):
    n_sp = lax.axis_size("sp")
    n_tp = lax.axis_size("tp")
    chips = n_tp // 2
    layers = norm_gain.shape[0]
    width = norm_gain.shape[1]
    tokens, _ = hidden_in.shape
    tok = tokens // 2
    feat = width // chips
    any_space = pl.BlockSpec(memory_space=pltpu.HBM)
    dma = pltpu.SemaphoreType.DMA
    bf16 = jnp.bfloat16
    table = offset_bias.transpose(0, 2, 1, 3)
    return pl.pallas_call(
        functools.partial(kernel, n_sp, n_tp, layers),
        out_shape=jax.ShapeDtypeStruct(hidden_in.shape, bf16),
        in_specs=[any_space] * 7,
        out_specs=any_space,
        scratch_shapes=[
            pltpu.VMEM(norm_gain.shape, jnp.float32),
            pltpu.VMEM(table.shape, jnp.float32),
            pltpu.VMEM((tokens, feat // 2), bf16),
            pltpu.VMEM((tok, feat // 2), bf16),
            pltpu.VMEM((tok, feat // 2), bf16),
            pltpu.VMEM((layers, chips, tok, feat), bf16),
            pltpu.VMEM((layers, chips, tok, 128), bf16),
            pltpu.VMEM((layers, 768, 256), bf16),
            pltpu.VMEM((layers, 384, width), bf16),
            pltpu.VMEM((layers, chips, 384, feat), bf16),
            pltpu.VMEM((layers, 1024, feat), bf16),
            pltpu.VMEM((3, layers, 16, 128), jnp.float32),
            pltpu.VMEM((layers, 2, 2, GRID_W, ROW_SPAN * GRID_W), jnp.float32),
            dma((layers, 3)),
            dma((layers,)),
            dma((6,)),
            dma((4 + 4 * layers,)),
            dma((4 + 4 * layers,)),
            dma((2, 2, chips)),
            dma((2, 2, chips)),
            dma((layers, 2, chips)),
            dma((layers, 2, chips)),
            dma((layers, 2, chips)),
            dma((layers, 2, chips)),
            dma((layers, 2, 5)),
            dma((layers, 2, 5)),
        ],
        compiler_params=pltpu.CompilerParams(
            collective_id=0, has_side_effects=True, vmem_limit_bytes=67043328
        ),
        name="layers",
    )(hidden_in, norm_gain, query_weight, key_weight, value_weight, output_weight, table)


def solution(mesh):
    return jax.shard_map(
        body,
        mesh=mesh,
        in_specs=(
            P(("grp", "sp"), "tp"),
            P(),
            P(None, "tp", None),
            P(None, "tp", None),
            P(None, "tp", None),
            P(None, None, "tp"),
            P(None, "tp", None, None),
        ),
        out_specs=P(("grp", "sp"), "tp"),
        check_vma=False,
    )
```

```python
import functools

import jax
import jax.numpy as jnp
from jax import lax
from jax.experimental import pallas as pl
from jax.experimental.pallas import tpu as pltpu
from jax.sharding import PartitionSpec as P

HEAD_DIM = 64
GRID_W = 64
ROW_SPAN = 8
COL_SPAN = 16
EPS = 1e-06
NEG = -1e30
MESH = pl.DeviceIdType.MESH
ORDER = (2, 6, 1, 7)
QUEUE = ((0, 2), (0, 6), (1, 2), (1, 6), (0, 1), (0, 7), (1, 1), (1, 7))
ARRIVE = (1, 7, 2, 6, 3, 5, 4)
HALF = GRID_W // 2
HAND = (
    (2, 2, 4, (0, HALF), 4),
    (2, 1, 3, (0, GRID_W), 3),
    (6, -2, 4, (HALF, HALF), 0),
    (6, -1, 5, (0, GRID_W), 5),
)


def kernel(
    n_sp,
    n_tp,
    layers,
    hid_ref,
    gain_hbm,
    wq_ref,
    wk_ref,
    wv_ref,
    wo_ref,
    ob_hbm,
    out_ref,
    gain_ref,
    ob_ref,
    xst,
    last_half,
    kept_half,
    xs,
    atts,
    kv,
    wraw,
    wg,
    wout,
    tab,
    bias,
    own_w_sem,
    own_o_sem,
    own_x_sem,
    d2d_s,
    d2d_r,
    f_s,
    f_r,
    x_s,
    x_r,
    a_s,
    a_r,
    h_s,
    h_r,
):
    chips = n_tp // 2
    tok = xs.shape[2]
    feat = xs.shape[3]
    half = feat // 2
    tp = lax.axis_index("tp")
    sp = lax.axis_index("sp")
    core = lax.rem(tp, 2)
    chip = lax.div(tp, 2)
    mate = tp + 1 - 2 * core
    up = lax.rem(sp + 1, n_sp)
    down = lax.rem(sp + n_sp - 1, n_sp)

    def peer(j):
        return {"tp": lax.rem(tp + 2 * j + n_tp, n_tp)}

    def rows_at(start, size, align):
        return pl.ds(pl.multiple_of(start, align), size)

    greet = [peer(j) for j in ORDER] + [{"tp": mate}]
    greet += [{"tp": lax.rem(mate + 2 * j, n_tp)} for j in ORDER]
    greet += [{"sp": z, "tp": t} for z in (up, down) for t in (tp, mate)]
    barrier = pltpu.get_barrier_semaphore()
    for device in greet:
        pl.semaphore_signal(barrier, inc=1, device_id=device, device_id_type=MESH)

    my_lanes = rows_at(core * half, half, half)
    own_x = [
        pltpu.make_async_copy(hid_ref, xst, own_x_sem.at[0]),
        pltpu.make_async_copy(
            hid_ref.at[rows_at(core * tok, tok, tok), :], xs.at[0, 0, :, my_lanes], own_x_sem.at[1]
        ),
    ]
    own_g = pltpu.make_async_copy(gain_hbm, gain_ref, own_x_sem.at[2])
    own_b = pltpu.make_async_copy(ob_hbm, ob_ref, own_x_sem.at[3])
    for copy in own_x + [own_b, own_g]:
        copy.start()
    w_rows = (
        rows_at(HEAD_DIM * (1 - core), HEAD_DIM, HEAD_DIM),
        rows_at(192 + 64 * core, HEAD_DIM, HEAD_DIM),
        rows_at(128 + 192 * core, HEAD_DIM, HEAD_DIM),
    )
    own_w = []
    own_o = []
    for layer in range(layers):
        for i, w_ref in enumerate((wq_ref, wk_ref, wv_ref)):
            copy = pltpu.make_async_copy(
                w_ref.at[layer], wraw.at[layer, w_rows[i], :], own_w_sem.at[layer, i]
            )
            copy.start()
            own_w.append(copy)
    for layer in range(layers):
        copy = pltpu.make_async_copy(
            wo_ref.at[layer], wout.at[layer, :, my_lanes], own_o_sem.at[layer]
        )
        copy.start()
        own_o.append(copy)

    tab[1] = jnp.zeros(tab.shape[1:], jnp.float32)
    own_b.wait()
    for layer in range(layers):
        for line in range(2 * ROW_SPAN - 1):
            tab[1, layer, line : line + 1, 0:31] = ob_ref[layer, line]
    for layer in range(layers):
        raw = tab[1, layer]
        low = pltpu.roll(raw, 128 - 15, 1)
        high = pltpu.roll(pltpu.roll(raw, 64 - 15, 1), 15, 0)
        tab[0, layer] = low + high

    pl.semaphore_wait(barrier, len(greet))

    sends = []

    def send(src, dst, s_sem, r_sem, device):
        copy = pltpu.make_async_remote_copy(
            src_ref=src,
            dst_ref=dst,
            send_sem=s_sem,
            recv_sem=r_sem,
            device_id=device,
            device_id_type=MESH,
        )
        copy.start()
        sends.append(copy)
        return copy

    own_x[0].wait()
    first_gather = [{}, {}]
    for i, j in QUEUE + ((0, 0), (1, 0)):
        spot = pl.ds(GRID_W * i, GRID_W)
        given = xst.at[rows_at((1 - core) * tok + GRID_W * i, GRID_W, GRID_W), :]
        kept = xst.at[rows_at(core * tok + GRID_W * i, GRID_W, GRID_W), :]
        far = (2 * j + 1 - 2 * core + n_tp) if j else (1 - 2 * core + n_tp)
        there = xs.at[0, j, spot, my_lanes]
        pair = []
        if j:
            pair.append(send(kept, there, f_s.at[i, 0, j], f_r.at[i, 0, j], peer(j)))
        device = {"tp": lax.rem(tp + far, n_tp)}
        pair.append(send(given, there, f_s.at[i, 1, j], f_r.at[i, 1, j], device))
        first_gather[i][j] = pair
    t_mate = send(tab.at[0], tab.at[2], d2d_s.at[1], d2d_r.at[1], {"tp": mate})
    w_mate = []
    o_mate = []

    def give_weights(layer):
        sem = 2 + 4 * layer
        pairs = [
            (w_ref.at[layer], wraw.at[layer, rows, :])
            for w_ref, rows in zip((wq_ref, wk_ref, wv_ref), w_rows, strict=True)
        ]
        pairs.append((wo_ref.at[layer], wout.at[layer, :, my_lanes]))
        for i, (mine, there) in enumerate(pairs):
            copy = send(mine, there, d2d_s.at[sem + i], d2d_r.at[sem + i], {"tp": mate})
            (w_mate if i < 3 else o_mate).append(copy)

    give_weights(0)

    def scale_layer(layer):
        for copy in own_w[3 * layer : 3 * layer + 3]:
            copy.wait()
        for copy in w_mate[3 * layer : 3 * layer + 3]:
            copy.wait_recv()

        def one(j, carry):
            source = lax.rem(chip - j + chips, chips)
            lanes = rows_at(source * feat, feat, feat)
            gain = gain_ref[pl.ds(layer, 1), lanes]
            scale = HEAD_DIM ** (-0.5)
            wg[layer, j, 0:128, :] = (
                wraw[layer, 0:128, lanes].astype(jnp.float32) * (gain * scale)
            ).astype(jnp.bfloat16)
            wg[layer, j, 128:384, :] = (
                wraw[layer, 128:384, lanes].astype(jnp.float32) * gain
            ).astype(jnp.bfloat16)
            return carry

        lax.fori_loop(0, chips, one, 0)

    all_rows = n_sp * 4
    starts = []
    offsets = []
    for i in range(2):
        row = sp * 4 + core * 2 + i
        first = jnp.clip(row - ROW_SPAN // 2, 0, all_rows - ROW_SPAN)
        starts.append(first - sp * 4 + 4)
        offsets.append(first - row + ROW_SPAN - 1)

    def make_bias():
        t_mate.wait_recv()
        lane = lax.broadcasted_iota(jnp.int32, (GRID_W, 128), 1)
        key_col = jnp.where(lane < GRID_W, lane, lane - GRID_W)
        query_col = lax.broadcasted_iota(jnp.int32, (GRID_W, 128), 0)
        window = jnp.clip(query_col - COL_SPAN // 2, 0, GRID_W - COL_SPAN)
        inside = (key_col >= window) & (key_col < window + COL_SPAN)

        def one(layer, carry):
            for head in range(2):
                which = jnp.where(core == head, 0, 2)
                for i in range(2):
                    for pair in range(4):
                        line = tab[which, layer, pl.ds(offsets[i] + 2 * pair, 1), :]
                        wide = jnp.broadcast_to(line, (GRID_W, 128))
                        rolled = pltpu.roll(wide, 0, 1, stride=1, stride_axis=0)
                        bias[layer, head, i, :, 128 * pair : 128 * pair + 128] = jnp.where(
                            inside, rolled, NEG
                        )
            return carry

        lax.fori_loop(0, layers, one, 0)


    lane_low = lax.broadcasted_iota(jnp.int32, (GRID_W, 128), 1) < HEAD_DIM
    not_last = sp < n_sp - 1
    not_first = sp > 0
    places = [rows_at(256 + core * tok + GRID_W * i, GRID_W, GRID_W) for i in range(2)]

    def halo_copies(layer, i):
        mine = kv.at[layer, places[i], :]
        above = kv.at[layer, rows_at(core * tok + GRID_W * i, GRID_W, GRID_W), :]
        below = kv.at[layer, rows_at(512 + core * tok + GRID_W * i, GRID_W, GRID_W), :]
        to_first = sp == 1
        to_last = sp == n_sp - 2
        at_first = sp == 0
        at_last = sp == n_sp - 1
        low = core == 0
        high = core == 1
        if i == 0:
            down_same, down_same_got = not_first, not_last
        else:
            down_same, down_same_got = to_first, at_first
        plan = (
            (above, up, tp, not_last, not_first),
            (below, down, tp, down_same, down_same_got),
            (
                above,
                up,
                mate,
                not_last & (high | to_last),
                not_first & (low | at_last),
            ),
            (
                below,
                down,
                mate,
                not_first & (low | to_first),
                not_last & (high | at_first),
            ),
        )
        copies = []
        for n, (spot, z, t, sent, got) in enumerate(plan):
            copy = pltpu.make_async_remote_copy(
                src_ref=mine,
                dst_ref=spot,
                send_sem=h_s.at[layer, i, n + 1],
                recv_sem=h_r.at[layer, i, n + 1],
                device_id={"sp": z, "tp": t},
                device_id_type=MESH,
            )
            copies.append((copy, sent, got))
        return mine, copies

    def arrive(coming, slot):
        for copy in coming.pop(slot, ()):
            copy.wait_recv()

    def hand_on(array, row, coming, s_sems, r_sems):
        for came, far, there, (first, size), sem in HAND:
            arrive(coming, came)
            spot = pl.ds(GRID_W * row + first, size)
            copy = send(
                array.at[came, spot, :],
                array.at[there, spot, :],
                s_sems.at[row, sem],
                r_sems.at[row, sem],
                peer(far),
            )
            coming.setdefault(there, []).append(copy)

    conditional = []
    x_gather = first_gather
    for layer in range(layers):
        queries = []
        mates = []
        halos = []
        for i in range(2):
            hand_on(xs.at[layer], i, x_gather[i], x_s.at[layer], x_r.at[layer])
        if layer == 0:
            own_g.wait()
            own_x[1].wait()
            make_bias()
        scale_layer(layer)
        for i in range(2):
            spot = slice(GRID_W * i, GRID_W * (i + 1))
            made = None
            squares = None
            for j in (0,) + ARRIVE:
                arrive(x_gather[i], j)
                block = xs[layer, j, spot]
                wide = block.astype(jnp.float32)
                square = wide * wide
                part = lax.dot_general(
                    block,
                    wg[layer, j],
                    (((1,), (1,)), ((), ())),
                    preferred_element_type=jnp.float32,
                )
                made = part if made is None else made + part
                squares = square if squares is None else squares + square
            mean = jnp.sum(squares, axis=1, keepdims=True) * (1.0 / (feat * chips))
            normed = made * lax.rsqrt(mean + EPS)
            queries.append(normed[:, 0:128].astype(jnp.bfloat16))
            kv[layer, places[i], :] = normed[:, 128:384].astype(jnp.bfloat16)
            mine, copies = halo_copies(layer, i)
            mates.append(send(mine, mine, h_s.at[layer, i, 0], h_r.at[layer, i, 0], {"tp": mate}))
            for copy, sent, _ in copies:

                @pl.when(sent)
                def _(copy=copy):
                    copy.start()

            halos += copies
            conditional += copies
        for copy in mates:
            copy.wait_recv()
        for copy, _, got in halos:

            @pl.when(got)
            def _(copy=copy):
                copy.wait_recv()

        gather = [{}, {}]
        x_gather = [{}, {}]
        cases = [(i, head) for i in range(2) for head in range(2)]
        pairs = [
            kv[
                layer,
                rows_at(starts[i] * GRID_W, ROW_SPAN * GRID_W, GRID_W),
                128 * head : 128 * head + 128,
            ]
            for i, head in cases
        ]
        scores = []
        for (i, head), pair in zip(cases, pairs, strict=True):
            pick = lane_low if head == 1 else jnp.logical_not(lane_low)
            query = jnp.where(pick, queries[i], 0)
            score = lax.dot_general(
                query, pair, (((1,), (1,)), ((), ())), preferred_element_type=jnp.float32
            )
            scores.append(score + bias[layer, head, i])
        peaks = [jnp.max(score, axis=1, keepdims=True) for score in scores]
        lifted = [jnp.exp(score - peak) for score, peak in zip(scores, peaks, strict=True)]
        totals = [jnp.sum(lift, axis=1, keepdims=True) for lift in lifted]
        mixed = [
            jnp.dot(lift.astype(jnp.bfloat16), pair, preferred_element_type=jnp.float32)
            for lift, pair in zip(lifted, pairs, strict=True)
        ]
        outs = [mix / total for mix, total in zip(mixed, totals, strict=True)]
        for i in range(2):
            both = jnp.where(lane_low, outs[2 * i], outs[2 * i + 1])
            atts[layer, 0, GRID_W * i : GRID_W * (i + 1), :] = both.astype(jnp.bfloat16)
        for i, j in QUEUE:
            spot = pl.ds(GRID_W * i, GRID_W)
            copy = send(
                atts.at[layer, 0, spot, :],
                atts.at[layer, j, spot, :],
                a_s.at[layer, i, j],
                a_r.at[layer, i, j],
                peer(j),
            )
            gather[i][j] = [copy]
        before = list(sends[: -2 * len(ORDER)])
        del sends[: len(before)]
        for i in range(2):
            hand_on(atts.at[layer], i, gather[i], a_s.at[layer], a_r.at[layer])
        if layer + 1 < layers:
            give_weights(layer + 1)
        for copy in before:
            copy.wait_send()

        own_o[layer].wait()
        o_mate[layer].wait_recv()
        last = []
        kept = []
        for i in range(2):
            spot = pl.ds(GRID_W * i, GRID_W)
            stream = xs[layer, 0, spot].astype(jnp.float32)
            for j in (0,) + ARRIVE:
                arrive(gather[i], j)
                source = lax.rem(chip - j + chips, chips)
                stream = stream + jnp.dot(
                    atts[layer, j, spot],
                    wout[layer, rows_at(source * 128, 128, 128), :],
                    preferred_element_type=jnp.float32,
                )
            final = stream.astype(jnp.bfloat16)
            if layer + 1 < layers:
                xs[layer + 1, 0, spot, :] = final
                for j in ORDER:
                    copy = send(
                        xs.at[layer + 1, 0, spot, :],
                        xs.at[layer + 1, j, spot, :],
                        x_s.at[layer + 1, i, j],
                        x_r.at[layer + 1, i, j],
                        peer(j),
                    )
                    x_gather[i][j] = [copy]
            else:
                swap = core == 0
                last_half[spot, :] = jnp.where(swap, final[:, half:feat], final[:, 0:half])
                place = rows_at(core * tok + GRID_W * i, GRID_W, GRID_W)
                last.append(
                    send(
                        last_half.at[spot, :],
                        out_ref.at[place, :],
                        d2d_s.at[2 + 4 * layers + i],
                        d2d_r.at[2 + 4 * layers + i],
                        {"tp": mate},
                    )
                )
                kept_half[spot, :] = jnp.where(swap, final[:, 0:half], final[:, half:feat])
                copy = pltpu.make_async_copy(
                    kept_half.at[spot, :], out_ref.at[place, :], own_x_sem.at[4 + i]
                )
                copy.start()
                kept.append(copy)
    for copy, sent, _ in conditional:

        @pl.when(sent)
        def _(copy=copy):
            copy.wait_send()

    for copy in sends:
        copy.wait_send()
    for copy in last:
        copy.wait_recv()
    for copy in kept:
        copy.wait()


def body(hidden_in, norm_gain, query_weight, key_weight, value_weight, output_weight, offset_bias):
    n_sp = lax.axis_size("sp")
    n_tp = lax.axis_size("tp")
    chips = n_tp // 2
    layers = norm_gain.shape[0]
    width = norm_gain.shape[1]
    tokens, _ = hidden_in.shape
    tok = tokens // 2
    feat = width // chips
    any_space = pl.BlockSpec(memory_space=pltpu.HBM)
    dma = pltpu.SemaphoreType.DMA
    bf16 = jnp.bfloat16
    table = offset_bias.transpose(0, 2, 1, 3)
    return pl.pallas_call(
        functools.partial(kernel, n_sp, n_tp, layers),
        out_shape=jax.ShapeDtypeStruct(hidden_in.shape, bf16),
        in_specs=[any_space] * 7,
        out_specs=any_space,
        scratch_shapes=[
            pltpu.VMEM(norm_gain.shape, jnp.float32),
            pltpu.VMEM(table.shape, jnp.float32),
            pltpu.VMEM((tokens, feat // 2), bf16),
            pltpu.VMEM((tok, feat // 2), bf16),
            pltpu.VMEM((tok, feat // 2), bf16),
            pltpu.VMEM((layers, chips, tok, feat), bf16),
            pltpu.VMEM((layers, chips, tok, 128), bf16),
            pltpu.VMEM((layers, 768, 256), bf16),
            pltpu.VMEM((layers, 384, width), bf16),
            pltpu.VMEM((layers, chips, 384, feat), bf16),
            pltpu.VMEM((layers, 1024, feat), bf16),
            pltpu.VMEM((3, layers, 16, 128), jnp.float32),
            pltpu.VMEM((layers, 2, 2, GRID_W, ROW_SPAN * GRID_W), jnp.float32),
            dma((layers, 3)),
            dma((layers,)),
            dma((6,)),
            dma((4 + 4 * layers,)),
            dma((4 + 4 * layers,)),
            dma((2, 2, chips)),
            dma((2, 2, chips)),
            dma((layers, 2, chips)),
            dma((layers, 2, chips)),
            dma((layers, 2, chips)),
            dma((layers, 2, chips)),
            dma((layers, 2, 5)),
            dma((layers, 2, 5)),
        ],
        compiler_params=pltpu.CompilerParams(
            collective_id=0, has_side_effects=True, vmem_limit_bytes=67043328
        ),
        name="layers",
    )(hidden_in, norm_gain, query_weight, key_weight, value_weight, output_weight, table)


def solution(mesh):
    return jax.shard_map(
        body,
        mesh=mesh,
        in_specs=(
            P(("grp", "sp"), "tp"),
            P(),
            P(None, "tp", None),
            P(None, "tp", None),
            P(None, "tp", None),
            P(None, None, "tp"),
            P(None, "tp", None, None),
        ),
        out_specs=P(("grp", "sp"), "tp"),
        check_vma=False,
    )
```
